128 devices in a mesh: sp: 16 (over z, y), dp: 8 (over x, core).
Axes of the slice: x: 4, y: 4, z: 4, core: 2. Of those that a mesh axis runs over, the one named last changes fastest.
Arguments:
- tokens: bfloat16 [8, 2048, 2048], P('dp', 'sp'), may hold values from -6 to 6
- cotangent: bfloat16 [8, 2048, 2048], P('dp', 'sp'), may hold values from -6 to 6
- value_weight: bfloat16 [2048, 2048], P(('sp', 'dp')), may hold values from -0.125 to 0.125
- query_heads: bfloat16 [8, 2048, 16, 128], P('dp', None, 'sp'), may hold values from -8 to 8
- key_heads: bfloat16 [8, 2048, 16, 128], P('dp', None, 'sp'), may hold values from -8 to 8
- lambdas: float32 [16], P('sp'), may hold values from 0.3 to 0.8
Outputs:
- grad_query: bfloat16 [8, 2048, 16, 128], P('dp', None, 'sp')
- grad_key: bfloat16 [8, 2048, 16, 128], P('dp', None, 'sp')
- grad_tokens: bfloat16 [8, 2048, 2048], P('dp', 'sp')
- grad_value_weight: float32 [2048, 2048], P(('sp', 'dp'))
- grad_lambda: float32 [16], P('sp')
The draws below stay inside these ranges and needn't reach their ends.
All inputs are finite; a program needn't handle non-finite values.
Results may differ from the reference program's by a relative error of at most 0.0095.
Values may be sent and summed in bfloat16 or wider, within the bound.
A program may use at most 192 MiB of HBM per device.

```python
import jax
import jax.numpy as jnp
from jax import lax

D = 2048
HEADS = 16
HEAD_DIM = 64
QBLOCK = 256
SEQS = 8
LENGTH = 2048
FEATURES = 2048


def pair_heads(key):
    array_shape = (SEQS, LENGTH, HEADS, 2 * HEAD_DIM)
    key_first = jax.random.fold_in(key, 11)
    key_second = jax.random.fold_in(key, 12)
    keys_part = jnp.clip(jax.random.normal(key_first, array_shape, jnp.float32) * 1.32, -8.0, 8.0)
    query_part = jnp.clip(jax.random.normal(key_second, array_shape, jnp.float32) * 1.32, -8.0, 8.0)
    return (query_part, keys_part)


def draw_query_heads(key, part):
    return pair_heads(key)[0].astype(jnp.bfloat16)


def draw_key_heads(key, part):
    return pair_heads(key)[1].astype(jnp.bfloat16)


def spiked(array, own_key, source, target, blocks, factor):
    def block_of(position):
        return (jnp.arange(array.shape[position]) // (array.shape[position] // blocks)).reshape((-1,) + (1,) * (array.ndim - 1 - position))

    first = jax.random.permutation(own_key, blocks)[block_of(target)]
    second = (block_of(target) + blocks // 2) % blocks
    return jnp.where((block_of(source) == first) | (block_of(source) == second), factor * array, array)


def block_levels(stream_key, shape, split, smallest, top_value):
    level, own = 1.0, jax.random.fold_in(stream_key, 6)
    for dim, blocks in split:
        steps = jnp.exp(jax.random.uniform(jax.random.fold_in(own, dim), (blocks,), jnp.float32, smallest / len(split), top_value / len(split)))
        level = level * jnp.repeat(steps, shape[dim] // blocks).reshape([-1 if axis == dim else 1 for axis in range(len(shape))])
    return level


def noise(own_key, shape, spread, limit, split=(), held_as=jnp.bfloat16):
    loudness = block_levels(own_key, shape, split, -0.22, 0.18) if split else 1.0
    values = jax.random.normal(own_key, shape, jnp.float32) * spread * loudness
    return jnp.minimum(jnp.maximum(values, -limit), limit).astype(held_as)


def bell_draw_with(rng, dims, deviation, reach, cuts, heavy, kind=jnp.bfloat16):
    drawn = deviation * jax.random.normal(rng, dims, jnp.float32)
    if cuts:
        drawn = drawn * block_levels(rng, dims, cuts, -0.22, 0.18)
    return jnp.clip(spiked(drawn, jax.random.fold_in(rng, 3), *heavy), -reach, reach).astype(kind)


def setup_inputs(seed: int = 0) -> dict:
    key_of = jax.random.split(jax.random.key(seed), 7)
    tokens = bell_draw_with(key_of[0], (SEQS, LENGTH, D), 1.0, 6.0, ((0, 8), (1, 16)), (1, 2, 16, 2.0))
    cotangent = noise(key_of[1], (SEQS, LENGTH, FEATURES), 1.0, 6.0, ((0, 8), (1, 16)))
    value_weight = noise(key_of[2], (D, FEATURES), D ** -0.5, 0.125, ((0, 128),))
    query_heads = draw_query_heads(jax.random.fold_in(key_of[6], 71), 0)
    key_heads = draw_key_heads(jax.random.fold_in(key_of[6], 71), 0)
    lambdas = jnp.clip(0.3 + 0.5 * jax.random.uniform(key_of[5], (HEADS,), jnp.float32) ** block_levels(key_of[5], (HEADS,), ((0, 16),), -0.2, 0.2), 0.3, 0.8)
    return {"tokens": tokens, "cotangent": cotangent, "value_weight": value_weight, "query_heads": query_heads, "key_heads": key_heads, "lambdas": lambdas}


EPS = 1e-06
NEGATIVE = -1e+30

def head_backward(queries, keys_in, values_in, cotangent, lambdas, block_rows):
    seq_length = queries.shape[0]
    head_count = queries.shape[1]
    head_width = queries.shape[3]
    scaling = head_width ** (-0.5)
    blocks_count = seq_length // block_rows
    positions = jnp.arange(seq_length, dtype=jnp.int32)
    keys_wide = keys_in.astype(jnp.float32)
    values_wide = values_in.astype(jnp.float32)
    lambda_col = lambdas[:, None, None]

    def block_step(totals, block_index):
        grad_key_sum, grad_value_sum, grad_lambda_sum = totals
        offset = (block_index * block_rows).astype(jnp.int32)
        query_block = lax.dynamic_slice_in_dim(queries, offset, block_rows, 0).astype(jnp.float32)
        cotan_block = lax.dynamic_slice_in_dim(cotangent, offset, block_rows, 0).astype(jnp.float32)
        scores = jnp.einsum('qhcd,khcd->hcqk', query_block, keys_wide) * scaling
        rows_pos = offset + jnp.arange(block_rows, dtype=jnp.int32)
        allowed = rows_pos[:, None] >= positions[None, :]
        scores = jnp.where(allowed, scores, NEGATIVE)
        highest = lax.optimization_barrier(jnp.max(scores, axis=-1, keepdims=True))
        exponent = jnp.exp(scores - highest)
        softmaxes = exponent / lax.optimization_barrier(jnp.sum(exponent, axis=-1, keepdims=True))
        weights = (softmaxes[:, 0] - lambda_col * softmaxes[:, 1]).astype(jnp.bfloat16)
        weights_wide = weights.astype(jnp.float32)
        mixed_out = jnp.einsum('hqk,khd->qhd', weights_wide, values_wide)
        inverse = lax.rsqrt(lax.optimization_barrier(jnp.mean(mixed_out * mixed_out, axis=-1, keepdims=True)) + EPS)
        normed = mixed_out * inverse
        grad_mixed = (inverse * (cotan_block - normed * lax.optimization_barrier(jnp.mean(cotan_block * normed, axis=-1, keepdims=True)))).astype(jnp.bfloat16)
        grad_mixed_wide = grad_mixed.astype(jnp.float32)
        grad_weights = jnp.einsum('qhd,khd->hqk', grad_mixed_wide, values_wide)
        grad_value_sum = grad_value_sum + jnp.einsum('hqk,qhd->khd', weights_wide, grad_mixed_wide)
        grad_lambda_sum = grad_lambda_sum - lax.optimization_barrier(jnp.sum(grad_weights * softmaxes[:, 1], axis=(1, 2)))
        first_grad = softmaxes[:, 0] * (grad_weights - lax.optimization_barrier(jnp.sum(grad_weights * softmaxes[:, 0], axis=-1, keepdims=True)))
        second_grad = -lambda_col * softmaxes[:, 1] * (grad_weights - lax.optimization_barrier(jnp.sum(grad_weights * softmaxes[:, 1], axis=-1, keepdims=True)))
        grad_scores = (jnp.stack([first_grad, second_grad], axis=1) * scaling).astype(jnp.bfloat16)
        grad_scores_wide = grad_scores.astype(jnp.float32)
        grad_query_block = jnp.einsum('hcqk,khcd->qhcd', grad_scores_wide, keys_wide).astype(jnp.bfloat16)
        grad_key_sum = grad_key_sum + jnp.einsum('hcqk,qhcd->khcd', grad_scores_wide, query_block)
        return ((grad_key_sum, grad_value_sum, grad_lambda_sum), grad_query_block)
    initial = (jnp.zeros(keys_in.shape, jnp.float32), jnp.zeros(values_in.shape, jnp.float32), jnp.zeros((head_count,), jnp.float32))
    totals, query_blocks = lax.scan(block_step, initial, jnp.arange(blocks_count, dtype=jnp.int32))
    grad_query = query_blocks.reshape(queries.shape)
    return (grad_query, totals[0].astype(jnp.bfloat16), totals[1].astype(jnp.bfloat16), totals[2])

def reference(tokens, cotangent, value_weight, query_heads, key_heads, lambdas):
    seq_count = tokens.shape[0]
    seq_length = tokens.shape[1]
    feature_count = value_weight.shape[1]
    flat_tokens = tokens.reshape(seq_count * seq_length, D)
    values_flat = jnp.dot(flat_tokens, value_weight, preferred_element_type=jnp.float32).astype(jnp.bfloat16)
    values_heads = values_flat.reshape(seq_count, seq_length, HEADS, 2 * HEAD_DIM)
    cotan_heads = cotangent.reshape(seq_count, seq_length, HEADS, 2 * HEAD_DIM)
    queries = query_heads.reshape(seq_count, seq_length, HEADS, 2, HEAD_DIM)
    keys_in = key_heads.reshape(seq_count, seq_length, HEADS, 2, HEAD_DIM)

    def one_sequence(items):
        return head_backward(items[0], items[1], items[2], items[3], lambdas, QBLOCK)
    grad_query, grad_key, grad_value, grad_lambda = lax.map(one_sequence, (queries, keys_in, values_heads, cotan_heads))
    grad_lambda = lax.optimization_barrier(jnp.sum(grad_lambda, axis=0))
    grad_flat = grad_value.reshape(seq_count * seq_length, feature_count)
    grad_tokens = jnp.dot(grad_flat, value_weight.T, preferred_element_type=jnp.float32).astype(jnp.bfloat16)
    grad_weight = jnp.dot(flat_tokens.T, grad_flat, preferred_element_type=jnp.float32)
    return (grad_query.reshape(query_heads.shape), grad_key.reshape(key_heads.shape), grad_tokens.reshape(tokens.shape), grad_weight, grad_lambda)
```

```python
import functools, math
import jax, jax.numpy as jnp
from jax import lax
from jax.experimental import pallas as pl
from jax.experimental.pallas import tpu as pltpu
from jax.sharding import PartitionSpec as P

EPS = 1e-6
B = 256
NB = 8
SCALE = 0.125
LOG2E = 1.4426950408889634
F32 = jnp.float32
BF = jnp.bfloat16

def nt(a, b):
    return lax.dot_general(a, b, (((1,), (1,)), ((), ())), preferred_element_type=F32)

def nn(a, b):
    return lax.dot_general(a, b, (((1,), (0,)), ((), ())), preferred_element_type=F32)

def tri(i, j):
    return (i * (i + 1)) // 2 + j

def paired(lo, n, body):
    def two(p, c):
        body(lo + 2 * p, 2)
        return c
    lax.fori_loop(0, n // 2, two, 0)
    def one(p, c):
        body(lo + n - 1, 1)
        return c
    lax.fori_loop(0, n % 2, one, 0)

def prepare(i, q_ref, k_ref, qz1, qz2, kt):
    rows = pl.ds(pl.multiple_of(i * B, B), B)
    q = q_ref[rows, :]
    first = lax.broadcasted_iota(jnp.int32, (B, 128), 1) < 64
    zero = jnp.zeros_like(q)
    qz1[i] = jnp.where(first, q, zero)
    qz2[i] = jnp.where(first, zero, q)
    kt[i] = k_ref[rows, :].T

def softmaxes(i, lam, k_ref, qz1, qz2, s1, s2, p1, p2, aa):
    q1, q2 = qz1[i], qz2[i]

    def score(j, m):
        k = k_ref[pl.ds(pl.multiple_of(j * B, B), B), :]
        a, b = nt(k, q1), nt(k, q2)
        return a, b

    def keep(j, a, b, m):
        s1[j] = a
        s2[j] = b
        return (jnp.maximum(m[0], jnp.max(a.reshape(B // 8, 8, B), axis=0)),
                jnp.maximum(m[1], jnp.max(b.reshape(B // 8, 8, B), axis=0)))

    a, b = score(i, None)
    seen = lax.broadcasted_iota(jnp.int32, (B, B), 0) <= lax.broadcasted_iota(jnp.int32, (B, B), 1)
    a = jnp.where(seen, a, -1e30)
    b = jnp.where(seen, b, -1e30)
    low = jnp.full((8, B), -1e30, F32)
    m = keep(i, a, b, (low, low))

    def off(j, m):
        a, b = score(j, m)
        return keep(j, a, b, m)
    def two(p, m):
        a, b = score(2 * p, m)
        c, d = score(2 * p + 1, m)
        m = keep(2 * p, a, b, m)
        return keep(2 * p + 1, c, d, m)
    m = lax.fori_loop(0, i // 2, two, m)
    m = lax.fori_loop(i - i % 2, i, off, m)
    m1 = jnp.max(m[0], axis=0, keepdims=True)
    m2 = jnp.max(m[1], axis=0, keepdims=True)
    c = SCALE * LOG2E

    def power(j, l):
        e1 = jnp.exp2((s1[j] - m1) * c)
        e2 = jnp.exp2((s2[j] - m2) * c)
        s1[j] = e1
        s2[j] = e2
        return (l[0] + jnp.sum(e1.reshape(B // 8, 8, B), axis=0),
                l[1] + jnp.sum(e2.reshape(B // 8, 8, B), axis=0))
    l = lax.fori_loop(0, i + 1, power, (jnp.zeros((8, B), F32), jnp.zeros((8, B), F32)))
    r1 = 1.0 / jnp.sum(l[0], axis=0, keepdims=True)
    r2 = 1.0 / jnp.sum(l[1], axis=0, keepdims=True)

    def norm(j, _):
        x1 = s1[j] * r1
        x2 = s2[j] * r2
        t = tri(i, j)
        p1[t] = x1.astype(BF)
        p2[t] = x2.astype(BF)
        aa[t] = (x1 - lam * x2).astype(BF)
        return _
    lax.fori_loop(0, i + 1, norm, 0)

def mixed(i, lam, vt, p2, aa, cot_ref, dot, do, delta):
    def acc(j, c):
        t = tri(i, j)
        v = vt[j]
        return c[0] + nn(v, aa[t]), c[1] + nn(v, p2[t])
    zero = jnp.zeros((128, B), F32)
    o, o2 = lax.fori_loop(0, i + 1, acc, (zero, zero))
    g = cot_ref[pl.ds(pl.multiple_of(i * B, B), B), :].astype(F32).T
    r = lax.rsqrt(jnp.mean(o * o, axis=0, keepdims=True) + EPS)
    y = r * o
    d = (r * (g - y * jnp.mean(g * y, axis=0, keepdims=True))).astype(BF)
    dw = d.astype(F32)
    d2 = jnp.sum(dw * o2, axis=0, keepdims=True)
    d1 = jnp.sum(dw * o, axis=0, keepdims=True) + lam * d2
    dot[i] = d
    do[i] = dw.T.astype(BF)
    delta[i, 0:1, :] = d1
    delta[i, 1:2, :] = d2
    return d2

def keys_block(j, vn, qz1, qz2, kt, p1, p2, aa, dot, do, delta, dqt):
    v = vn[j]
    k1t, k2t = kt[j, 0:64, :], kt[j, 64:128, :]

    def parts(i):
        t = tri(i, j)
        da = nn(v, dot[i])
        x1 = (p1[t].astype(F32) * (da - delta[i, 0:1, :])).astype(BF)
        x2 = (p2[t].astype(F32) * (da - delta[i, 1:2, :])).astype(BF)
        dv = nn(aa[t], do[i])
        dk1 = nn(x1, qz1[i])
        dk2 = nn(x2, qz2[i])
        dqt[i, 0:64, :] += nn(k1t, x1)
        dqt[i, 64:128, :] += nn(k2t, x2)
        return dv, dk1 , dk2

    def two(p, c):
        a = parts(j + 2 * p)
        b = parts(j + 2 * p + 1)
        return tuple(x + (y + z) for x, y, z in zip(c, a, b))
    def one(p, c):
        a = parts(p)
        return tuple(x + y for x, y in zip(c, a))
    n = NB - j
    zero = jnp.zeros((B, 128), F32)
    c = lax.fori_loop(0, n // 2, two, (zero, zero, zero))
    c = lax.fori_loop(NB - n % 2, NB, one, c)
    return c[0], c[1], c[2]

V = pltpu.VMEM
S = jax.ShapeDtypeStruct


def first_kernel(lam_ref, q_ref, k_ref, p1, p2, aa, qz1, qz2, kt, s1, s2):
    lam = lam_ref[0]
    lax.fori_loop(0, NB, lambda i, c: (prepare(i, q_ref, k_ref, qz1, qz2, kt), c)[1], 0)
    lax.fori_loop(0, NB, lambda i, c: (softmaxes(i, lam, k_ref, qz1, qz2, s1, s2, p1, p2, aa), c)[1], 0)


def second_kernel(lam_ref, q_ref, k_ref, v_ref, cot_ref, p1, p2, aa, gq, gk, gv, gl, qz1, qz2, kt, vt, vn, dot, do, delta, dqt):
    lam = lam_ref[0]

    def prep(i, c):
        prepare(i, q_ref, k_ref, qz1, qz2, kt)
        v = v_ref[pl.ds(pl.multiple_of(i * B, B), B), :]
        vn[i] = v
        vt[i] = v.T
        dqt[i] = jnp.zeros((128, B), F32)
        return c
    lax.fori_loop(0, NB, prep, 0)
    t = lax.fori_loop(0, NB, lambda i, c: c + mixed(i, lam, vt, p2, aa, cot_ref, dot, do, delta), jnp.zeros((1, B), F32))
    gl[...] = jnp.broadcast_to(-jnp.sum(t, axis=1, keepdims=True), (8, 128))
    half = lax.broadcasted_iota(jnp.int32, (1, 128), 1) < 64
    ks = jnp.where(half, SCALE, -lam * SCALE)

    def main(j, c):
        dv, dk1, dk2 = keys_block(j, vn, qz1, qz2, kt, p1, p2, aa, dot, do, delta, dqt)
        rows = pl.ds(pl.multiple_of(j * B, B), B)
        gv[rows, :] = dv.astype(BF)
        gk[rows, :] = ((dk1 + dk2) * ks).astype(BF)
        return c
    lax.fori_loop(0, NB, main, 0)

    def fin(i, c):
        rows = pl.ds(pl.multiple_of(i * B, B), B)
        gq[rows, :] = (dqt[i].T * ks).astype(BF)
        return c
    lax.fori_loop(0, NB, fin, 0)


def body(tokens, cotangent, value_weight, query_heads, key_heads, lambdas):
    L = query_heads.shape[1]
    sp, dp, r = lax.axis_size("sp"), lax.axis_size("dp"), value_weight.shape[0]
    q = query_heads.reshape(L, 128)
    k = key_heads.reshape(L, 128)
    wide = lax.all_gather(tokens, "sp", axis=1, tiled=True)[0]
    full = lax.all_gather(value_weight, ("sp", "dp"), axis=0, tiled=True)
    own = lax.all_to_all(value_weight, "sp", split_axis=1, concat_axis=0, tiled=True)
    wh = lax.all_gather(own.reshape(sp, r, 128), "dp", axis=1).reshape(sp * dp * r, 128)
    cot = lax.all_to_all(cotangent, "sp", split_axis=2, concat_axis=1, tiled=True)[0]
    smem = pl.BlockSpec(memory_space=pltpu.SMEM)
    vm = pl.BlockSpec(memory_space=pltpu.VMEM)
    tiles = (NB * (NB + 1) // 2, B, B)
    p1, p2, aa = pl.pallas_call(
        first_kernel, out_shape=(S(tiles, BF),) * 3, in_specs=[smem, vm, vm], out_specs=[vm] * 3,
        scratch_shapes=[V((NB, B, 128), BF), V((NB, B, 128), BF), V((NB, 128, B), BF), V((NB, B, B), F32), V((NB, B, B), F32)],
        compiler_params=pltpu.CompilerParams(vmem_limit_bytes=48 * 1024 * 1024),
        cost_estimate=pl.CostEstimate(flops=20_000_000_000, bytes_accessed=20_000_000, transcendentals=0),
        name="softmaxes")(lambdas, q, k)
    v = jnp.dot(wide, wh, preferred_element_type=F32).astype(BF)
    gq, gk, gv, gl = pl.pallas_call(
        second_kernel, out_shape=(S((L, 128), BF),) * 3 + (S((8, 128), F32),),
        in_specs=[smem] + [vm] * 7, out_specs=[vm] * 4,
        scratch_shapes=[V((NB, B, 128), BF), V((NB, B, 128), BF), V((NB, 128, B), BF), V((NB, 128, B), BF), V((NB, B, 128), BF),
                        V((NB, 128, B), BF), V((NB, B, 128), BF), V((NB, 8, B), F32), V((NB, 128, B), F32)],
        compiler_params=pltpu.CompilerParams(vmem_limit_bytes=48 * 1024 * 1024),
        cost_estimate=pl.CostEstimate(flops=50_000_000_000, bytes_accessed=20_000_000, transcendentals=0),
        name="gradients")(lambdas, q, k, v, cot, p1, p2, aa)
    lam_all = lax.all_gather(gl[0:1, 0], "dp", axis=0, tiled=True)
    grad_lambda = jnp.sum(lam_all).reshape(1)
    gvt = lax.all_to_all(gv[None], "sp", split_axis=1, concat_axis=2, tiled=True)[0]
    gt = lax.dot_general(gvt, full, (((1,), (1,)), ((), ())), preferred_element_type=F32).astype(BF)[None]
    part = lax.dot_general(wide, gv, (((0,), (0,)), ((), ())), preferred_element_type=F32).astype(BF)
    part = part.reshape(sp, dp, r, 128)
    got = lax.all_to_all(part, "dp", split_axis=1, concat_axis=1, tiled=True)
    summed = jnp.sum(got.astype(F32), axis=1).astype(BF)
    gw = lax.all_to_all(summed.reshape(sp * r, 128), "sp", split_axis=0, concat_axis=1, tiled=True).astype(F32)
    return gq.reshape(query_heads.shape), gk.reshape(key_heads.shape), gt, gw, grad_lambda


def solution(mesh):
    placed = (P("dp", "sp", None), P("dp", "sp", None), P(("sp", "dp"), None),
              P("dp", None, "sp", None), P("dp", None, "sp", None), P("sp"))
    outs = (P("dp", None, "sp", None), P("dp", None, "sp", None), P("dp", "sp", None), P(("sp", "dp"), None), P("sp"))
    return jax.shard_map(body, mesh=mesh, in_specs=placed, out_specs=outs, check_vma=False)
```

```python
import functools, math
import jax, jax.numpy as jnp
from jax import lax
from jax.experimental import pallas as pl
from jax.experimental.pallas import tpu as pltpu
from jax.sharding import PartitionSpec as P

EPS = 1e-6
B = 256
NB = 8
SCALE = 0.125
LOG2E = 1.4426950408889634
F32 = jnp.float32
BF = jnp.bfloat16

def nt(a, b):
    return lax.dot_general(a, b, (((1,), (1,)), ((), ())), preferred_element_type=F32)

def nn(a, b):
    return lax.dot_general(a, b, (((1,), (0,)), ((), ())), preferred_element_type=F32)

def tri(i, j):
    return (i * (i + 1)) // 2 + j

def paired(lo, n, body):
    def two(p, c):
        body(lo + 2 * p, 2)
        return c
    lax.fori_loop(0, n // 2, two, 0)
    def one(p, c):
        body(lo + n - 1, 1)
        return c
    lax.fori_loop(0, n % 2, one, 0)

def prepare(i, q_ref, k_ref, qz1, qz2, kt):
    rows = pl.ds(pl.multiple_of(i * B, B), B)
    q = q_ref[rows, :]
    first = lax.broadcasted_iota(jnp.int32, (B, 128), 1) < 64
    zero = jnp.zeros_like(q)
    qz1[i] = jnp.where(first, q, zero)
    qz2[i] = jnp.where(first, zero, q)
    kt[i] = k_ref[rows, :].T

def softmaxes(i, lam, k_ref, qz1, qz2, s1, s2, p1, p2, aa):
    q1, q2 = qz1[i], qz2[i]

    def score(j, m):
        k = k_ref[pl.ds(pl.multiple_of(j * B, B), B), :]
        a, b = nt(k, q1), nt(k, q2)
        return a, b

    def keep(j, a, b, m):
        s1[j] = a
        s2[j] = b
        return (jnp.maximum(m[0], jnp.max(a.reshape(B // 8, 8, B), axis=0)),
                jnp.maximum(m[1], jnp.max(b.reshape(B // 8, 8, B), axis=0)))

    a, b = score(i, None)
    seen = lax.broadcasted_iota(jnp.int32, (B, B), 0) <= lax.broadcasted_iota(jnp.int32, (B, B), 1)
    a = jnp.where(seen, a, -1e30)
    b = jnp.where(seen, b, -1e30)
    low = jnp.full((8, B), -1e30, F32)
    m = keep(i, a, b, (low, low))

    def off(j, m):
        a, b = score(j, m)
        return keep(j, a, b, m)
    def two(p, m):
        a, b = score(2 * p, m)
        c, d = score(2 * p + 1, m)
        m = keep(2 * p, a, b, m)
        return keep(2 * p + 1, c, d, m)
    m = lax.fori_loop(0, i // 2, two, m)
    m = lax.fori_loop(i - i % 2, i, off, m)
    m1 = jnp.max(m[0], axis=0, keepdims=True)
    m2 = jnp.max(m[1], axis=0, keepdims=True)
    c = SCALE * LOG2E

    def power(j, l):
        e1 = jnp.exp2((s1[j] - m1) * c)
        e2 = jnp.exp2((s2[j] - m2) * c)
        s1[j] = e1
        s2[j] = e2
        return (l[0] + jnp.sum(e1.reshape(B // 8, 8, B), axis=0),
                l[1] + jnp.sum(e2.reshape(B // 8, 8, B), axis=0))
    l = lax.fori_loop(0, i + 1, power, (jnp.zeros((8, B), F32), jnp.zeros((8, B), F32)))
    r1 = 1.0 / jnp.sum(l[0], axis=0, keepdims=True)
    r2 = 1.0 / jnp.sum(l[1], axis=0, keepdims=True)

    def norm(j, _):
        x1 = s1[j] * r1
        x2 = s2[j] * r2
        t = tri(i, j)
        p1[t] = x1.astype(BF)
        p2[t] = x2.astype(BF)
        aa[t] = (x1 - lam * x2).astype(BF)
        return _
    lax.fori_loop(0, i + 1, norm, 0)

def keys_block(j, vn, qz1, qz2, kt, p1, p2, aa, dot, do, delta, dqt):
    v = vn[j]
    k1t, k2t = kt[j, 0:64, :], kt[j, 64:128, :]

    def parts(i):
        t = tri(i, j)
        da = nn(v, dot[i])
        x1 = (p1[t].astype(F32) * (da - delta[i, 0:1, :])).astype(BF)
        x2 = (p2[t].astype(F32) * (da - delta[i, 1:2, :])).astype(BF)
        dv = nn(aa[t], do[i])
        dk1 = nn(x1, qz1[i])
        dk2 = nn(x2, qz2[i])
        dqt[i, 0:64, :] += nn(k1t, x1)
        dqt[i, 64:128, :] += nn(k2t, x2)
        return dv, dk1 , dk2

    def two(p, c):
        a = parts(j + 2 * p)
        b = parts(j + 2 * p + 1)
        return tuple(x + (y + z) for x, y, z in zip(c, a, b))
    def one(p, c):
        a = parts(p)
        return tuple(x + y for x, y in zip(c, a))
    n = NB - j
    zero = jnp.zeros((B, 128), F32)
    c = lax.fori_loop(0, n // 2, two, (zero, zero, zero))
    c = lax.fori_loop(NB - n % 2, NB, one, c)
    return c[0], c[1], c[2]


MESH = pl.DeviceIdType.MESH
V = pltpu.VMEM
S = jax.ShapeDtypeStruct


class Plane:
    def __init__(self, at, ss, rs, sp, dp):
        self.at, self.ss, self.rs, self.dp = at, ss, rs, dp
        self.pos = (lax.rem(sp, 4), lax.div(sp, 4))

    def block(self, k, o, p):
        a = lax.rem(self.pos[k] + (o + 4), 4)
        b = lax.rem(self.pos[1 - k] + (p + 4), 4)
        return b * 4 + a if k == 0 else a * 4 + b

    def copy(self, k, slot, o, p, part, axis, delta):
        s = self.block(k, o, p)
        cols = pl.ds(k * 1024 + (512 if part == 2 else 0), 1024 if part == 0 else 512)
        to = self.block(0, delta, 0) if axis == 0 else self.block(0, 0, delta)
        return pltpu.make_async_remote_copy(
            src_ref=self.at(s, cols), dst_ref=self.at(s, cols), send_sem=self.ss.at[k, slot], recv_sem=self.rs.at[k, slot],
            device_id={"sp": to, "dp": self.dp}, device_id_type=MESH)

    def first(self):
        for k in (0, 1):
            self.copy(k, 0, 0, 0, 0, k, 1).start()
            self.copy(k, 1, 0, 0, 0, k, -1).start()

    def second(self, k, n):
        o = (0, -1, 1, 2)[n]
        self.copy(k, 4 + 4 * n, o, 0, 0, 1 - k, 1).start()
        self.copy(k, 5 + 4 * n, o, 0, 0, 1 - k, -1).start()

    def near(self):
        for k in (0, 1):
            self.copy(k, 0, -1, 0, 0, k, 1).wait_recv()
            self.copy(k, 2, -1, 0, 1, k, 1).start()
            self.copy(k, 1, 1, 0, 0, k, -1).wait_recv()
            self.copy(k, 3, 1, 0, 2, k, -1).start()
        for k in (0, 1):
            self.second(k, 1)
        for k in (0, 1):
            self.second(k, 2)

    def far(self):
        for k in (0, 1):
            self.copy(k, 2, 2, 0, 1, k, 1).wait_recv()
            self.copy(k, 3, 2, 0, 2, k, 1).wait_recv()
            self.second(k, 3)

    def across(self, n):
        o = (0, -1, 1, 2)[n]
        for k in (0, 1):
            self.copy(k, 4 + 4 * n, o, -1, 0, 1 - k, 1).wait_recv()
            self.copy(k, 6 + 4 * n, o, -1, 1, 1 - k, 1).start()
            self.copy(k, 5 + 4 * n, o, 1, 0, 1 - k, -1).wait_recv()
            self.copy(k, 7 + 4 * n, o, 1, 2, 1 - k, -1).start()

    def last(self, n):
        o = (0, -1, 1, 2)[n]
        for k in (0, 1):
            self.copy(k, 6 + 4 * n, o, 2, 1, 1 - k, 1).wait_recv()
            self.copy(k, 7 + 4 * n, o, 2, 2, 1 - k, 1).wait_recv()

    def drain(self):
        for k in (0, 1):
            for slot in range(20):
                self.copy(k, slot, 0, 0, 0 if slot % 4 < 2 else 1, 0, 1).wait_send()


class Row:
    def __init__(self, w, ss, rs, sp, dp):
        self.w, self.ss, self.rs, self.sp, self.dp = w, ss, rs, sp, dp
        self.x, self.c = lax.div(dp, 2), lax.rem(dp, 2)

    def own(self, o):
        return 2 * lax.rem(self.x + (o + 4), 4) + self.c

    def copy(self, slot, o, to, half=None):
        part = pl.ds(0, 16) if half is None else pl.ds(8 * half, 8)
        return pltpu.make_async_remote_copy(
            src_ref=self.w.at[part, self.own(o)], dst_ref=self.w.at[part, self.own(o)],
            send_sem=self.ss.at[slot], recv_sem=self.rs.at[slot],
            device_id={"sp": self.sp, "dp": to}, device_id_type=MESH)

    def other(self, slot, o):
        return self.copy(slot, o, self.dp + 1 - 2 * self.c)

    def start(self):
        self.copy(0, 0, self.own(1)).start()
        self.copy(1, 0, self.own(-1)).start()
        self.other(4, 0).start()

    def near(self):
        self.copy(0, -1, self.own(1)).wait_recv()
        self.copy(2, -1, self.own(1), 0).start()
        self.other(5, -1).start()
        self.copy(1, 1, self.own(-1)).wait_recv()
        self.copy(3, 1, self.own(-1), 1).start()
        self.other(6, 1).start()

    def far(self):
        self.copy(2, 2, self.own(1), 0).wait_recv()
        self.copy(3, 2, self.own(1), 1).wait_recv()
        self.other(7, 2).start()

    def finish(self):
        for slot in (4, 5, 6, 7):
            self.other(slot, 0).wait_recv()
        for slot in (0, 1, 4, 5, 6, 7):
            self.copy(slot, 0, self.own(1)).wait_send()
        for slot in (2, 3):
            self.copy(slot, 0, self.own(1), 0).wait_send()


def kernel(lam_ref, tok_h, cot_h, w_h, q_h, k_h, gq_h, gk_h, gt_h, gw_h, gl_h,
           x, w, wh, cota, q_ref, k_ref, qz1, qz2, kt, vt, vn, s1, s2, p1, p2, aa, dot, do, delta, dqt, ot, o2t,
           dvb, dvrow, gwt, gwp, gwin, gws, gwf, gqb, gkb, gtb, gwo, glb, glin,
           load, save, xs, xr, ws, wr, rs_, rr, h1s, h1r, h2s, h2r, cs, cr, ds_, dr, es, er, ls, lr, fs, fr):
    sp, dp = lax.axis_index("sp"), lax.axis_index("dp")
    lam = lam_ref[0]

    def sp_peers(body):
        lax.fori_loop(1, 16, lambda d, c: (body(lax.rem(sp + d, 16)), c)[1], 0)

    def dp_peers(body):
        lax.fori_loop(1, 8, lambda d, c: (body(lax.rem(dp + d, 8)), c)[1], 0)

    def remote(src, dst, ss, rs, s, d):
        return pltpu.make_async_remote_copy(src_ref=src, dst_ref=dst, send_sem=ss, recv_sem=rs,
                                            device_id={"sp": s, "dp": d}, device_id_type=MESH)

    def lanes(h):
        return pl.ds(pl.multiple_of(h * 128, 128), 128)

    def rows(i, n=B):
        return pl.ds(pl.multiple_of(i * n, n), n)

    barrier = pltpu.get_barrier_semaphore()
    sp_peers(lambda s: pl.semaphore_signal(barrier, inc=1, device_id={"sp": s, "dp": dp}, device_id_type=MESH))
    dp_peers(lambda d: pl.semaphore_signal(barrier, inc=1, device_id={"sp": sp, "dp": d}, device_id_type=MESH))
    loads = [pltpu.make_async_copy(a, b, load.at[n]) for n, (a, b) in enumerate((
        (w_h, w.at[sp, dp]), (tok_h, x.at[sp]), (q_h, q_ref), (k_h, k_ref), (cot_h.at[:, lanes(sp)], cota.at[rows(sp, 128)])))]
    for a in loads:
        a.start()
    wplane = Plane(lambda s, cols: w.at[s, dp, :, cols], ws, wr, sp, dp)
    xplane = Plane(lambda s, cols: x.at[s, :, cols], xs, xr, sp, dp)
    wrow = Row(w, rs_, rr, sp, dp)
    loads[0].wait()
    wh[sp, dp] = w[sp, dp, :, lanes(sp)]
    loads[1].wait()
    pl.semaphore_wait(barrier, 22)

    wplane.first()

    def part_of(s, src, dst):
        return remote(w.at[sp, dp, :, lanes(src)], wh.at[dst, dp], h1s.at[src], h1r.at[dst], s, dp)
    sp_peers(lambda s: part_of(s, s, sp).start())
    xplane.first()
    for k in (0, 1):
        wplane.second(k, 0)
    for n in (2, 3):
        loads[n].wait()

    def prep(i, c):
        prepare(i, q_ref, k_ref, qz1, qz2, kt)
        zero = jnp.zeros((128, B), F32)
        dqt[i] = zero
        ot[i] = zero
        o2t[i] = zero
        return c
    lax.fori_loop(0, NB, prep, 0)

    def soft(lo, hi):
        lax.fori_loop(lo, hi, lambda i, c: (softmaxes(i, lam, k_ref, qz1, qz2, s1, s2, p1, p2, aa), c)[1], 0)

    wplane.near()
    for k in (0, 1):
        xplane.second(k, 0)

    sp_peers(lambda s: part_of(s, sp, s).wait_recv())

    def column(d, src):
        return remote(wh.at[:, src], wh.at[:, src], h2s.at[d], h2r.at[src], sp, d)
    dp_peers(lambda d: column(d, dp).start())
    soft(0, 3)
    for n in (0,):
        wplane.across(n)
    wplane.far()
    xplane.near()
    soft(3, 5)
    for n in (1, 2, 3):
        wplane.across(n)
    xplane.across(0)
    xplane.far()
    soft(5, 6)
    for n in range(4):
        wplane.last(n)
    wrow.start()
    soft(6, 8)
    dp_peers(lambda d: column(dp, d).wait_recv())

    def values(j):
        v = nn(x[pl.ds(2 * j, 2)].reshape(B, 2048), wh[...].reshape(2048, 128)).astype(BF)
        vn[j] = v
        v = v.T
        vt[j] = v

        def add(i, count):
            for m in range(count):
                t = tri(i + m, j)
                ot[i + m] += nn(v, aa[t])
                o2t[i + m] += nn(v, p2[t])
        paired(j, NB - j, add)

    y, z = lax.rem(sp, 4), lax.div(sp, 4)
    side = lax.div(y, 2)

    def pair(dz, which):
        return 2 * lax.rem(z + dz, 4) + (side if which == 0 else 1 - side)
    many = lambda js: lax.fori_loop(0, len(js), lambda n, c: (values(sum(jnp.where(n == m, j, 0) for m, j in enumerate(js))), c)[1], 0)

    many([pair(0, 0)])
    xplane.across(1)
    xplane.across(2)
    many([pair(1, 0), pair(3, 0)])
    xplane.last(0)
    many([pair(0, 1)])
    xplane.across(3)

    def cot_part(s, src, dst):
        return remote(cot_h.at[:, lanes(src)], cota.at[rows(dst, 128)], cs.at[src], cr.at[dst], s, dp)
    sp_peers(lambda s: cot_part(s, s, sp).start())
    xplane.last(1)
    xplane.last(2)
    many([pair(1, 1), pair(3, 1), pair(2, 0)])
    xplane.last(3)
    many([pair(2, 1)])
    wrow.near()
    loads[4].wait()
    sp_peers(lambda s: cot_part(s, sp, s).wait_recv())

    def mix(i, total):
        o, o2 = ot[i], o2t[i]
        g = cota[rows(i), :].astype(F32).T
        r = lax.rsqrt(jnp.mean(o * o, axis=0, keepdims=True) + EPS)
        yy = r * o
        d = (r * (g - yy * jnp.mean(g * yy, axis=0, keepdims=True))).astype(BF)
        dw = d.astype(F32)
        d2 = jnp.sum(dw * o2, axis=0, keepdims=True)
        d1 = jnp.sum(dw * o, axis=0, keepdims=True) + lam * d2
        dot[i] = d
        do[i] = dw.T.astype(BF)
        delta[i, 0:1, :] = d1
        delta[i, 1:2, :] = d2
        return total + d2
    total = lax.fori_loop(0, NB, mix, jnp.zeros((1, B), F32))
    glb[...] = jnp.broadcast_to(-jnp.sum(total, axis=1, keepdims=True), (8, 128))
    gwt[...] = jnp.zeros_like(gwt)

    half = lax.broadcasted_iota(jnp.int32, (1, 128), 1) < 64
    ks = jnp.where(half, SCALE, -lam * SCALE)

    def dv_part(s, t, src):
        return remote(dvb.at[t], dvrow.at[:, lanes(src)], ds_.at[t], dr.at[src], s, dp)

    def main(j, c):
        dv, dk1, dk2 = keys_block(j, vn, qz1, qz2, kt, p1, p2, aa, dot, do, delta, dqt)
        gkb[rows(j), :] = ((dk1 + dk2) * ks).astype(BF)
        dvt = dv.T.astype(BF)
        dvl = dv.astype(BF)
        dvb[2 * j] = dvl[:128]
        dvb[2 * j + 1] = dvl[128:]
        for n in range(4):
            cols = pl.ds(n * 512, 512)
            gwt[:, cols] += nn(dvt, x[pl.ds(2 * j, 2), :, cols].reshape(B, 512))
        for e in range(2):
            t = 2 * j + e

            @pl.when(t != sp)
            def _():
                dv_part(t, t, sp).start()
        return c
    lax.fori_loop(0, NB, main, 0)
    dvrow[:, lanes(sp)] = dvb[sp]

    def out_rows(n, c):
        part = gwt[:, rows(n, 128)].T.astype(BF)
        gwp[n] = part.reshape(8, 16, 128)
        return c
    lax.fori_loop(0, 16, out_rows, 0)

    def gw_part(d, to, src):
        return remote(gwp.at[:, to], gwin.at[src], es.at[to], er.at[src], sp, d)

    def gl_part(d, to, src):
        return remote(glb, glin.at[src], ls.at[to], lr.at[src], sp, d)
    dp_peers(lambda d: gw_part(d, d, dp).start())
    dp_peers(lambda d: gl_part(d, d, dp).start())
    gwin[dp] = gwp[:, dp]
    glin[dp] = glb[...]

    save_k = pltpu.make_async_copy(gkb, gk_h, save.at[0])
    save_k.start()
    wrow.far()

    def fin(i, c):
        gqb[rows(i), :] = (dqt[i].T * ks).astype(BF)
        return c
    lax.fori_loop(0, NB, fin, 0)
    save_q = pltpu.make_async_copy(gqb, gq_h, save.at[1])
    save_q.start()
    sp_peers(lambda s: dv_part(s, s, s).wait_recv())
    wrow.finish()

    def tokens_grad(n, c):
        g = nt(dvrow[...], w[pl.ds(2 * n, 2)].reshape(B, 2048))
        gtb[:, rows(n)] = g.astype(BF)
        return c
    lax.fori_loop(0, NB, tokens_grad, 0)
    save_t = pltpu.make_async_copy(gtb, gt_h, save.at[2])
    save_t.start()

    dp_peers(lambda d: gw_part(d, d, d).wait_recv())
    acc = gwin[0].astype(F32)
    for d in range(1, 8):
        acc = acc + gwin[d].astype(F32)
    gws[...] = acc.astype(BF)

    def fin_part(s, to, src):
        return remote(gws.at[to], gwf.at[src], fs.at[to], fr.at[src], s, dp)
    sp_peers(lambda s: fin_part(s, s, sp).start())
    gwf[sp] = gws[sp]
    dp_peers(lambda d: gl_part(d, d, d).wait_recv())
    tot = glin[0]
    for d in range(1, 8):
        tot = tot + glin[d]
    glb2 = delta
    glb2[0] = jnp.concatenate([tot, tot], axis=1)
    save_l = pltpu.make_async_copy(glb2.at[0, :, pl.ds(0, 128)], gl_h, save.at[3])
    save_l.start()
    xplane.drain()
    wplane.drain()
    sp_peers(lambda s: part_of(s, s, sp).wait_send())
    dp_peers(lambda d: column(d, dp).wait_send())
    sp_peers(lambda s: cot_part(s, s, sp).wait_send())
    sp_peers(lambda s: dv_part(s, s, sp).wait_send())
    dp_peers(lambda d: gw_part(d, d, dp).wait_send())
    dp_peers(lambda d: gl_part(d, d, dp).wait_send())
    sp_peers(lambda s: fin_part(s, s, s).wait_recv())
    for h in range(16):
        gwo[:, h * 128:(h + 1) * 128] = gwf[h].astype(F32)
    save_w = pltpu.make_async_copy(gwo, gw_h, save.at[4])
    save_w.start()
    sp_peers(lambda s: fin_part(s, s, sp).wait_send())
    for a in (save_k, save_q, save_t, save_l, save_w):
        a.wait()


def body(tokens, cotangent, value_weight, query_heads, key_heads, lambdas):
    L = query_heads.shape[1]
    smem = pl.BlockSpec(memory_space=pltpu.SMEM)
    anywhere = pl.BlockSpec(memory_space=pl.ANY)
    tiles = (NB * (NB + 1) // 2, B, B)
    dma = lambda *n: pltpu.SemaphoreType.DMA(n)
    gq, gk, gt, gw, gl = pl.pallas_call(
        kernel,
        out_shape=(S((L, 128), BF), S((L, 128), BF), S((128, 2048), BF), S((16, 2048), F32), S((8, 128), F32)),
        in_specs=[smem] + [anywhere] * 5, out_specs=[anywhere] * 5,
        scratch_shapes=[
            V((16, 128, 2048), BF), V((16, 8, 16, 2048), BF), V((16, 8, 16, 128), BF), V((L, 128), BF), V((L, 128), BF), V((L, 128), BF),
            V((NB, B, 128), BF), V((NB, B, 128), BF), V((NB, 128, B), BF), V((NB, 128, B), BF), V((NB, B, 128), BF),
            V((NB, B, B), F32), V((NB, B, B), F32), V(tiles, BF), V(tiles, BF), V(tiles, BF),
            V((NB, 128, B), BF), V((NB, B, 128), BF), V((NB, 8, B), F32), V((NB, 128, B), F32), V((NB, 128, B), F32), V((NB, 128, B), F32),
            V((16, 128, 128), BF), V((128, 2048), BF), V((128, 2048), F32), V((16, 8, 16, 128), BF), V((8, 16, 16, 128), BF),
            V((16, 16, 128), BF), V((16, 16, 128), BF), V((L, 128), BF), V((L, 128), BF), V((128, 2048), BF), V((16, 2048), F32),
            V((8, 128), F32), V((8, 8, 128), F32),
            dma(5), dma(5), dma(2, 20), dma(2, 20), dma(2, 20), dma(2, 20), dma(8), dma(8), dma(16), dma(16), dma(8), dma(8),
            dma(16), dma(16), dma(16), dma(16), dma(8), dma(8), dma(8), dma(8), dma(16), dma(16)],
        compiler_params=pltpu.CompilerParams(vmem_limit_bytes=60 * 1024 * 1024, collective_id=0, has_side_effects=True),
        name="whole")(lambdas, tokens[0], cotangent[0], value_weight, query_heads.reshape(L, 128), key_heads.reshape(L, 128))
    return gq.reshape(query_heads.shape), gk.reshape(key_heads.shape), gt[None], gw, gl[0, 0:1]


def solution(mesh):
    placed = (P("dp", "sp", None), P("dp", "sp", None), P(("sp", "dp"), None),
              P("dp", None, "sp", None), P("dp", None, "sp", None), P("sp"))
    outs = (P("dp", None, "sp", None), P("dp", None, "sp", None), P("dp", "sp", None), P(("sp", "dp"), None), P("sp"))
    return jax.shard_map(body, mesh=mesh, in_specs=placed, out_specs=outs, check_vma=False)
```

```python
import functools, math
import jax, jax.numpy as jnp
from jax import lax
from jax.experimental import pallas as pl
from jax.experimental.pallas import tpu as pltpu
from jax.sharding import PartitionSpec as P

EPS = 1e-6
B = 256
NB = 8
SCALE = 0.125
LOG2E = 1.4426950408889634
F32 = jnp.float32
BF = jnp.bfloat16

def nt(a, b):
    return lax.dot_general(a, b, (((1,), (1,)), ((), ())), preferred_element_type=F32)

def nn(a, b):
    return lax.dot_general(a, b, (((1,), (0,)), ((), ())), preferred_element_type=F32)

def tri(i, j):
    return (i * (i + 1)) // 2 + j

def paired(lo, n, body):
    def two(p, c):
        body(lo + 2 * p, 2)
        return c
    lax.fori_loop(0, n // 2, two, 0)
    def one(p, c):
        body(lo + n - 1, 1)
        return c
    lax.fori_loop(0, n % 2, one, 0)

def prepare(i, q_ref, k_ref, qz1, qz2, kt):
    rows = pl.ds(pl.multiple_of(i * B, B), B)
    q = q_ref[rows, :]
    first = lax.broadcasted_iota(jnp.int32, (B, 128), 1) < 64
    zero = jnp.zeros_like(q)
    qz1[i] = jnp.where(first, q, zero)
    qz2[i] = jnp.where(first, zero, q)
    kt[i] = k_ref[rows, :].T

def softmaxes(i, lam, k_ref, qz1, qz2, s1, s2, p1, p2, aa):
    q1, q2 = qz1[i], qz2[i]

    def score(j, m):
        k = k_ref[pl.ds(pl.multiple_of(j * B, B), B), :]
        a, b = nt(k, q1), nt(k, q2)
        return a, b

    def keep(j, a, b, m):
        s1[j] = a
        s2[j] = b
        return (jnp.maximum(m[0], jnp.max(a.reshape(B // 8, 8, B), axis=0)),
                jnp.maximum(m[1], jnp.max(b.reshape(B // 8, 8, B), axis=0)))

    a, b = score(i, None)
    seen = lax.broadcasted_iota(jnp.int32, (B, B), 0) <= lax.broadcasted_iota(jnp.int32, (B, B), 1)
    a = jnp.where(seen, a, -1e30)
    b = jnp.where(seen, b, -1e30)
    low = jnp.full((8, B), -1e30, F32)
    m = keep(i, a, b, (low, low))

    def off(j, m):
        a, b = score(j, m)
        return keep(j, a, b, m)
    def two(p, m):
        a, b = score(2 * p, m)
        c, d = score(2 * p + 1, m)
        m = keep(2 * p, a, b, m)
        return keep(2 * p + 1, c, d, m)
    m = lax.fori_loop(0, i // 2, two, m)
    m = lax.fori_loop(i - i % 2, i, off, m)
    m1 = jnp.max(m[0], axis=0, keepdims=True)
    m2 = jnp.max(m[1], axis=0, keepdims=True)
    c = SCALE * LOG2E

    def power(j, l):
        e1 = jnp.exp2((s1[j] - m1) * c)
        e2 = jnp.exp2((s2[j] - m2) * c)
        s1[j] = e1
        s2[j] = e2
        return (l[0] + jnp.sum(e1.reshape(B // 8, 8, B), axis=0),
                l[1] + jnp.sum(e2.reshape(B // 8, 8, B), axis=0))
    l = lax.fori_loop(0, i + 1, power, (jnp.zeros((8, B), F32), jnp.zeros((8, B), F32)))
    r1 = 1.0 / jnp.sum(l[0], axis=0, keepdims=True)
    r2 = 1.0 / jnp.sum(l[1], axis=0, keepdims=True)

    def norm(j, _):
        x1 = s1[j] * r1
        x2 = s2[j] * r2
        t = tri(i, j)
        p1[t] = x1.astype(BF)
        p2[t] = x2.astype(BF)
        aa[t] = (x1 - lam * x2).astype(BF)
        return _
    lax.fori_loop(0, i + 1, norm, 0)

def keys_block(j, vn, qz1, qz2, kt, p1, p2, aa, dot, do, delta, dqt):
    v = vn[j]
    k1t, k2t = kt[j, 0:64, :], kt[j, 64:128, :]

    def parts(i):
        t = tri(i, j)
        da = nn(v, dot[i])
        x1 = (p1[t].astype(F32) * (da - delta[i, 0:1, :])).astype(BF)
        x2 = (p2[t].astype(F32) * (da - delta[i, 1:2, :])).astype(BF)
        dv = nn(aa[t], do[i])
        dk1 = nn(x1, qz1[i])
        dk2 = nn(x2, qz2[i])
        dqt[i, 0:64, :] += nn(k1t, x1)
        dqt[i, 64:128, :] += nn(k2t, x2)
        return dv, dk1 , dk2

    def two(p, c):
        a = parts(j + 2 * p)
        b = parts(j + 2 * p + 1)
        return tuple(x + (y + z) for x, y, z in zip(c, a, b))
    def one(p, c):
        a = parts(p)
        return tuple(x + y for x, y in zip(c, a))
    n = NB - j
    zero = jnp.zeros((B, 128), F32)
    c = lax.fori_loop(0, n // 2, two, (zero, zero, zero))
    c = lax.fori_loop(NB - n % 2, NB, one, c)
    return c[0], c[1], c[2]


MESH = pl.DeviceIdType.MESH
V = pltpu.VMEM
S = jax.ShapeDtypeStruct


class Plane:
    def __init__(self, at, ss, rs, sp, dp):
        self.at, self.ss, self.rs, self.dp = at, ss, rs, dp
        self.pos = (lax.rem(sp, 4), lax.div(sp, 4))

    def block(self, k, o, p):
        a = lax.rem(self.pos[k] + (o + 4), 4)
        b = lax.rem(self.pos[1 - k] + (p + 4), 4)
        return b * 4 + a if k == 0 else a * 4 + b

    def copy(self, k, slot, o, p, part, axis, delta):
        s = self.block(k, o, p)
        cols = pl.ds(k * 1024 + (512 if part == 2 else 0), 1024 if part == 0 else 512)
        to = self.block(0, delta, 0) if axis == 0 else self.block(0, 0, delta)
        return pltpu.make_async_remote_copy(
            src_ref=self.at(s, cols), dst_ref=self.at(s, cols), send_sem=self.ss.at[k, slot], recv_sem=self.rs.at[k, slot],
            device_id={"sp": to, "dp": self.dp}, device_id_type=MESH)

    def first(self):
        for k in (0, 1):
            self.copy(k, 0, 0, 0, 0, k, 1).start()
            self.copy(k, 1, 0, 0, 0, k, -1).start()

    def second(self, k, n):
        o = (0, -1, 1, 2)[n]
        self.copy(k, 4 + 4 * n, o, 0, 0, 1 - k, 1).start()
        self.copy(k, 5 + 4 * n, o, 0, 0, 1 - k, -1).start()

    def near(self):
        for k in (0, 1):
            self.copy(k, 0, -1, 0, 0, k, 1).wait_recv()
            self.copy(k, 2, -1, 0, 1, k, 1).start()
            self.copy(k, 1, 1, 0, 0, k, -1).wait_recv()
            self.copy(k, 3, 1, 0, 2, k, -1).start()
        for k in (0, 1):
            self.second(k, 1)
        for k in (0, 1):
            self.second(k, 2)

    def far(self):
        for k in (0, 1):
            self.copy(k, 2, 2, 0, 1, k, 1).wait_recv()
            self.copy(k, 3, 2, 0, 2, k, 1).wait_recv()
            self.second(k, 3)

    def across(self, n):
        o = (0, -1, 1, 2)[n]
        for k in (0, 1):
            self.copy(k, 4 + 4 * n, o, -1, 0, 1 - k, 1).wait_recv()
            self.copy(k, 6 + 4 * n, o, -1, 1, 1 - k, 1).start()
            self.copy(k, 5 + 4 * n, o, 1, 0, 1 - k, -1).wait_recv()
            self.copy(k, 7 + 4 * n, o, 1, 2, 1 - k, -1).start()

    def last(self, n):
        o = (0, -1, 1, 2)[n]
        for k in (0, 1):
            self.copy(k, 6 + 4 * n, o, 2, 1, 1 - k, 1).wait_recv()
            self.copy(k, 7 + 4 * n, o, 2, 2, 1 - k, 1).wait_recv()

    def drain(self):
        for k in (0, 1):
            for slot in range(20):
                self.copy(k, slot, 0, 0, 0 if slot % 4 < 2 else 1, 0, 1).wait_send()


class Ring:
    def __init__(self, at, ss, rs, sp, dp, axis):
        self.at, self.ss, self.rs, self.sp, self.dp, self.axis = at, ss, rs, sp, dp, axis

    def index(self, o):
        return lax.rem((lax.rem(self.sp, 4) if self.axis == 0 else lax.div(self.sp, 4)) + (o + 4), 4)

    def copy(self, slot, o, part, delta):
        i = self.index(delta)
        to = lax.div(self.sp, 4) * 4 + i if self.axis == 0 else i * 4 + lax.rem(self.sp, 4)
        ref = self.at(self.index(o), part)
        return pltpu.make_async_remote_copy(
            src_ref=ref, dst_ref=ref, send_sem=self.ss(slot), recv_sem=self.rs(slot),
            device_id={"sp": to, "dp": self.dp}, device_id_type=MESH)

    def start(self):
        self.copy(0, 0, None, 1).start()
        self.copy(1, 0, None, -1).start()

    def near(self):
        self.copy(0, -1, None, 1).wait_recv()
        self.copy(2, -1, 0, 1).start()
        self.copy(1, 1, None, -1).wait_recv()
        self.copy(3, 1, 1, -1).start()

    def far(self):
        self.copy(2, 2, 0, 1).wait_recv()
        self.copy(3, 2, 1, 1).wait_recv()

    def drain(self):
        for slot in range(4):
            self.copy(slot, 0, None if slot < 2 else slot - 2, 1).wait_send()


class Row:
    def __init__(self, w, ss, rs, sp, dp):
        self.w, self.ss, self.rs, self.sp, self.dp = w, ss, rs, sp, dp
        self.x, self.c = lax.div(dp, 2), lax.rem(dp, 2)

    def own(self, o):
        return 2 * lax.rem(self.x + (o + 4), 4) + self.c

    def copy(self, slot, o, to, half=None):
        part = pl.ds(0, 16) if half is None else pl.ds(8 * half, 8)
        return pltpu.make_async_remote_copy(
            src_ref=self.w.at[part, self.own(o)], dst_ref=self.w.at[part, self.own(o)],
            send_sem=self.ss.at[slot], recv_sem=self.rs.at[slot],
            device_id={"sp": self.sp, "dp": to}, device_id_type=MESH)

    def other(self, slot, o):
        return self.copy(slot, o, self.dp + 1 - 2 * self.c)

    def start(self):
        self.copy(0, 0, self.own(1)).start()
        self.copy(1, 0, self.own(-1)).start()
        self.other(4, 0).start()

    def near(self):
        self.copy(0, -1, self.own(1)).wait_recv()
        self.copy(2, -1, self.own(1), 0).start()
        self.other(5, -1).start()
        self.copy(1, 1, self.own(-1)).wait_recv()
        self.copy(3, 1, self.own(-1), 1).start()
        self.other(6, 1).start()

    def far(self):
        self.copy(2, 2, self.own(1), 0).wait_recv()
        self.copy(3, 2, self.own(1), 1).wait_recv()
        self.other(7, 2).start()

    def arrived(self):
        for slot in (4, 5, 6, 7):
            self.other(slot, 0).wait_recv()

    def drain(self):
        for slot in (0, 1, 4, 5, 6, 7):
            self.copy(slot, 0, self.own(1)).wait_send()
        for slot in (2, 3):
            self.copy(slot, 0, self.own(1), 0).wait_send()


def kernel(lam_ref, tok_h, cot_h, w_h, q_h, k_h, gq_h, gk_h, gt_h, gw_h, gl_h,
           xr, xc, w, wo, wq, cota, q_ref, k_ref, qz1, qz2, kt, vt, vn, v4, s1, s2, p1, p2, aa, dot, do, delta, dqt, ot, o2t,
           dvg, dvrow, gwt, gwp, gwin, gws, gwf, gqb, gkb, gtb, gwo, glb, glin,
           load, wload, save, xs, xr_, ys, yr, zs, zr, ws, wr, rs_, rr, qs, qr, h1s, h1r, cs, cr, vs, vr, gs, gr, ds_, dr,
           es, er, ls, lr, fs, fr):
    sp, dp = lax.axis_index("sp"), lax.axis_index("dp")
    y, z = lax.rem(sp, 4), lax.div(sp, 4)
    lam = lam_ref[0]
    scope = jax.named_scope

    def sp_peers(body):
        lax.fori_loop(1, 16, lambda d, c: (body(lax.rem(sp + d, 16)), c)[1], 0)

    def dp_peers(body):
        lax.fori_loop(1, 8, lambda d, c: (body(lax.rem(dp + d, 8)), c)[1], 0)

    def remote(src, dst, ss, rs, s, d):
        return pltpu.make_async_remote_copy(src_ref=src, dst_ref=dst, send_sem=ss, recv_sem=rs,
                                            device_id={"sp": s, "dp": d}, device_id_type=MESH)

    def lanes(h, n=128):
        return pl.ds(pl.multiple_of(h * n, n), n)

    def rows(i, n=B):
        return pl.ds(pl.multiple_of(i * n, n), n)

    barrier = pltpu.get_barrier_semaphore()
    sp_peers(lambda s: pl.semaphore_signal(barrier, inc=1, device_id={"sp": s, "dp": dp}, device_id_type=MESH))
    dp_peers(lambda d: pl.semaphore_signal(barrier, inc=1, device_id={"sp": sp, "dp": d}, device_id_type=MESH))
    loads = [pltpu.make_async_copy(a, b, load.at[n]) for n, (a, b) in enumerate((
        (w_h, w.at[sp, dp]), (tok_h, xr.at[y]), (q_h, q_ref), (k_h, k_ref), (cot_h.at[:, lanes(sp)], cota.at[rows(sp, 128)])))]
    for a in loads:
        a.start()
    parts = [pltpu.make_async_copy(w_h.at[:, pl.ds((4 * b + a) * 128, 128)], wo.at[a, :, pl.ds(b * 128, 128)], wload.at[a, b])
             for a in range(4) for b in range(4)]
    for a in parts:
        a.start()

    def half_rows(ref):
        return lambda i, part: ref.at[i] if part is None else ref.at[i, pl.ds(64 * part, 64)]

    wplane = Plane(lambda s, cols: w.at[s, dp, :, cols], ws, wr, sp, dp)
    xring = Ring(half_rows(xr), lambda n: xs.at[n], lambda n: xr_.at[n], sp, dp, 0)
    cring = Ring(lambda i, part: xc.at[i] if part is None else xc.at[i, pl.ds(2 * part, 2)],
                 lambda n: ys.at[n], lambda n: yr.at[n], sp, dp, 0)
    wrow = Row(w, rs_, rr, sp, dp)
    qrow = Row(wq, qs, qr, sp, dp)
    for a in parts + loads[:2]:
        a.wait()
    wq[sp, dp] = wo[y]
    xc[y, z] = xr[y, :, lanes(z, 512)]
    with scope("barrier"):
        pl.semaphore_wait(barrier, 22)

    def head_rows(s, src, to):
        return remote(wo.at[lax.rem(to, 4)], wq.at[src, dp], h1s.at[to], h1r.at[src], s, dp)

    def columns(zz, src, to):
        return remote(xr.at[y, :, lanes(to, 512)], xc.at[y, src], zs.at[to], zr.at[src], zz * 4 + y, dp)

    def z_peers(body):
        for d in (1, 3, 2):
            body(lax.rem(z + d, 4))

    wplane.first()
    sp_peers(lambda s: head_rows(s, sp, s).start())
    xring.start()
    z_peers(lambda t: columns(t, z, t).start())
    for k in (0, 1):
        wplane.second(k, 0)
    for n in (2, 3):
        loads[n].wait()

    def prep(i, c):
        prepare(i, q_ref, k_ref, qz1, qz2, kt)
        zero = jnp.zeros((128, B), F32)
        dqt[i] = zero
        ot[i] = zero
        o2t[i] = zero
        return c
    lax.fori_loop(0, NB, prep, 0)

    def soft(lo, hi):
        lax.fori_loop(lo, hi, lambda i, c: (softmaxes(i, lam, k_ref, qz1, qz2, s1, s2, p1, p2, aa), c)[1], 0)

    with scope("soft03"):
        soft(0, 3)
    with scope("heads"):
        sp_peers(lambda s: head_rows(s, s, sp).wait_recv())
    qrow.start()
    with scope("soft35"):
        soft(3, 5)
    with scope("wnear"):
        wplane.near()
    with scope("soft56"):
        soft(5, 6)
    with scope("qnear"):
        qrow.near()
    with scope("xnear"):
        xring.near()

    def cot_part(s, src, to):
        return remote(cot_h.at[:, lanes(to)], cota.at[rows(src, 128)], cs.at[to], cr.at[src], s, dp)
    sp_peers(lambda s: cot_part(s, sp, s).start())
    with scope("soft67"):
        soft(6, 7)
    with scope("qfar"):
        qrow.far()
    with scope("soft78"):
        soft(7, 8)
    with scope("wacross0"):
        wplane.across(0)
    with scope("wfar"):
        wplane.far()
    with scope("qall"):
        qrow.arrived()
    with scope("xfar"):
        xring.far()

    def v_part(zz, src, to):
        return remote(v4.at[to], vn.at[pl.ds(2 * src, 2)], vs.at[to], vr.at[src], zz * 4 + y, dp)

    with scope("values"):
        for n in (0, 1):
            v = nn(xr[...].reshape(512, 2048), wq[:, :, :, n * 256:(n + 1) * 256].reshape(2048, 256)).astype(BF)
            for m in (0, 1):
                t = 2 * n + m
                v4[t] = v[:, m * 128:(m + 1) * 128].reshape(2, B, 128)

                @pl.when(t != z)
                def _():
                    v_part(t, z, t).start()
        vn[pl.ds(2 * z, 2)] = v4[z]
    with scope("columns"):
        z_peers(lambda t: columns(t, t, z).wait_recv())
    cring.start()

    def mixed(r):
        def one(e, c):
            j = 2 * r + e
            v = vn[j].T
            vt[j] = v

            def add(i, count):
                for m in range(count):
                    t = tri(i + m, j)
                    ot[i + m] += nn(v, aa[t])
                    o2t[i + m] += nn(v, p2[t])
            paired(j, NB - j, add)
            return c
        lax.fori_loop(0, 2, one, 0)

    with scope("mix0"):
        mixed(z)
    with scope("wacross"):
        for n in (1, 2, 3):
            wplane.across(n)
    for d in (1, 3):
        t = lax.rem(z + d, 4)
        with scope("v%d" % d):
            v_part(t, t, z).wait_recv()
        with scope("mix%d" % d):
            mixed(t)
    with scope("wlast"):
        for n in range(4):
            wplane.last(n)
    wrow.start()
    t = lax.rem(z + 2, 4)
    with scope("v2"):
        v_part(t, t, z).wait_recv()
    with scope("mix2"):
        mixed(t)
    with scope("cot"):
        loads[4].wait()
        sp_peers(lambda s: cot_part(s, s, sp).wait_recv())

    def mix(i, total):
        o, o2 = ot[i], o2t[i]
        g = cota[rows(i), :].astype(F32).T
        r = lax.rsqrt(jnp.mean(o * o, axis=0, keepdims=True) + EPS)
        yy = r * o
        d = (r * (g - yy * jnp.mean(g * yy, axis=0, keepdims=True))).astype(BF)
        dw = d.astype(F32)
        d2 = jnp.sum(dw * o2, axis=0, keepdims=True)
        d1 = jnp.sum(dw * o, axis=0, keepdims=True) + lam * d2
        dot[i] = d
        do[i] = dw.T.astype(BF)
        delta[i, 0:1, :] = d1
        delta[i, 1:2, :] = d2
        return total + d2
    with scope("mix"):
        total = lax.fori_loop(0, NB, mix, jnp.zeros((1, B), F32))
    glb[...] = jnp.broadcast_to(-jnp.sum(total, axis=1, keepdims=True), (8, 128))

    half = lax.broadcasted_iota(jnp.int32, (1, 128), 1) < 64
    ks = jnp.where(half, SCALE, -lam * SCALE)

    def gl_part(d, src, to):
        return remote(glb, glin.at[src], ls.at[to], lr.at[src], sp, d)

    def dv_part(s, src, to):
        j = lax.div(to, 2)
        return remote(dvg.at[z, j, rows(lax.rem(to, 2), 128)], dvrow.at[:, lanes(src)], ds_.at[to], dr.at[src], s, dp)

    def dv_ring(j):
        return Ring(lambda i, part: dvg.at[i, j] if part is None else dvg.at[i, j, pl.ds(128 * part, 128)],
                    lambda n: gs.at[j, n], lambda n: gr.at[j, n], sp, dp, 1)

    def main(n, c):
        j = NB - 1 - n
        dv, dk1, dk2 = keys_block(j, vn, qz1, qz2, kt, p1, p2, aa, dot, do, delta, dqt)
        dvg[z, j] = dv.astype(BF)
        gkb[rows(j), :] = ((dk1 + dk2) * ks).astype(BF)
        dv_ring(j).start()
        for e in range(2):
            t = 2 * j + e

            @pl.when(t != sp)
            def _():
                dv_part(t, sp, t).start()

        @pl.when(n >= 4)
        def _():
            dv_ring(j + 4).near()
        return c
    with scope("cnear"):
        cring.near()
    with scope("main"):
        lax.fori_loop(0, NB, main, 0)
    save_k = pltpu.make_async_copy(gkb, gk_h, save.at[0])
    save_k.start()

    def fin(i, c):
        gqb[rows(i), :] = (dqt[i].T * ks).astype(BF)
        return c
    with scope("fin"):
        lax.fori_loop(0, NB, fin, 0)
    save_q = pltpu.make_async_copy(gqb, gq_h, save.at[1])
    save_q.start()
    dvrow[:, lanes(sp)] = dvg[z, lax.div(sp, 2), rows(lax.rem(sp, 2), 128), :]
    gwt[...] = jnp.zeros_like(gwt)

    def weight_part(h, j):
        jz, jy = lax.div(j, 2), lax.rem(j, 2)
        cols = xc[pl.ds(2 * jy, 2), jz].reshape(B, 512)
        gwt[h] += nn(dvg[h, j].T, cols)

    def pieces(lo, hi, offsets):
        def one(j, c):
            for o in offsets:
                weight_part(lax.rem(z + o, 4), j)
            return c
        lax.fori_loop(lo, hi, one, 0)

    with scope("cfar"):
        cring.far()
    with scope("pieces0"):
        pieces(0, 8, (0,))
    with scope("pieces13"):
        pieces(4, 8, (1, 3))

    def late(n, c):
        j = 3 - n
        dv_ring(j).near()
        weight_part(lax.rem(z + 1, 4), j)
        weight_part(lax.rem(z + 3, 4), j)
        return c
    with scope("late"):
        lax.fori_loop(0, 4, late, 0)

    def distant(n, c):
        dv_ring(7 - n).far()
        weight_part(lax.rem(z + 2, 4), 7 - n)
        return c
    with scope("distant"):
        lax.fori_loop(0, 8, distant, 0)

    def out_rows(n, c):
        for h in range(4):
            gwp[n, :, :, h * 128:(h + 1) * 128] = gwt[h, :, rows(n, 128)].T.astype(BF).reshape(8, 16, 128)
        return c
    with scope("outrows"):
        lax.fori_loop(0, 4, out_rows, 0)

    def gw_part(d, src, to):
        return remote(gwp.at[:, to], gwin.at[src], es.at[to], er.at[src], sp, d)
    dp_peers(lambda d: gw_part(d, dp, d).start())
    dp_peers(lambda d: gl_part(d, dp, d).start())
    gwin[dp] = gwp[:, dp]
    glin[dp] = glb[...]
    with scope("wrownear"):
        wrow.near()
    with scope("dvwait"):
        sp_peers(lambda s: dv_part(s, s, sp).wait_recv())
    with scope("wrowfar"):
        wrow.far()
    with scope("gwwait"):
        dp_peers(lambda d: gw_part(d, d, dp).wait_recv())
    acc = gwin[0].astype(F32)
    for d in range(1, 8):
        acc = acc + gwin[d].astype(F32)
    gws[...] = acc.astype(BF)

    def y_peers(body):
        for d in (1, 3, 2):
            body(lax.rem(y + d, 4))

    def fin_part(yy, src, to):
        return remote(gws.at[to], gwf.at[src], fs.at[to], fr.at[src], z * 4 + yy, dp)
    y_peers(lambda t: fin_part(t, y, t).start())
    gwf[y] = gws[y]
    dp_peers(lambda d: gl_part(d, d, dp).wait_recv())
    tot = glin[0]
    for d in range(1, 8):
        tot = tot + glin[d]
    delta[0] = jnp.concatenate([tot, tot], axis=1)
    save_l = pltpu.make_async_copy(delta.at[0, :, pl.ds(0, 128)], gl_h, save.at[3])
    save_l.start()
    with scope("wrowall"):
        wrow.arrived()

    def tokens_grad(n, c):
        g = nt(dvrow[...], w[pl.ds(2 * n, 2)].reshape(B, 2048))
        gtb[:, rows(n)] = g.astype(BF)
        return c
    with scope("tgrad"):
        lax.fori_loop(0, NB, tokens_grad, 0)
    save_t = pltpu.make_async_copy(gtb, gt_h, save.at[2])
    save_t.start()
    with scope("finwait"):
        y_peers(lambda t: fin_part(t, t, y).wait_recv())
    for a in range(4):
        for b in range(4):
            gwo[:, (4 * b + a) * 128:(4 * b + a + 1) * 128] = gwf[a, :, b * 128:(b + 1) * 128].astype(F32)
    save_w = pltpu.make_async_copy(gwo, gw_h, save.at[4])
    save_w.start()
    xring.drain()
    cring.drain()
    wplane.drain()
    wrow.drain()
    qrow.drain()
    lax.fori_loop(0, NB, lambda j, c: (dv_ring(j).drain(), c)[1], 0)
    sp_peers(lambda s: head_rows(s, sp, s).wait_send())
    sp_peers(lambda s: cot_part(s, sp, s).wait_send())
    sp_peers(lambda s: dv_part(s, sp, s).wait_send())
    z_peers(lambda t: columns(t, z, t).wait_send())
    z_peers(lambda t: v_part(t, z, t).wait_send())
    dp_peers(lambda d: gw_part(d, dp, d).wait_send())
    dp_peers(lambda d: gl_part(d, dp, d).wait_send())
    y_peers(lambda t: fin_part(t, y, t).wait_send())
    with scope("savewait"):
        for a in (save_k, save_q, save_t, save_l, save_w):
            a.wait()


def body(tokens, cotangent, value_weight, query_heads, key_heads, lambdas):
    L = query_heads.shape[1]
    smem = pl.BlockSpec(memory_space=pltpu.SMEM)
    anywhere = pl.BlockSpec(memory_space=pl.ANY)
    tiles = (NB * (NB + 1) // 2, B, B)
    dma = lambda *n: pltpu.SemaphoreType.DMA(n)
    gq, gk, gt, gw, gl = pl.pallas_call(
        kernel,
        out_shape=(S((L, 128), BF), S((L, 128), BF), S((128, 2048), BF), S((16, 2048), F32), S((8, 128), F32)),
        in_specs=[smem] + [anywhere] * 5, out_specs=[anywhere] * 5,
        scratch_shapes=[
            V((4, 128, 2048), BF), V((4, 4, 128, 512), BF), V((16, 8, 16, 2048), BF), V((4, 16, 512), BF), V((16, 8, 16, 512), BF),
            V((L, 128), BF), V((L, 128), BF), V((L, 128), BF),
            V((NB, B, 128), BF), V((NB, B, 128), BF), V((NB, 128, B), BF), V((NB, 128, B), BF), V((NB, B, 128), BF), V((4, 2, B, 128), BF),
            V((NB, B, B), F32), V((NB, B, B), F32), V(tiles, BF), V(tiles, BF), V(tiles, BF),
            V((NB, 128, B), BF), V((NB, B, 128), BF), V((NB, 8, B), F32), V((NB, 128, B), F32), V((NB, 128, B), F32), V((NB, 128, B), F32),
            V((4, NB, B, 128), BF), V((128, 2048), BF), V((4, 128, 512), F32), V((4, 8, 16, 512), BF), V((8, 4, 16, 512), BF),
            V((4, 16, 512), BF), V((4, 16, 512), BF), V((L, 128), BF), V((L, 128), BF), V((128, 2048), BF), V((16, 2048), F32),
            V((8, 128), F32), V((8, 8, 128), F32),
            dma(5), dma(4, 4), dma(5), dma(4), dma(4), dma(4), dma(4), dma(4), dma(4), dma(2, 20), dma(2, 20), dma(8), dma(8), dma(8), dma(8),
            dma(16), dma(16), dma(16), dma(16), dma(4), dma(4), dma(8, 4), dma(8, 4), dma(16), dma(16),
            dma(8), dma(8), dma(8), dma(8), dma(4), dma(4)],
        compiler_params=pltpu.CompilerParams(vmem_limit_bytes=60 * 1024 * 1024, collective_id=0, has_side_effects=True),
        name="whole")(lambdas, tokens[0], cotangent[0], value_weight, query_heads.reshape(L, 128), key_heads.reshape(L, 128))
    return gq.reshape(query_heads.shape), gk.reshape(key_heads.shape), gt[None], gw, gl[0, 0:1]


def solution(mesh):
    placed = (P("dp", "sp", None), P("dp", "sp", None), P(("sp", "dp"), None),
              P("dp", None, "sp", None), P("dp", None, "sp", None), P("sp"))
    outs = (P("dp", None, "sp", None), P("dp", None, "sp", None), P("dp", "sp", None), P(("sp", "dp"), None), P("sp"))
    return jax.shard_map(body, mesh=mesh, in_specs=placed, out_specs=outs, check_vma=False)
```

```python
import functools, math
import jax, jax.numpy as jnp
from jax import lax
from jax.experimental import pallas as pl
from jax.experimental.pallas import tpu as pltpu
from jax.sharding import PartitionSpec as P

EPS = 1e-6
B = 256
NB = 8
SCALE = 0.125
LOG2E = 1.4426950408889634
F32 = jnp.float32
BF = jnp.bfloat16

def nt(a, b):
    return lax.dot_general(a, b, (((1,), (1,)), ((), ())), preferred_element_type=F32)

def nn(a, b):
    return lax.dot_general(a, b, (((1,), (0,)), ((), ())), preferred_element_type=F32)

def tri(i, j):
    return (i * (i + 1)) // 2 + j

def paired(lo, n, body):
    def two(p, c):
        body(lo + 2 * p, 2)
        return c
    lax.fori_loop(0, n // 2, two, 0)
    def one(p, c):
        body(lo + n - 1, 1)
        return c
    lax.fori_loop(0, n % 2, one, 0)

def prepare(i, q_ref, k_ref, qz1, qz2, kt):
    rows = pl.ds(pl.multiple_of(i * B, B), B)
    q = q_ref[rows, :]
    first = lax.broadcasted_iota(jnp.int32, (B, 128), 1) < 64
    zero = jnp.zeros_like(q)
    qz1[i] = jnp.where(first, q, zero)
    qz2[i] = jnp.where(first, zero, q)
    kt[i] = k_ref[rows, :].T

def softmaxes(i, lam, k_ref, qz1, qz2, s1, s2, p1, p2, aa):
    q1, q2 = qz1[i], qz2[i]

    def score(j, m):
        k = k_ref[pl.ds(pl.multiple_of(j * B, B), B), :]
        a, b = nt(k, q1), nt(k, q2)
        return a, b

    def keep(j, a, b, m):
        s1[j] = a
        s2[j] = b
        return (jnp.maximum(m[0], jnp.max(a.reshape(B // 8, 8, B), axis=0)),
                jnp.maximum(m[1], jnp.max(b.reshape(B // 8, 8, B), axis=0)))

    a, b = score(i, None)
    seen = lax.broadcasted_iota(jnp.int32, (B, B), 0) <= lax.broadcasted_iota(jnp.int32, (B, B), 1)
    a = jnp.where(seen, a, -1e30)
    b = jnp.where(seen, b, -1e30)
    low = jnp.full((8, B), -1e30, F32)
    m = keep(i, a, b, (low, low))

    def off(j, m):
        a, b = score(j, m)
        return keep(j, a, b, m)
    def two(p, m):
        a, b = score(2 * p, m)
        c, d = score(2 * p + 1, m)
        m = keep(2 * p, a, b, m)
        return keep(2 * p + 1, c, d, m)
    m = lax.fori_loop(0, i // 2, two, m)
    m = lax.fori_loop(i - i % 2, i, off, m)
    m1 = jnp.max(m[0], axis=0, keepdims=True)
    m2 = jnp.max(m[1], axis=0, keepdims=True)
    c = SCALE * LOG2E

    def power(j, l):
        e1 = jnp.exp2((s1[j] - m1) * c)
        e2 = jnp.exp2((s2[j] - m2) * c)
        s1[j] = e1
        s2[j] = e2
        return (l[0] + jnp.sum(e1.reshape(B // 8, 8, B), axis=0),
                l[1] + jnp.sum(e2.reshape(B // 8, 8, B), axis=0))
    l = lax.fori_loop(0, i + 1, power, (jnp.zeros((8, B), F32), jnp.zeros((8, B), F32)))
    r1 = 1.0 / jnp.sum(l[0], axis=0, keepdims=True)
    r2 = 1.0 / jnp.sum(l[1], axis=0, keepdims=True)

    def norm(j, _):
        x1 = s1[j] * r1
        x2 = s2[j] * r2
        t = tri(i, j)
        p1[t] = x1.astype(BF)
        p2[t] = x2.astype(BF)
        aa[t] = (x1 - lam * x2).astype(BF)
        return _
    lax.fori_loop(0, i + 1, norm, 0)

def keys_block(j, vn, qz1, qz2, kt, p1, p2, aa, dot, do, delta, dqt):
    v = vn[j]
    k1t, k2t = kt[j, 0:64, :], kt[j, 64:128, :]

    def parts(i):
        t = tri(i, j)
        da = nn(v, dot[i])
        x1 = (p1[t].astype(F32) * (da - delta[i, 0:1, :])).astype(BF)
        x2 = (p2[t].astype(F32) * (da - delta[i, 1:2, :])).astype(BF)
        dv = nn(aa[t], do[i])
        dk1 = nn(x1, qz1[i])
        dk2 = nn(x2, qz2[i])
        dqt[i, 0:64, :] += nn(k1t, x1)
        dqt[i, 64:128, :] += nn(k2t, x2)
        return dv, dk1 , dk2

    def two(p, c):
        a = parts(j + 2 * p)
        b = parts(j + 2 * p + 1)
        return tuple(x + (y + z) for x, y, z in zip(c, a, b))
    def one(p, c):
        a = parts(p)
        return tuple(x + y for x, y in zip(c, a))
    n = NB - j
    zero = jnp.zeros((B, 128), F32)
    c = lax.fori_loop(0, n // 2, two, (zero, zero, zero))
    c = lax.fori_loop(NB - n % 2, NB, one, c)
    return c[0], c[1], c[2]


MESH = pl.DeviceIdType.MESH
V = pltpu.VMEM
S = jax.ShapeDtypeStruct


class Ring:
    def __init__(self, at, ss, rs, sp, dp, axis):
        self.at, self.ss, self.rs, self.sp, self.dp, self.axis = at, ss, rs, sp, dp, axis

    def index(self, o):
        return lax.rem((lax.rem(self.sp, 4) if self.axis == 0 else lax.div(self.sp, 4)) + (o + 4), 4)

    def copy(self, slot, o, part, delta):
        i = self.index(delta)
        to = lax.div(self.sp, 4) * 4 + i if self.axis == 0 else i * 4 + lax.rem(self.sp, 4)
        ref = self.at(self.index(o), part)
        return pltpu.make_async_remote_copy(
            src_ref=ref, dst_ref=ref, send_sem=self.ss(slot), recv_sem=self.rs(slot),
            device_id={"sp": to, "dp": self.dp}, device_id_type=MESH)

    def start(self):
        self.copy(0, 0, None, 1).start()
        self.copy(1, 0, None, -1).start()

    def near(self):
        self.copy(0, -1, None, 1).wait_recv()
        self.copy(2, -1, 0, 1).start()
        self.copy(1, 1, None, -1).wait_recv()
        self.copy(3, 1, 1, -1).start()

    def far(self):
        self.copy(2, 2, 0, 1).wait_recv()
        self.copy(3, 2, 1, 1).wait_recv()

    def drain(self):
        for slot in range(4):
            self.copy(slot, 0, None if slot < 2 else slot - 2, 1).wait_send()


class SplitRing(Ring):
    def start(self, n):
        self.copy(2 * n, 0, n, 1).start()
        self.copy(2 * n + 1, 0, n, -1).start()

    def near(self, n):
        if n == 0:
            self.copy(0, -1, 0, 1).wait_recv()
            self.copy(4, -1, 0, 1).start()
            self.copy(1, 1, 0, -1).wait_recv()
        else:
            self.copy(3, 1, 1, -1).wait_recv()
            self.copy(5, 1, 1, -1).start()
            self.copy(2, -1, 1, 1).wait_recv()

    def far(self):
        self.copy(4, 2, 0, 1).wait_recv()
        self.copy(5, 2, 1, -1).wait_recv()

    def drain(self):
        for slot, n in enumerate((0, 0, 1, 1, 0, 1)):
            self.copy(slot, 0, n, 1).wait_send()


class Row:
    def __init__(self, w, ss, rs, sp, dp):
        self.w, self.ss, self.rs, self.sp, self.dp = w, ss, rs, sp, dp
        self.x, self.c = lax.div(dp, 2), lax.rem(dp, 2)

    def own(self, o):
        return 2 * lax.rem(self.x + (o + 4), 4) + self.c

    def copy(self, slot, o, to, half=None):
        part = pl.ds(0, 16) if half is None else pl.ds(8 * half, 8)
        return pltpu.make_async_remote_copy(
            src_ref=self.w.at[part, self.own(o)], dst_ref=self.w.at[part, self.own(o)],
            send_sem=self.ss.at[slot], recv_sem=self.rs.at[slot],
            device_id={"sp": self.sp, "dp": to}, device_id_type=MESH)

    def other(self, slot, o):
        return self.copy(slot, o, self.dp + 1 - 2 * self.c)

    def start(self):
        self.copy(0, 0, self.own(1)).start()
        self.copy(1, 0, self.own(-1)).start()
        self.other(4, 0).start()

    def near(self):
        self.copy(0, -1, self.own(1)).wait_recv()
        self.copy(2, -1, self.own(1), 0).start()
        self.other(5, -1).start()
        self.copy(1, 1, self.own(-1)).wait_recv()
        self.copy(3, 1, self.own(-1), 1).start()
        self.other(6, 1).start()

    def far(self):
        self.copy(2, 2, self.own(1), 0).wait_recv()
        self.copy(3, 2, self.own(1), 1).wait_recv()
        self.other(7, 2).start()

    def arrived(self):
        for slot in (4, 5, 6, 7):
            self.other(slot, 0).wait_recv()

    def drain(self):
        for slot in (0, 1, 4, 5, 6, 7):
            self.copy(slot, 0, self.own(1)).wait_send()
        for slot in (2, 3):
            self.copy(slot, 0, self.own(1), 0).wait_send()


def kernel(lam_ref, tok_h, cot_h, w_h, q_h, k_h, gq_h, gk_h, gt_h, gw_h, gl_h,
           xr, xc, w, wo, wq, cota, q_ref, k_ref, qz1, qz2, kt, vt, vn, v4, s1, s2, p1, p2, aa, dot, do, delta, dqt, ot, o2t,
           dvg, dvin, dvrow, gwt, gwp, gwin, gws, gwf, gqb, gkb, gtb, gwo, glb, glin,
           load, wload, save, xs, xr_, ys, yr, zs, zr, ws, wr, rs_, rr, qs, qr, h1s, h1r, cs, cr, vs, vr, gs, gr, ds_, dr,
           es, er, ls, lr, fs, fr):
    sp, dp = lax.axis_index("sp"), lax.axis_index("dp")
    y, z = lax.rem(sp, 4), lax.div(sp, 4)
    lam = lam_ref[0]
    scope = jax.named_scope

    def sp_peers(body):
        lax.fori_loop(1, 16, lambda d, c: (body(lax.rem(sp + d, 16)), c)[1], 0)

    def dp_peers(body):
        lax.fori_loop(1, 8, lambda d, c: (body(lax.rem(dp + d, 8)), c)[1], 0)

    def remote(src, dst, ss, rs, s, d):
        return pltpu.make_async_remote_copy(src_ref=src, dst_ref=dst, send_sem=ss, recv_sem=rs,
                                            device_id={"sp": s, "dp": d}, device_id_type=MESH)

    def all_of(ref, sem):
        pltpu.make_async_copy(ref, ref, sem.at[0]).wait()

    def lanes(h, n=128):
        return pl.ds(pl.multiple_of(h * n, n), n)

    def rows(i, n=B):
        return pl.ds(pl.multiple_of(i * n, n), n)

    barrier = pltpu.get_barrier_semaphore()
    sp_peers(lambda s: pl.semaphore_signal(barrier, inc=1, device_id={"sp": s, "dp": dp}, device_id_type=MESH))
    dp_peers(lambda d: pl.semaphore_signal(barrier, inc=1, device_id={"sp": sp, "dp": d}, device_id_type=MESH))
    loads = [pltpu.make_async_copy(a, b, load.at[n]) for n, (a, b) in enumerate((
        (w_h, w.at[sp, dp]), (tok_h, xr.at[y]), (q_h, q_ref), (k_h, k_ref), (cot_h.at[:, lanes(sp)], cota.at[rows(sp, 128)])))]
    for a in loads:
        a.start()
    parts = [pltpu.make_async_copy(w_h.at[:, pl.ds((4 * b + a) * 128, 128)], wo.at[a, :, pl.ds(b * 128, 128)], wload.at[0])
             for a in range(4) for b in range(4)]
    for a in parts:
        a.start()

    def half_rows(ref):
        return lambda i, part: ref.at[i] if part is None else ref.at[i, pl.ds(64 * part, 64)]

    wy = Ring(lambda i, part: w.at[z * 4 + i, dp] if part is None else w.at[z * 4 + i, dp, :, pl.ds(1024 * part, 1024)],
              lambda n: ws.at[0, n], lambda n: wr.at[0, n], sp, dp, 0)
    wz = Ring(lambda i, part: w.at[pl.ds(4 * i, 4), dp] if part is None else w.at[pl.ds(4 * i + 2 * part, 2), dp],
              lambda n: ws.at[1, n], lambda n: wr.at[1, n], sp, dp, 1)
    xring = SplitRing(half_rows(xr), lambda n: xs.at[n], lambda n: xr_.at[n], sp, dp, 0)
    cring = Ring(lambda i, part: xc.at[i] if part is None else xc.at[i, pl.ds(2 * part, 2)],
                 lambda n: ys.at[n], lambda n: yr.at[n], sp, dp, 0)
    wrow = Row(w, rs_, rr, sp, dp)
    qrow = Row(wq, qs, qr, sp, dp)
    for a in loads[:2]:
        a.wait()
    all_of(wo, wload)
    wq[sp, dp] = wo[y]
    xc[y, z] = xr[y, :, lanes(z, 512)]
    with scope("barrier"):
        pl.semaphore_wait(barrier, 22)

    def head_rows(s, src, to):
        return remote(wo.at[lax.rem(to, 4)], wq.at[src, dp], h1s.at[0], h1r.at[0], s, dp)

    def columns(zz, src, to):
        return remote(xr.at[y, :, lanes(to, 512)], xc.at[y, src], zs.at[0], zr.at[0], zz * 4 + y, dp)

    def z_peers(body):
        for d in (1, 3, 2):
            body(lax.rem(z + d, 4))

    sp_peers(lambda s: head_rows(s, sp, s).start())
    wy.start()
    xring.start(0)
    z_peers(lambda t: columns(t, z, t).start())
    def cot_part(s, src, to):
        return remote(cot_h.at[:, lanes(to)], cota.at[rows(src, 128)], cs.at[0], cr.at[0], s, dp)

    for n in (2, 3):
        loads[n].wait()

    def prep(i, c):
        prepare(i, q_ref, k_ref, qz1, qz2, kt)
        zero = jnp.zeros((128, B), F32)
        dqt[i] = zero
        ot[i] = zero
        o2t[i] = zero
        return c
    lax.fori_loop(0, NB, prep, 0)

    def soft(lo, hi):
        lax.fori_loop(lo, hi, lambda i, c: (softmaxes(i, lam, k_ref, qz1, qz2, s1, s2, p1, p2, aa), c)[1], 0)

    with scope("soft03"):
        soft(0, 3)
    with scope("heads"):
        all_of(wq.at[pl.ds(0, 15), 0], h1r)
    qrow.start()
    with scope("wynear"):
        wy.near()
    xring.start(1)
    with scope("soft35"):
        soft(3, 5)
    with scope("xnear0"):
        xring.near(0)
    with scope("soft56"):
        soft(5, 6)
    with scope("wyfar"):
        wy.far()
    wz.start()
    with scope("soft67"):
        soft(6, 7)
    with scope("qnear"):
        qrow.near()
    with scope("xnear1"):
        xring.near(1)
    sp_peers(lambda s: cot_part(s, sp, s).start())
    with scope("columns"):
        all_of(xc.at[0, pl.ds(0, 3)], zr)
    cring.start()
    with scope("soft78"):
        soft(7, 8)
    with scope("wznear"):
        wz.near()
    with scope("qfar"):
        qrow.far()
    with scope("qall"):
        qrow.arrived()
    with scope("xfar"):
        xring.far()

    def v_part(zz, src, to):
        return remote(v4.at[to], vn.at[pl.ds(2 * src, 2)], vs.at[0], vr.at[src], zz * 4 + y, dp)

    with scope("values"):
        for n in (0, 1):
            v = nn(xr[...].reshape(512, 2048), wq[:, :, :, n * 256:(n + 1) * 256].reshape(2048, 256)).astype(BF)
            for m in (0, 1):
                t = 2 * n + m
                v4[t] = v[:, m * 128:(m + 1) * 128].reshape(2, B, 128)

                @pl.when(t != z)
                def _():
                    v_part(t, z, t).start()
        vn[pl.ds(2 * z, 2)] = v4[z]
    with scope("wzfar"):
        wz.far()
    wrow.start()

    def mixed(r):
        def one(e, c):
            j = 2 * r + e
            v = vn[j].T
            vt[j] = v

            def add(i, count):
                for m in range(count):
                    t = tri(i + m, j)
                    ot[i + m] += nn(v, aa[t])
                    o2t[i + m] += nn(v, p2[t])
            paired(j, NB - j, add)
            return c
        lax.fori_loop(0, 2, one, 0)

    with scope("mix0"):
        mixed(z)
    for d in (1, 3):
        t = lax.rem(z + d, 4)
        with scope("v%d" % d):
            v_part(t, t, z).wait_recv()
        with scope("mix%d" % d):
            mixed(t)
    t = lax.rem(z + 2, 4)
    with scope("v2"):
        v_part(t, t, z).wait_recv()
    with scope("mix2"):
        mixed(t)
    with scope("cot"):
        loads[4].wait()
        all_of(cota.at[pl.ds(0, 1920)], cr)

    def mix(i, total):
        o, o2 = ot[i], o2t[i]
        g = cota[rows(i), :].astype(F32).T
        r = lax.rsqrt(jnp.mean(o * o, axis=0, keepdims=True) + EPS)
        yy = r * o
        d = (r * (g - yy * jnp.mean(g * yy, axis=0, keepdims=True))).astype(BF)
        dw = d.astype(F32)
        d2 = jnp.sum(dw * o2, axis=0, keepdims=True)
        d1 = jnp.sum(dw * o, axis=0, keepdims=True) + lam * d2
        dot[i] = d
        do[i] = dw.T.astype(BF)
        delta[i, 0:1, :] = d1
        delta[i, 1:2, :] = d2
        return total + d2
    with scope("mix"):
        total = lax.fori_loop(0, NB, mix, jnp.zeros((1, B), F32))
    glb[...] = jnp.broadcast_to(-jnp.sum(total, axis=1, keepdims=True), (8, 128))

    half = lax.broadcasted_iota(jnp.int32, (1, 128), 1) < 64
    ks = jnp.where(half, SCALE, -lam * SCALE)

    def gl_part(d, src, to):
        return remote(glb, glin.at[src], ls.at[0], lr.at[0], sp, d)

    def dv_part(yy, src, to, h):
        part = rows(lax.rem(to, 2), 128)
        return remote(dvg.at[h, 2 * z + lax.div(to, 2), part], dvin.at[h, src], ds_.at[0], dr.at[0], z * 4 + yy, dp)

    def y_peers(body):
        for d in (1, 3, 2):
            body(lax.rem(y + d, 4))

    def gw_part(d, src, to, h):
        return remote(gwp.at[h, to], gwin.at[h, src], es.at[0], er.at[0], sp, d)

    def send_head(o, weights):
        h = lax.rem(z + o, 4)
        if weights:
            for n in range(4):
                gwp[h, :, n] = gwt[h, :, n * 128:(n + 1) * 128].T.astype(BF).reshape(8, 16, 128)
            dp_peers(lambda d: gw_part(d, dp, d, h).start())
        else:
            y_peers(lambda t: dv_part(t, y, t, h).start())

    def dv_ring(j):
        return Ring(lambda i, part: dvg.at[i, j] if part is None else dvg.at[i, j, pl.ds(128 * part, 128)],
                    lambda n: gs.at[0], lambda n: gr.at[j, n], sp, dp, 1)

    def main(n, c):
        j = NB - 1 - n
        dv, dk1, dk2 = keys_block(j, vn, qz1, qz2, kt, p1, p2, aa, dot, do, delta, dqt)
        dvg[z, j] = dv.astype(BF)
        gkb[rows(j), :] = ((dk1 + dk2) * ks).astype(BF)
        dv_ring(j).start()

        @pl.when(n >= 5)
        def _():
            dv_ring(j + 5).near()

        @pl.when(n == 5)
        def _():
            cring.near()
        return c
    with scope("main"):
        lax.fori_loop(0, NB, main, 0)
    with scope("wrownear"):
        wrow.near()
    save_k = pltpu.make_async_copy(gkb, gk_h, save.at[0])
    save_k.start()

    def fin(i, c):
        gqb[rows(i), :] = (dqt[i].T * ks).astype(BF)
        return c
    with scope("fin"):
        lax.fori_loop(0, NB, fin, 0)
    save_q = pltpu.make_async_copy(gqb, gq_h, save.at[1])
    save_q.start()
    gwt[...] = jnp.zeros_like(gwt)

    def weight_part(h, j):
        jz, jy = lax.div(j, 2), lax.rem(j, 2)
        cols = xc[pl.ds(2 * jy, 2), jz].reshape(B, 512)
        gwt[h] += nn(dvg[h, j].T, cols)

    def pieces(lo, hi, offsets):
        def one(j, c):
            for o in offsets:
                weight_part(lax.rem(z + o, 4), j)
            return c
        lax.fori_loop(lo, hi, one, 0)

    with scope("cfar"):
        cring.far()
    send_head(0, False)
    with scope("pieces0"):
        pieces(0, 8, (0,))
        send_head(0, True)
    with scope("pieces13"):
        pieces(5, 8, (1, 3))

    def late(n, c):
        j = 4 - n
        dv_ring(j).near()
        weight_part(lax.rem(z + 1, 4), j)
        weight_part(lax.rem(z + 3, 4), j)
        return c
    with scope("late"):
        lax.fori_loop(0, 5, late, 0)
        for o in (1, 3):
            send_head(o, False)
        for o in (1, 3):
            send_head(o, True)

    def distant(n, c):
        dv_ring(7 - n).far()
        weight_part(lax.rem(z + 2, 4), 7 - n)
        return c
    with scope("distant"):
        lax.fori_loop(0, 8, distant, 0)
    send_head(2, False)
    send_head(2, True)
    dp_peers(lambda d: gl_part(d, dp, d).start())
    glin[dp] = glb[...]
    for h in range(4):
        gwin[h, dp] = gwp[h, dp]
        dvin[h, y] = dvg[h, 2 * z + lax.div(y, 2), rows(lax.rem(y, 2), 128), :]
    with scope("wrowfar"):
        wrow.far()
    with scope("dvwait"):
        all_of(dvin.at[pl.ds(0, 3)], dr)
    for b in range(4):
        for a in range(4):
            dvrow[:, (4 * b + a) * 128:(4 * b + a + 1) * 128] = dvin[b, a]
    with scope("gwwait"):
        all_of(gwin.at[:, pl.ds(0, 7)], er)
    for h in range(4):
        acc = gwin[h, 0].astype(F32)
        for d in range(1, 8):
            acc = acc + gwin[h, d].astype(F32)
        gws[:, h] = acc.astype(BF)

    def fin_part(yy, src, to):
        return remote(gws.at[to], gwf.at[src], fs.at[0], fr.at[0], z * 4 + yy, dp)
    y_peers(lambda t: fin_part(t, y, t).start())
    gwf[y] = gws[y]
    all_of(glin.at[pl.ds(0, 7)], lr)
    tot = glin[0]
    for d in range(1, 8):
        tot = tot + glin[d]
    delta[0] = jnp.concatenate([tot, tot], axis=1)
    save_l = pltpu.make_async_copy(delta.at[0, :, pl.ds(0, 128)], gl_h, save.at[3])
    save_l.start()
    with scope("wrowall"):
        wrow.arrived()

    def tokens_grad(n, c):
        g = nt(dvrow[...], w[pl.ds(2 * n, 2)].reshape(B, 2048))
        gtb[:, rows(n)] = g.astype(BF)
        return c
    with scope("tgrad"):
        lax.fori_loop(0, NB, tokens_grad, 0)
    save_t = pltpu.make_async_copy(gtb, gt_h, save.at[2])
    save_t.start()
    with scope("finwait"):
        all_of(gwf.at[pl.ds(0, 3)], fr)
    for a in range(4):
        for b in range(4):
            gwo[:, (4 * b + a) * 128:(4 * b + a + 1) * 128] = gwf[a, b].astype(F32)
    save_w = pltpu.make_async_copy(gwo, gw_h, save.at[4])
    save_w.start()
    xring.drain()
    cring.drain()
    wy.drain()
    wz.drain()
    wrow.drain()
    qrow.drain()
    all_of(dvg.at[pl.ds(0, 3)], gs)
    all_of(wq.at[pl.ds(0, 15), 0], h1s)
    all_of(cota.at[pl.ds(0, 1920)], cs)
    all_of(dvin.at[pl.ds(0, 3)], ds_)
    all_of(gwin.at[:, pl.ds(0, 7)], es)
    all_of(xc.at[0, pl.ds(0, 3)], zs)
    all_of(v4.at[pl.ds(0, 3)], vs)
    all_of(glin.at[pl.ds(0, 7)], ls)
    all_of(gwf.at[pl.ds(0, 3)], fs)
    with scope("savewait"):
        for a in (save_k, save_q, save_t, save_l, save_w):
            a.wait()


def hand_out(*refs):
    came, outs, held, (got, put) = refs[:5], refs[5:10], refs[10:15], refs[15:]
    loads = [pltpu.make_async_copy(came[n], held[n], got.at[n]) for n in range(5)]
    saves = [pltpu.make_async_copy(held[n], outs[n], put.at[n]) for n in range(4)]
    for a in loads:
        a.start()
    for n in range(4):
        loads[n].wait()
        saves[n].start()
    loads[4].wait()
    outs[4][0] = held[4][0, 0]
    for a in saves:
        a.wait()


def body(tokens, cotangent, value_weight, query_heads, key_heads, lambdas):
    L = query_heads.shape[1]
    smem = pl.BlockSpec(memory_space=pltpu.SMEM)
    anywhere = pl.BlockSpec(memory_space=pl.ANY)
    hbm = pl.BlockSpec(memory_space=pltpu.HBM)
    tiles = (NB * (NB + 1) // 2, B, B)
    dma = lambda *n: pltpu.SemaphoreType.DMA(n)
    gq, gk, gt, gw, gl = pl.pallas_call(
        kernel,
        out_shape=(S((L, 128), BF), S((L, 128), BF), S((128, 2048), BF), S((16, 2048), F32), S((8, 128), F32)),
        in_specs=[smem] + [anywhere] * 5, out_specs=[anywhere] * 5,
        scratch_shapes=[
            V((4, 128, 2048), BF), V((4, 4, 128, 512), BF), V((16, 8, 16, 2048), BF), V((4, 16, 512), BF), V((16, 8, 16, 512), BF),
            V((L, 128), BF), V((L, 128), BF), V((L, 128), BF),
            V((NB, B, 128), BF), V((NB, B, 128), BF), V((NB, 128, B), BF), V((NB, 128, B), BF), V((NB, B, 128), BF), V((4, 2, B, 128), BF),
            V((NB, B, B), F32), V((NB, B, B), F32), V(tiles, BF), V(tiles, BF), V(tiles, BF),
            V((NB, 128, B), BF), V((NB, B, 128), BF), V((NB, 8, B), F32), V((NB, 128, B), F32), V((NB, 128, B), F32), V((NB, 128, B), F32),
            V((4, NB, B, 128), BF), V((4, 4, 128, 128), BF), V((128, 2048), BF), V((4, 128, 512), F32), V((4, 8, 4, 16, 128), BF), V((4, 8, 4, 16, 128), BF),
            V((4, 4, 16, 128), BF), V((4, 4, 16, 128), BF), V((L, 128), BF), V((L, 128), BF), V((128, 2048), BF), V((16, 2048), F32),
            V((8, 128), F32), V((8, 8, 128), F32),
            dma(5), dma(1), dma(5), dma(6), dma(6), dma(4), dma(4), dma(1), dma(1), dma(2, 4), dma(2, 4), dma(8), dma(8), dma(8), dma(8), dma(1), dma(1), dma(1), dma(1), dma(1), dma(4), dma(1), dma(8, 4), dma(1), dma(1), dma(1), dma(1), dma(1), dma(1), dma(1), dma(1)],
        compiler_params=pltpu.CompilerParams(vmem_limit_bytes=60 * 1024 * 1024, collective_id=0, has_side_effects=True),
        name="whole")(lambdas, tokens[0], cotangent[0], value_weight, query_heads.reshape(L, 128), key_heads.reshape(L, 128))
    gq, gk, gt, gw, gl = pl.pallas_call(
        hand_out,
        out_shape=(S((L, 128), BF), S((L, 128), BF), S((128, 2048), BF), S((16, 2048), F32), S((1,), F32)),
        in_specs=[hbm] * 5, out_specs=[hbm] * 4 + [smem],
        scratch_shapes=[V((L, 128), BF), V((L, 128), BF), V((128, 2048), BF), V((16, 2048), F32), pltpu.SMEM((8, 128), F32), dma(5), dma(4)],
        compiler_params=pltpu.CompilerParams(vmem_limit_bytes=60 * 1024 * 1024),
        name="hand_out")(gq, gk, gt, gw, gl)
    return gq.reshape(query_heads.shape), gk.reshape(key_heads.shape), gt[None], gw, gl


def solution(mesh):
    placed = (P("dp", "sp", None), P("dp", "sp", None), P(("sp", "dp"), None),
              P("dp", None, "sp", None), P("dp", None, "sp", None), P("sp"))
    outs = (P("dp", None, "sp", None), P("dp", None, "sp", None), P("dp", "sp", None), P(("sp", "dp"), None), P("sp"))
    return jax.shard_map(body, mesh=mesh, in_specs=placed, out_specs=outs, check_vma=False)
```

```python
import functools, math
import jax, jax.numpy as jnp
from jax import lax
from jax.experimental import pallas as pl
from jax.experimental.pallas import tpu as pltpu
from jax.sharding import PartitionSpec as P

EPS = 1e-6
B = 256
NB = 8
SCALE = 0.125
LOG2E = 1.4426950408889634
F32 = jnp.float32
BF = jnp.bfloat16

def nt(a, b):
    return lax.dot_general(a, b, (((1,), (1,)), ((), ())), preferred_element_type=F32)

def nn(a, b):
    return lax.dot_general(a, b, (((1,), (0,)), ((), ())), preferred_element_type=F32)

def tri(i, j):
    return (i * (i + 1)) // 2 + j

def paired(lo, n, body):
    def two(p, c):
        body(lo + 2 * p, 2)
        return c
    lax.fori_loop(0, n // 2, two, 0)
    def one(p, c):
        body(lo + n - 1, 1)
        return c
    lax.fori_loop(0, n % 2, one, 0)

def prepare(i, q_ref, k_ref, qz1, qz2, kt):
    rows = pl.ds(pl.multiple_of(i * B, B), B)
    q = q_ref[rows, :]
    first = lax.broadcasted_iota(jnp.int32, (B, 128), 1) < 64
    zero = jnp.zeros_like(q)
    qz1[i] = jnp.where(first, q, zero)
    qz2[i] = jnp.where(first, zero, q)
    kt[i] = k_ref[rows, :].T

def softmaxes(i, lam, k_ref, qz1, qz2, s1, s2, p1, p2, aa):
    q1, q2 = qz1[i], qz2[i]

    def score(j, m):
        k = k_ref[pl.ds(pl.multiple_of(j * B, B), B), :]
        a, b = nt(k, q1), nt(k, q2)
        return a, b

    def keep(j, a, b, m):
        s1[j] = a
        s2[j] = b
        return (jnp.maximum(m[0], jnp.max(a.reshape(B // 8, 8, B), axis=0)),
                jnp.maximum(m[1], jnp.max(b.reshape(B // 8, 8, B), axis=0)))

    a, b = score(i, None)
    seen = lax.broadcasted_iota(jnp.int32, (B, B), 0) <= lax.broadcasted_iota(jnp.int32, (B, B), 1)
    a = jnp.where(seen, a, -1e30)
    b = jnp.where(seen, b, -1e30)
    low = jnp.full((8, B), -1e30, F32)
    m = keep(i, a, b, (low, low))

    def off(j, m):
        a, b = score(j, m)
        return keep(j, a, b, m)
    def two(p, m):
        a, b = score(2 * p, m)
        c, d = score(2 * p + 1, m)
        m = keep(2 * p, a, b, m)
        return keep(2 * p + 1, c, d, m)
    m = lax.fori_loop(0, i // 2, two, m)
    m = lax.fori_loop(i - i % 2, i, off, m)
    m1 = jnp.max(m[0], axis=0, keepdims=True)
    m2 = jnp.max(m[1], axis=0, keepdims=True)
    c = SCALE * LOG2E

    def power(j, l):
        e1 = jnp.exp2((s1[j] - m1) * c)
        e2 = jnp.exp2((s2[j] - m2) * c)
        s1[j] = e1
        s2[j] = e2
        return (l[0] + jnp.sum(e1.reshape(B // 8, 8, B), axis=0),
                l[1] + jnp.sum(e2.reshape(B // 8, 8, B), axis=0))
    l = lax.fori_loop(0, i + 1, power, (jnp.zeros((8, B), F32), jnp.zeros((8, B), F32)))
    r1 = 1.0 / jnp.sum(l[0], axis=0, keepdims=True)
    r2 = 1.0 / jnp.sum(l[1], axis=0, keepdims=True)

    def norm(j, _):
        x1 = s1[j] * r1
        x2 = s2[j] * r2
        t = tri(i, j)
        p1[t] = x1.astype(BF)
        p2[t] = x2.astype(BF)
        aa[t] = (x1 - lam * x2).astype(BF)
        return _
    lax.fori_loop(0, i + 1, norm, 0)

def keys_block(j, vn, qz1, qz2, kt, p1, p2, aa, dot, do, delta, dqt):
    v = vn[j]
    k1t, k2t = kt[j, 0:64, :], kt[j, 64:128, :]

    def parts(i):
        t = tri(i, j)
        da = nn(v, dot[i])
        x1 = (p1[t].astype(F32) * (da - delta[i, 0:1, :])).astype(BF)
        x2 = (p2[t].astype(F32) * (da - delta[i, 1:2, :])).astype(BF)
        dv = nn(aa[t], do[i])
        dk1 = nn(x1, qz1[i])
        dk2 = nn(x2, qz2[i])
        dqt[i, 0:64, :] += nn(k1t, x1)
        dqt[i, 64:128, :] += nn(k2t, x2)
        return dv, dk1 , dk2

    def two(p, c):
        a = parts(j + 2 * p)
        b = parts(j + 2 * p + 1)
        return tuple(x + (y + z) for x, y, z in zip(c, a, b))
    def one(p, c):
        a = parts(p)
        return tuple(x + y for x, y in zip(c, a))
    n = NB - j
    zero = jnp.zeros((B, 128), F32)
    c = lax.fori_loop(0, n // 2, two, (zero, zero, zero))
    c = lax.fori_loop(NB - n % 2, NB, one, c)
    return c[0], c[1], c[2]


MESH = pl.DeviceIdType.MESH
V = pltpu.VMEM
S = jax.ShapeDtypeStruct


class Ring:
    def __init__(self, at, ss, rs, me, to):
        self.at, self.ss, self.rs, self.me, self.to = at, ss, rs, me, to

    def index(self, o):
        return lax.rem(self.me + (o + 4), 4)

    def copy(self, o, part, delta, sem):
        s, d = self.to(self.index(delta))
        ref = self.at(self.index(o), part)
        return pltpu.make_async_remote_copy(
            src_ref=ref, dst_ref=ref, send_sem=self.ss, recv_sem=self.rs(sem),
            device_id={"sp": s, "dp": d}, device_id_type=MESH)

    def start(self):
        self.copy(0, 0, 1, 0).start()
        self.copy(0, 1, -1, 1).start()
        self.copy(0, 1, 1, 2).start()
        self.copy(0, 0, -1, 2).start()

    def near(self):
        self.copy(-1, 0, 1, 0).wait_recv()
        self.copy(-1, 0, 1, 3).start()
        self.copy(1, 1, -1, 1).wait_recv()
        self.copy(1, 1, -1, 3).start()

    def both(self, o, sem):
        ref = self.at(self.index(o), None)
        pltpu.make_async_copy(ref, ref, self.rs(sem)).wait()

    def full(self):
        self.both(1, 2)

    def far(self):
        self.both(2, 3)


def kernel(lam_h, tok_h, cot_h, w_h, q_h, k_h, gq_h, gk_h, gt_h, gw_h, gl_h,
           xr, xc, w, wo, wq, cota, q_ref, k_ref, qz1, qz2, kt, vt, vn, v4, s1, s2, p1, p2, aa, dot, do, delta, dqt, ot, o2t,
           dvg, dvin, dvrow, gta, gwt, gwp, gwin, gws, gwf, gqb, gkb, gtb, gwo, glb, glin,
           lam_ref, load, wload, save, xs, xr_, ys, yr, zs, zr, ws, wr, rs_, rr, qs, qr, h1s, h1r, cs, cr, vs, vr, gs, gr, ds_, dr,
           es, er, ls, lr, fs, fr, wds, wdr, qds, qdr):
    sp, dp = lax.axis_index("sp"), lax.axis_index("dp")
    y, z = lax.rem(sp, 4), lax.div(sp, 4)
    scope = jax.named_scope

    def sp_peers(body):
        lax.fori_loop(1, 16, lambda d, c: (body(lax.rem(sp + d, 16)), c)[1], 0)

    def dp_peers(body):
        lax.fori_loop(1, 8, lambda d, c: (body(lax.rem(dp + d, 8)), c)[1], 0)

    def remote(src, dst, ss, rs, s, d):
        return pltpu.make_async_remote_copy(src_ref=src, dst_ref=dst, send_sem=ss, recv_sem=rs,
                                            device_id={"sp": s, "dp": d}, device_id_type=MESH)

    def all_of(ref, sem):
        pltpu.make_async_copy(ref, ref, sem.at[0]).wait()

    def lanes(h, n=128):
        return pl.ds(pl.multiple_of(h * n, n), n)

    def rows(i, n=B):
        return pl.ds(pl.multiple_of(i * n, n), n)

    barrier = pltpu.get_barrier_semaphore()
    sp_peers(lambda s: pl.semaphore_signal(barrier, inc=1, device_id={"sp": s, "dp": dp}, device_id_type=MESH))
    dp_peers(lambda d: pl.semaphore_signal(barrier, inc=1, device_id={"sp": sp, "dp": d}, device_id_type=MESH))
    loads = [pltpu.make_async_copy(a, b, load.at[n]) for n, (a, b) in enumerate((
        (w_h, w.at[sp, dp]), (tok_h, xr.at[y]), (q_h, q_ref), (k_h, k_ref), (cot_h.at[:, lanes(sp)], cota.at[rows(sp, 128)]), (lam_h, lam_ref)))]
    for a in loads:
        a.start()
    parts = [pltpu.make_async_copy(w_h.at[:, pl.ds((4 * b + a) * 128, 128)], wo.at[a, :, pl.ds(b * 128, 128)], wload.at[0])
             for a in range(4) for b in range(4)]
    for a in parts:
        a.start()

    x_, core = lax.div(dp, 2), lax.rem(dp, 2)
    along_y = lambda i: (z * 4 + i, dp)
    along_z = lambda i: (i * 4 + y, dp)
    along_x = lambda i: (sp, 2 * i + core)

    def split(ref, view, n):
        return lambda i, part: view(i, pl.ds(0, n) if part is None else pl.ds(n // 2 * part, n // 2))

    wy = Ring(lambda i, part: w.at[z * 4 + i, dp] if part is None else w.at[z * 4 + i, dp, :, pl.ds(1024 * part, 1024)],
              ws.at[0], lambda n: wr.at[0, n], y, along_y)
    wz = Ring(lambda i, part: w.at[pl.ds(4 * i, 4), dp] if part is None else w.at[pl.ds(4 * i + 2 * part, 2), dp],
              ws.at[1], lambda n: wr.at[1, n], z, along_z)
    xring = Ring(split(xr, lambda i, d: xr.at[i, d], 128), xs.at[0], lambda n: xr_.at[n], y, along_y)
    cring = Ring(split(xc, lambda i, d: xc.at[i, d], 4), ys.at[0], lambda n: yr.at[n], y, along_y)
    wrow = Ring(split(w, lambda i, d: w.at[d, 2 * i + core], 16), rs_.at[0], lambda n: rr.at[n], x_, along_x)
    qrow = Ring(split(wq, lambda i, d: wq.at[d, 2 * i + core], 16), qs.at[0], lambda n: qr.at[n], x_, along_x)

    def other(ref, ring, o, ss, rs):
        d = 2 * ring.index(o) + core
        return remote(ref.at[:, d], ref.at[:, d], ss.at[0], rs.at[0], sp, dp + 1 - 2 * core)

    for a in loads[:2]:
        a.wait()
    all_of(wo, wload)
    wq[sp, dp] = wo[y]
    xc[y, z] = xr[y, :, lanes(z, 512)]
    with scope("barrier"):
        pl.semaphore_wait(barrier, 22)

    def head_rows(s, src, to):
        return remote(wo.at[lax.rem(to, 4)], wq.at[src, dp], h1s.at[0], h1r.at[0], s, dp)

    def columns(zz, src, to):
        return remote(xr.at[y, :, lanes(to, 512)], xc.at[y, src], zs.at[0], zr.at[0], zz * 4 + y, dp)

    def z_peers(body):
        for d in (1, 3, 2):
            body(lax.rem(z + d, 4))

    wy.start()
    sp_peers(lambda s: head_rows(s, sp, s).start())
    z_peers(lambda t: columns(t, z, t).start())
    def cot_part(s, src, to):
        return remote(cot_h.at[:, lanes(to)], cota.at[rows(src, 128)], cs.at[0], cr.at[0], s, dp)

    for n in (2, 3, 5):
        loads[n].wait()
    lam = lam_ref[0]

    def prep(i, c):
        prepare(i, q_ref, k_ref, qz1, qz2, kt)
        zero = jnp.zeros((128, B), F32)
        dqt[i] = zero
        ot[i] = zero
        o2t[i] = zero
        return c
    lax.fori_loop(0, NB, prep, 0)

    def soft(lo, hi):
        lax.fori_loop(lo, hi, lambda i, c: (softmaxes(i, lam, k_ref, qz1, qz2, s1, s2, p1, p2, aa), c)[1], 0)

    with scope("soft03"):
        soft(0, 3)
    with scope("wynear"):
        wy.near()
    xring.start()
    with scope("heads"):
        all_of(wq.at[pl.ds(0, 15), 0], h1r)
    qrow.start()
    other(wq, qrow, 0, qds, qdr).start()
    with scope("soft34"):
        soft(3, 4)
    with scope("wyfar"):
        wy.full()
        wy.far()
    wz.start()
    with scope("soft46"):
        soft(4, 6)
    with scope("xnear0"):
        xring.near()
    with scope("soft67"):
        soft(6, 7)
    with scope("qnear"):
        qrow.near()
        qrow.full()
        for o in (-1, 1):
            other(wq, qrow, o, qds, qdr).start()
    with scope("wznear"):
        wz.near()
    with scope("xfull"):
        xring.full()
    sp_peers(lambda s: cot_part(s, sp, s).start())
    with scope("columns"):
        all_of(xc.at[0, pl.ds(0, 3)], zr)
    cring.start()
    with scope("soft78"):
        soft(7, 8)
    with scope("wzfar"):
        wz.full()
        wz.far()
    wrow.start()
    other(w, wrow, 0, wds, wdr).start()
    with scope("qfar"):
        qrow.far()
        other(wq, qrow, 2, qds, qdr).start()
    with scope("qall"):
        all_of(wq.at[:, pl.ds(0, 4)], qdr)
    with scope("xfar"):
        xring.far()

    def v_part(zz, src, to):
        return remote(v4.at[to], vn.at[pl.ds(2 * src, 2)], vs.at[0], vr.at[src], zz * 4 + y, dp)

    with scope("values"):
        for n in (0, 1):
            v = nn(xr[...].reshape(512, 2048), wq[:, :, :, n * 256:(n + 1) * 256].reshape(2048, 256)).astype(BF)
            for m in (0, 1):
                t = 2 * n + m
                v4[t] = v[:, m * 128:(m + 1) * 128].reshape(2, B, 128)

                @pl.when(t != z)
                def _():
                    v_part(t, z, t).start()
        vn[pl.ds(2 * z, 2)] = v4[z]

    def mixed(r):
        def one(e, c):
            j = 2 * r + e
            v = vn[j].T
            vt[j] = v

            def add(i, count):
                for m in range(count):
                    t = tri(i + m, j)
                    ot[i + m] += nn(v, aa[t])
                    o2t[i + m] += nn(v, p2[t])
            paired(j, NB - j, add)
            return c
        lax.fori_loop(0, 2, one, 0)

    with scope("mix0"):
        mixed(z)
    for d in (1, 3):
        t = lax.rem(z + d, 4)
        with scope("v%d" % d):
            v_part(t, t, z).wait_recv()
        with scope("mix%d" % d):
            mixed(t)
    t = lax.rem(z + 2, 4)
    with scope("v2"):
        v_part(t, t, z).wait_recv()
    with scope("mix2"):
        mixed(t)
    with scope("cot"):
        loads[4].wait()
        all_of(cota.at[pl.ds(0, 1920)], cr)

    def mix(i, total):
        o, o2 = ot[i], o2t[i]
        g = cota[rows(i), :].astype(F32).T
        r = lax.rsqrt(jnp.mean(o * o, axis=0, keepdims=True) + EPS)
        yy = r * o
        d = (r * (g - yy * jnp.mean(g * yy, axis=0, keepdims=True))).astype(BF)
        dw = d.astype(F32)
        d2 = jnp.sum(dw * o2, axis=0, keepdims=True)
        d1 = jnp.sum(dw * o, axis=0, keepdims=True) + lam * d2
        dot[i] = d
        do[i] = dw.T.astype(BF)
        delta[i, 0:1, :] = d1
        delta[i, 1:2, :] = d2
        return total + d2
    with scope("mix"):
        total = lax.fori_loop(0, NB, mix, jnp.zeros((1, B), F32))
    glb[...] = jnp.broadcast_to(-jnp.sum(total, axis=1, keepdims=True), (8, 128))

    half = lax.broadcasted_iota(jnp.int32, (1, 128), 1) < 64
    ks = jnp.where(half, SCALE, -lam * SCALE)

    def gl_part(d, src, to):
        return remote(glb, glin.at[src], ls.at[0], lr.at[0], sp, d)

    def dv_part(yy, src, to, h):
        part = rows(lax.rem(to, 2), 128)
        return remote(dvg.at[h, 2 * z + lax.div(to, 2), part], dvin.at[h, src], ds_.at[0], dr.at[h], z * 4 + yy, dp)

    def y_peers(body):
        for d in (1, 3, 2):
            body(lax.rem(y + d, 4))

    def gw_part(d, src, to, h):
        return remote(gwp.at[h, to], gwin.at[h, src], es.at[0], er.at[0], sp, d)

    def send_head(o, weights):
        h = lax.rem(z + o, 4)
        if weights:
            for n in range(4):
                gwp[h, :, n] = gwt[h, :, n * 128:(n + 1) * 128].T.astype(BF).reshape(8, 16, 128)
            dp_peers(lambda d: gw_part(d, dp, d, h).start())
        else:
            y_peers(lambda t: dv_part(t, y, t, h).start())

    def dv_ring(j):
        return Ring(lambda i, part: dvg.at[i, j] if part is None else dvg.at[i, j, pl.ds(128 * part, 128)],
                    gs.at[0], lambda n: gr.at[j, n], z, along_z)

    def main(n, c):
        j = NB - 1 - n
        dv, dk1, dk2 = keys_block(j, vn, qz1, qz2, kt, p1, p2, aa, dot, do, delta, dqt)
        dvg[z, j] = dv.astype(BF)
        dv_ring(j).start()
        gkb[rows(j), :] = ((dk1 + dk2) * ks).astype(BF)

        @pl.when(n == 2)
        def _():
            wrow.near()

        @pl.when(n == 4)
        def _():
            cring.near()
            dv_ring(7).near()

        @pl.when(n == 5)
        def _():
            dv_ring(6).near()

        @pl.when(n == 6)
        def _():
            dv_ring(5).near()

        @pl.when(n == 7)
        def _():
            dv_ring(4).near()
            wrow.full()
            for o in (-1, 1):
                other(w, wrow, o, wds, wdr).start()
        return c
    with scope("main"):
        lax.fori_loop(0, NB, main, 0)
    send_head(0, False)
    save_k = pltpu.make_async_copy(gkb, gk_h, save.at[0])
    save_k.start()

    def fin(i, c):
        gqb[rows(i), :] = (dqt[i].T * ks).astype(BF)
        return c
    with scope("fin"):
        lax.fori_loop(0, NB, fin, 0)
    save_q = pltpu.make_async_copy(gqb, gq_h, save.at[1])
    save_q.start()
    gwt[...] = jnp.zeros_like(gwt)

    def weight_part(h, j):
        jz, jy = lax.div(j, 2), lax.rem(j, 2)
        cols = xc[pl.ds(2 * jy, 2), jz].reshape(B, 512)
        gwt[h] += nn(dvg[h, j].T, cols)

    def pieces(lo, hi, offsets):
        def one(j, c):
            for o in offsets:
                weight_part(lax.rem(z + o, 4), j)
            return c
        lax.fori_loop(lo, hi, one, 0)

    with scope("near3"):
        dv_ring(3).near()
    with scope("cfar"):
        cring.full()
        cring.far()
    with scope("pieces0"):
        pieces(0, 8, (0,))
        send_head(0, True)
    with scope("near2"):
        dv_ring(2).near()
    with scope("near1"):
        dv_ring(1).near()

    def neighbours(lo, hi):
        def one(n, c):
            j = hi - 1 - n
            dv_ring(j).full()
            weight_part(lax.rem(z + 1, 4), j)
            weight_part(lax.rem(z + 3, 4), j)
            return c
        lax.fori_loop(0, hi - lo, one, 0)
    with scope("pieces13"):
        neighbours(2, 8)
    with scope("near0"):
        dv_ring(0).near()
    with scope("pieces01"):
        neighbours(0, 2)
    for o in (1, 3):
        send_head(o, False)
    for o in (1, 3):
        send_head(o, True)

    def gather(o):
        h = lax.rem(z + o, 4)
        dvin[h, y] = dvg[h, 2 * z + lax.div(y, 2), rows(lax.rem(y, 2), 128), :]
        pltpu.make_async_copy(dvin.at[h, pl.ds(0, 3)], dvin.at[h, pl.ds(0, 3)], dr.at[h]).wait()
        for a in range(4):
            dvrow[h, :, a * 128:(a + 1) * 128] = dvin[h, a]

    def times_rows(n, o):
        h = lax.rem(z + o, 4)
        return nt(dvrow[h], w[pl.ds(2 * n, 2), :, :, lanes(h, 512)].reshape(B, 512))

    with scope("wrowfar"):
        wrow.far()
        other(w, wrow, 2, wds, wdr).start()
    with scope("far"):
        lax.fori_loop(0, NB, lambda n, c: (dv_ring(7 - n).far(), c)[1], 0)
    send_head(2, False)
    with scope("distant"):
        pieces(0, 8, (2,))
    send_head(2, True)
    dp_peers(lambda d: gl_part(d, dp, d).start())
    glin[dp] = glb[...]
    for h in range(4):
        gwin[h, dp] = gwp[h, dp]
    with scope("gather"):
        for o in (0, 1, 3):
            gather(o)
    with scope("wrowall"):
        all_of(w.at[:, pl.ds(0, 4)], wdr)

    def most(n, c):
        gta[:, rows(n)] = times_rows(n, 0) + times_rows(n, 1) + times_rows(n, 3)
        return c
    with scope("tgrada"):
        lax.fori_loop(0, NB, most, 0)
    with scope("gwwait"):
        all_of(gwin.at[:, pl.ds(0, 7)], er)
    for h in range(4):
        acc = gwin[h, 0].astype(F32)
        for d in range(1, 8):
            acc = acc + gwin[h, d].astype(F32)
        gws[:, h] = acc.astype(BF)

    def fin_part(yy, src, to):
        return remote(gws.at[to], gwf.at[src], fs.at[0], fr.at[0], z * 4 + yy, dp)
    y_peers(lambda t: fin_part(t, y, t).start())
    gwf[y] = gws[y]
    all_of(glin.at[pl.ds(0, 7)], lr)
    tot = glin[0]
    for d in range(1, 8):
        tot = tot + glin[d]
    delta[0] = jnp.concatenate([tot, tot], axis=1)
    save_l = pltpu.make_async_copy(delta.at[0, :, pl.ds(0, 128)], gl_h, save.at[3])
    save_l.start()
    with scope("dvwait"):
        gather(2)

    def tokens_grad(n, c):
        gtb[:, rows(n)] = (gta[:, rows(n)] + times_rows(n, 2)).astype(BF)
        return c
    with scope("tgradb"):
        lax.fori_loop(0, NB, tokens_grad, 0)
    save_t = pltpu.make_async_copy(gtb, gt_h, save.at[2])
    save_t.start()
    with scope("finwait"):
        all_of(gwf.at[pl.ds(0, 3)], fr)
    for a in range(4):
        for b in range(4):
            gwo[:, (4 * b + a) * 128:(4 * b + a + 1) * 128] = gwf[a, b].astype(F32)
    save_w = pltpu.make_async_copy(gwo, gw_h, save.at[4])
    save_w.start()
    all_of(xr.at[pl.ds(0, 3)], xs)
    all_of(xc.at[pl.ds(0, 3)], ys)
    all_of(w.at[pl.ds(0, 3), 0], ws)
    pltpu.make_async_copy(w.at[pl.ds(0, 12), 0], w.at[pl.ds(0, 12), 0], ws.at[1]).wait()
    all_of(w.at[:, pl.ds(0, 3)], rs_)
    all_of(wq.at[:, pl.ds(0, 3)], qs)
    all_of(w.at[:, pl.ds(0, 4)], wds)
    all_of(wq.at[:, pl.ds(0, 4)], qds)
    all_of(dvg.at[pl.ds(0, 3)], gs)
    all_of(wq.at[pl.ds(0, 15), 0], h1s)
    all_of(cota.at[pl.ds(0, 1920)], cs)
    all_of(dvin.at[pl.ds(0, 3)], ds_)
    all_of(gwin.at[:, pl.ds(0, 7)], es)
    all_of(xc.at[0, pl.ds(0, 3)], zs)
    all_of(v4.at[pl.ds(0, 3)], vs)
    all_of(glin.at[pl.ds(0, 7)], ls)
    all_of(gwf.at[pl.ds(0, 3)], fs)
    with scope("savewait"):
        for a in (save_k, save_q, save_t, save_l, save_w):
            a.wait()


def hand_out(*refs):
    came, outs, held, (got, put) = refs[:5], refs[5:10], refs[10:15], refs[15:]
    loads = [pltpu.make_async_copy(came[n], held[n], got.at[n]) for n in range(5)]
    saves = [pltpu.make_async_copy(held[n], outs[n], put.at[n]) for n in range(4)]
    for a in loads:
        a.start()
    for n in range(4):
        loads[n].wait()
        saves[n].start()
    loads[4].wait()
    outs[4][0] = held[4][0, 0]
    for a in saves:
        a.wait()


def body(tokens, cotangent, value_weight, query_heads, key_heads, lambdas):
    L = query_heads.shape[1]
    smem = pl.BlockSpec(memory_space=pltpu.SMEM)
    anywhere = pl.BlockSpec(memory_space=pl.ANY)
    hbm = pl.BlockSpec(memory_space=pltpu.HBM)
    tiles = (NB * (NB + 1) // 2, B, B)
    dma = lambda *n: pltpu.SemaphoreType.DMA(n)
    gq, gk, gt, gw, gl = pl.pallas_call(
        kernel,
        out_shape=(S((L, 128), BF), S((L, 128), BF), S((128, 2048), BF), S((16, 2048), F32), S((8, 128), F32)),
        in_specs=[anywhere] * 6, out_specs=[anywhere] * 5,
        scratch_shapes=[
            V((4, 128, 2048), BF), V((4, 4, 128, 512), BF), V((16, 8, 16, 2048), BF), V((4, 16, 512), BF), V((16, 8, 16, 512), BF),
            V((L, 128), BF), V((L, 128), BF), V((L, 128), BF),
            V((NB, B, 128), BF), V((NB, B, 128), BF), V((NB, 128, B), BF), V((NB, 128, B), BF), V((NB, B, 128), BF), V((4, 2, B, 128), BF),
            V((NB, B, B), F32), V((NB, B, B), F32), V(tiles, BF), V(tiles, BF), V(tiles, BF),
            V((NB, 128, B), BF), V((NB, B, 128), BF), V((NB, 8, B), F32), V((NB, 128, B), F32), V((NB, 128, B), F32), V((NB, 128, B), F32),
            V((4, NB, B, 128), BF), V((4, 4, 128, 128), BF), V((4, 128, 512), BF), V((128, 2048), F32), V((4, 128, 512), F32), V((4, 8, 4, 16, 128), BF), V((4, 8, 4, 16, 128), BF),
            V((4, 4, 16, 128), BF), V((4, 4, 16, 128), BF), V((L, 128), BF), V((L, 128), BF), V((128, 2048), BF), V((16, 2048), F32),
            V((8, 128), F32), V((8, 8, 128), F32), pltpu.SMEM((1,), F32),
            dma(6), dma(1), dma(5), dma(1), dma(4), dma(1), dma(4), dma(1), dma(1), dma(2), dma(2, 4), dma(1), dma(4), dma(1), dma(4), dma(1), dma(1), dma(1), dma(1), dma(1), dma(4), dma(1), dma(8, 4), dma(1), dma(4), dma(1), dma(1), dma(1), dma(1), dma(1), dma(1), dma(1), dma(1), dma(1), dma(1)],
        compiler_params=pltpu.CompilerParams(vmem_limit_bytes=60 * 1024 * 1024, collective_id=0, has_side_effects=True),
        name="whole")(lambdas, tokens[0], cotangent[0], value_weight, query_heads.reshape(L, 128), key_heads.reshape(L, 128))
    gq, gk, gt, gw, gl = pl.pallas_call(
        hand_out,
        out_shape=(S((L, 128), BF), S((L, 128), BF), S((128, 2048), BF), S((16, 2048), F32), S((1,), F32)),
        in_specs=[hbm] * 5, out_specs=[hbm] * 4 + [smem],
        scratch_shapes=[V((L, 128), BF), V((L, 128), BF), V((128, 2048), BF), V((16, 2048), F32), pltpu.SMEM((8, 128), F32), dma(5), dma(4)],
        compiler_params=pltpu.CompilerParams(vmem_limit_bytes=60 * 1024 * 1024),
        name="hand_out")(gq, gk, gt, gw, gl)
    return gq.reshape(query_heads.shape), gk.reshape(key_heads.shape), gt[None], gw, gl


def solution(mesh):
    placed = (P("dp", "sp", None), P("dp", "sp", None), P(("sp", "dp"), None),
              P("dp", None, "sp", None), P("dp", None, "sp", None), P("sp"))
    outs = (P("dp", None, "sp", None), P("dp", None, "sp", None), P("dp", "sp", None), P(("sp", "dp"), None), P("sp"))
    return jax.shard_map(body, mesh=mesh, in_specs=placed, out_specs=outs, check_vma=False)
```

```python
import functools, math
import jax, jax.numpy as jnp
from jax import lax
from jax.experimental import pallas as pl
from jax.experimental.pallas import tpu as pltpu
from jax.sharding import PartitionSpec as P

EPS = 1e-6
B = 256
NB = 8
SCALE = 0.125
LOG2E = 1.4426950408889634
F32 = jnp.float32
BF = jnp.bfloat16

def nt(a, b):
    return lax.dot_general(a, b, (((1,), (1,)), ((), ())), preferred_element_type=F32)

def nn(a, b):
    return lax.dot_general(a, b, (((1,), (0,)), ((), ())), preferred_element_type=F32)

def tri(i, j):
    return (i * (i + 1)) // 2 + j

def paired(lo, n, body):
    def two(p, c):
        body(lo + 2 * p, 2)
        return c
    lax.fori_loop(0, n // 2, two, 0)
    def one(p, c):
        body(lo + n - 1, 1)
        return c
    lax.fori_loop(0, n % 2, one, 0)

def prepare(i, q_ref, k_ref, qz1, qz2, kt):
    rows = pl.ds(pl.multiple_of(i * B, B), B)
    q = q_ref[rows, :]
    first = lax.broadcasted_iota(jnp.int32, (B, 128), 1) < 64
    zero = jnp.zeros_like(q)
    qz1[i] = jnp.where(first, q, zero)
    qz2[i] = jnp.where(first, zero, q)
    kt[i] = k_ref[rows, :].T

def softmaxes(i, lam, k_ref, qz1, qz2, s1, s2, p1, p2, aa):
    q1, q2 = qz1[i], qz2[i]

    def score(j, m):
        k = k_ref[pl.ds(pl.multiple_of(j * B, B), B), :]
        a, b = nt(k, q1), nt(k, q2)
        return a, b

    def keep(j, a, b, m):
        s1[j] = a
        s2[j] = b
        return (jnp.maximum(m[0], jnp.max(a.reshape(B // 8, 8, B), axis=0)),
                jnp.maximum(m[1], jnp.max(b.reshape(B // 8, 8, B), axis=0)))

    a, b = score(i, None)
    seen = lax.broadcasted_iota(jnp.int32, (B, B), 0) <= lax.broadcasted_iota(jnp.int32, (B, B), 1)
    a = jnp.where(seen, a, -1e30)
    b = jnp.where(seen, b, -1e30)
    low = jnp.full((8, B), -1e30, F32)
    m = keep(i, a, b, (low, low))

    def off(j, m):
        a, b = score(j, m)
        return keep(j, a, b, m)
    def two(p, m):
        a, b = score(2 * p, m)
        c, d = score(2 * p + 1, m)
        m = keep(2 * p, a, b, m)
        return keep(2 * p + 1, c, d, m)
    m = lax.fori_loop(0, i // 2, two, m)
    m = lax.fori_loop(i - i % 2, i, off, m)
    m1 = jnp.max(m[0], axis=0, keepdims=True)
    m2 = jnp.max(m[1], axis=0, keepdims=True)
    c = SCALE * LOG2E

    def power(j, l):
        e1 = jnp.exp2((s1[j] - m1) * c)
        e2 = jnp.exp2((s2[j] - m2) * c)
        s1[j] = e1
        s2[j] = e2
        return (l[0] + jnp.sum(e1.reshape(B // 8, 8, B), axis=0),
                l[1] + jnp.sum(e2.reshape(B // 8, 8, B), axis=0))
    l = lax.fori_loop(0, i + 1, power, (jnp.zeros((8, B), F32), jnp.zeros((8, B), F32)))
    r1 = 1.0 / jnp.sum(l[0], axis=0, keepdims=True)
    r2 = 1.0 / jnp.sum(l[1], axis=0, keepdims=True)

    def norm(j, _):
        x1 = s1[j] * r1
        x2 = s2[j] * r2
        t = tri(i, j)
        p1[t] = x1.astype(BF)
        p2[t] = x2.astype(BF)
        aa[t] = (x1 - lam * x2).astype(BF)
        return _
    lax.fori_loop(0, i + 1, norm, 0)

def keys_block(j, vn, qz1, qz2, kt, p1, p2, aa, dot, do, delta, dqt):
    v = vn[j]
    k1t, k2t = kt[j, 0:64, :], kt[j, 64:128, :]

    def parts(i):
        t = tri(i, j)
        da = nn(v, dot[i])
        x1 = (p1[t].astype(F32) * (da - delta[i, 0:1, :])).astype(BF)
        x2 = (p2[t].astype(F32) * (da - delta[i, 1:2, :])).astype(BF)
        dv = nn(aa[t], do[i])
        dk1 = nn(x1, qz1[i])
        dk2 = nn(x2, qz2[i])
        dqt[i, 0:64, :] += nn(k1t, x1)
        dqt[i, 64:128, :] += nn(k2t, x2)
        return dv, dk1 , dk2

    def two(p, c):
        a = parts(j + 2 * p)
        b = parts(j + 2 * p + 1)
        return tuple(x + (y + z) for x, y, z in zip(c, a, b))
    def one(p, c):
        a = parts(p)
        return tuple(x + y for x, y in zip(c, a))
    n = NB - j
    zero = jnp.zeros((B, 128), F32)
    c = lax.fori_loop(0, n // 2, two, (zero, zero, zero))
    c = lax.fori_loop(NB - n % 2, NB, one, c)
    return c[0], c[1], c[2]


MESH = pl.DeviceIdType.MESH
V = pltpu.VMEM
S = jax.ShapeDtypeStruct


class Ring:
    def __init__(self, at, ss, rs, me, to):
        self.at, self.ss, self.rs, self.me, self.to = at, ss, rs, me, to

    def index(self, o):
        return lax.rem(self.me + (o + 4), 4)

    def copy(self, o, part, delta, sem):
        s, d = self.to(self.index(delta))
        ref = self.at(self.index(o), part)
        return pltpu.make_async_remote_copy(
            src_ref=ref, dst_ref=ref, send_sem=self.ss, recv_sem=self.rs(sem),
            device_id={"sp": s, "dp": d}, device_id_type=MESH)

    def start(self):
        self.copy(0, 0, 1, 0).start()
        self.copy(0, 1, -1, 1).start()
        self.copy(0, 1, 1, 2).start()
        self.copy(0, 0, -1, 2).start()

    def near(self):
        self.copy(-1, 0, 1, 0).wait_recv()
        self.copy(-1, 0, 1, 3).start()
        self.copy(1, 1, -1, 1).wait_recv()
        self.copy(1, 1, -1, 3).start()

    def both(self, o, sem):
        ref = self.at(self.index(o), None)
        pltpu.make_async_copy(ref, ref, self.rs(sem)).wait()

    def full(self):
        self.both(1, 2)

    def far(self):
        self.both(2, 3)


def kernel(lam_h, tok_h, cot_h, w_h, q_h, k_h, gq_h, gk_h, gt_h, gw_h, gl_h,
           xr, xc, w, wo, wq, cota, q_ref, k_ref, qz1, qz2, kt, vt, vn, v4, s1, s2, p1, p2, aa, dot, do, delta, dqt, ot, o2t,
           dvg, dvin, dvrow, gta, gwp, gwin, gws, gwf, gqb, gkb, gtb, gwo, glb, glin,
           lam_ref, load, wload, save, xs, xr_, ys, yr, zs, zr, ws, wr, rs_, rr, qs, qr, h1s, h1r, cs, cr, vs, vr, gs, gr, ds_, dr,
           es, er, ls, lr, fs, fr, wds, wdr, qds, qdr, gf):
    sp, dp = lax.axis_index("sp"), lax.axis_index("dp")
    y, z = lax.rem(sp, 4), lax.div(sp, 4)
    scope = jax.named_scope

    def sp_peers(body):
        lax.fori_loop(1, 16, lambda d, c: (body(lax.rem(sp + d, 16)), c)[1], 0)

    def dp_peers(body):
        lax.fori_loop(1, 8, lambda d, c: (body(lax.rem(dp + d, 8)), c)[1], 0)

    def remote(src, dst, ss, rs, s, d):
        return pltpu.make_async_remote_copy(src_ref=src, dst_ref=dst, send_sem=ss, recv_sem=rs,
                                            device_id={"sp": s, "dp": d}, device_id_type=MESH)

    def all_of(ref, sem):
        pltpu.make_async_copy(ref, ref, sem.at[0]).wait()

    def lanes(h, n=128):
        return pl.ds(pl.multiple_of(h * n, n), n)

    def rows(i, n=B):
        return pl.ds(pl.multiple_of(i * n, n), n)

    barrier = pltpu.get_barrier_semaphore()
    sp_peers(lambda s: pl.semaphore_signal(barrier, inc=1, device_id={"sp": s, "dp": dp}, device_id_type=MESH))
    dp_peers(lambda d: pl.semaphore_signal(barrier, inc=1, device_id={"sp": sp, "dp": d}, device_id_type=MESH))
    loads = [pltpu.make_async_copy(a, b, load.at[n]) for n, (a, b) in enumerate((
        (w_h, w.at[sp, dp]), (tok_h, xr.at[y]), (q_h, q_ref), (k_h, k_ref), (cot_h.at[:, lanes(sp)], cota.at[rows(sp, 128)]), (lam_h, lam_ref)))]
    for a in loads:
        a.start()
    parts = [pltpu.make_async_copy(w_h.at[:, pl.ds((4 * b + a) * 128, 128)], wo.at[a, :, pl.ds(b * 128, 128)], wload.at[0])
             for a in range(4) for b in range(4)]
    for a in parts:
        a.start()

    x_, core = lax.div(dp, 2), lax.rem(dp, 2)
    along_y = lambda i: (z * 4 + i, dp)
    along_z = lambda i: (i * 4 + y, dp)
    along_x = lambda i: (sp, 2 * i + core)

    def split(ref, view, n):
        return lambda i, part: view(i, pl.ds(0, n) if part is None else pl.ds(n // 2 * part, n // 2))

    wy = Ring(lambda i, part: w.at[z * 4 + i, dp] if part is None else w.at[z * 4 + i, dp, :, pl.ds(1024 * part, 1024)],
              ws.at[0], lambda n: wr.at[0, n], y, along_y)
    wz = Ring(lambda i, part: w.at[pl.ds(4 * i, 4), dp] if part is None else w.at[pl.ds(4 * i + 2 * part, 2), dp],
              ws.at[1], lambda n: wr.at[1, n], z, along_z)
    xring = Ring(split(xr, lambda i, d: xr.at[i, d], 128), xs.at[0], lambda n: xr_.at[n], y, along_y)
    cring = Ring(split(xc, lambda i, d: xc.at[i, d], 4), ys.at[0], lambda n: yr.at[n], y, along_y)
    wrow = Ring(split(w, lambda i, d: w.at[d, 2 * i + core], 16), rs_.at[0], lambda n: rr.at[n], x_, along_x)
    qrow = Ring(split(wq, lambda i, d: wq.at[d, 2 * i + core], 16), qs.at[0], lambda n: qr.at[n], x_, along_x)

    def other(ref, ring, o, ss, rs):
        d = 2 * ring.index(o) + core
        return remote(ref.at[:, d], ref.at[:, d], ss.at[0], rs.at[0], sp, dp + 1 - 2 * core)

    for a in loads[:2]:
        a.wait()
    all_of(wo, wload)
    wq[sp, dp] = wo[y]
    xc[y, z] = xr[y, :, lanes(z, 512)]
    with scope("barrier"):
        pl.semaphore_wait(barrier, 22)

    def head_rows(s, src, to):
        return remote(wo.at[lax.rem(to, 4)], wq.at[src, dp], h1s.at[0], h1r.at[0], s, dp)

    def columns(zz, src, to):
        return remote(xr.at[y, :, lanes(to, 512)], xc.at[y, src], zs.at[0], zr.at[0], zz * 4 + y, dp)

    def z_peers(body):
        for d in (1, 3, 2):
            body(lax.rem(z + d, 4))

    wy.start()
    sp_peers(lambda s: head_rows(s, sp, s).start())
    z_peers(lambda t: columns(t, z, t).start())
    def cot_part(s, src, to):
        return remote(cot_h.at[:, lanes(to)], cota.at[rows(src, 128)], cs.at[0], cr.at[0], s, dp)

    for n in (2, 3, 5):
        loads[n].wait()
    lam = lam_ref[0]

    def prep(i, c):
        prepare(i, q_ref, k_ref, qz1, qz2, kt)
        zero = jnp.zeros((128, B), F32)
        dqt[i] = zero
        ot[i] = zero
        o2t[i] = zero
        return c
    lax.fori_loop(0, NB, prep, 0)

    def soft(lo, hi):
        lax.fori_loop(lo, hi, lambda i, c: (softmaxes(i, lam, k_ref, qz1, qz2, s1, s2, p1, p2, aa), c)[1], 0)

    with scope("soft03"):
        soft(0, 3)
    with scope("wynear"):
        wy.near()
    xring.start()
    with scope("heads"):
        all_of(wq.at[pl.ds(0, 15), 0], h1r)
    qrow.start()
    other(wq, qrow, 0, qds, qdr).start()
    with scope("soft34"):
        soft(3, 4)
    with scope("wyfar"):
        wy.full()
        wy.far()
    wz.start()
    with scope("soft46"):
        soft(4, 6)
    with scope("xnear0"):
        xring.near()
    with scope("soft67"):
        soft(6, 7)
    with scope("qnear"):
        qrow.near()
        qrow.full()
        for o in (-1, 1):
            other(wq, qrow, o, qds, qdr).start()
    with scope("wznear"):
        wz.near()
    sp_peers(lambda s: cot_part(s, sp, s).start())
    with scope("xfull"):
        xring.full()
    with scope("soft78"):
        soft(7, 8)
    with scope("wzfar"):
        wz.full()
        wz.far()
    wrow.start()
    other(w, wrow, 0, wds, wdr).start()
    with scope("qfar"):
        qrow.far()
        other(wq, qrow, 2, qds, qdr).start()
    with scope("qall"):
        all_of(wq.at[:, pl.ds(0, 4)], qdr)
    def v_part(zz, src, to, b):
        return remote(v4.at[to, b], vn.at[2 * src + lax.div(b, 2), rows(lax.rem(b, 2), 128)], vs.at[0], vr.at[src], zz * 4 + y, dp)

    def values(b):
        v = nn(xr[b], wq[...].reshape(2048, 512)).astype(BF)
        for t in range(4):
            v4[t, b] = v[:, t * 128:(t + 1) * 128]

            @pl.when(t != z)
            def _():
                v_part(t, z, t, b).start()
        vn[2 * z + lax.div(b, 2), rows(lax.rem(b, 2), 128), :] = v4[z, b]

    with scope("values3"):
        lax.fori_loop(0, 3, lambda n, c: (values(lax.rem(y + n + lax.div(n, 2), 4)), c)[1], 0)
    with scope("xfar"):
        xring.far()
    with scope("values1"):
        values(lax.rem(y + 2, 4))
    with scope("columns"):
        all_of(xc.at[0, pl.ds(0, 3)], zr)
    cring.start()

    def mixed(r):
        def one(e, c):
            j = 2 * r + e
            v = vn[j].T
            vt[j] = v

            def add(i, count):
                for m in range(count):
                    t = tri(i + m, j)
                    ot[i + m] += nn(v, aa[t])
                    o2t[i + m] += nn(v, p2[t])
            paired(j, NB - j, add)
            return c
        lax.fori_loop(0, 2, one, 0)

    def all_v(t):
        ref = vn.at[pl.ds(2 * t, 2)]
        pltpu.make_async_copy(ref, ref, vr.at[t]).wait()

    with scope("mix0"):
        mixed(z)
    for d in (1, 3):
        t = lax.rem(z + d, 4)
        with scope("v%d" % d):
            all_v(t)
        with scope("mix%d" % d):
            mixed(t)
    t = lax.rem(z + 2, 4)
    with scope("v2"):
        all_v(t)
    with scope("mix2"):
        mixed(t)
    with scope("cot"):
        loads[4].wait()
        all_of(cota.at[pl.ds(0, 1920)], cr)

    def mix(i, total):
        o, o2 = ot[i], o2t[i]
        g = cota[rows(i), :].astype(F32).T
        r = lax.rsqrt(jnp.mean(o * o, axis=0, keepdims=True) + EPS)
        yy = r * o
        d = (r * (g - yy * jnp.mean(g * yy, axis=0, keepdims=True))).astype(BF)
        dw = d.astype(F32)
        d2 = jnp.sum(dw * o2, axis=0, keepdims=True)
        d1 = jnp.sum(dw * o, axis=0, keepdims=True) + lam * d2
        dot[i] = d
        do[i] = dw.T.astype(BF)
        delta[i, 0:1, :] = d1
        delta[i, 1:2, :] = d2
        return total + d2
    with scope("mix"):
        total = lax.fori_loop(0, NB, mix, jnp.zeros((1, B), F32))
    glb[...] = jnp.broadcast_to(-jnp.sum(total, axis=1, keepdims=True), (8, 128))

    half = lax.broadcasted_iota(jnp.int32, (1, 128), 1) < 64
    ks = jnp.where(half, SCALE, -lam * SCALE)

    def gl_part(d, src, to):
        return remote(glb, glin.at[src], ls.at[0], lr.at[0], sp, d)

    def dv_part(yy, src, to, h):
        part = rows(lax.rem(to, 2), 128)
        return remote(dvg.at[h, 2 * z + lax.div(to, 2), part], dvin.at[h, src], ds_.at[0], dr.at[h], z * 4 + yy, dp)

    def y_peers(body):
        for d in (1, 3, 2):
            body(lax.rem(y + d, 4))

    def gw_part(d, src, to, h):
        return remote(gwp.at[h, to], gwin.at[h, src], es.at[0], er.at[0], sp, d)

    def send_dv(o):
        h = lax.rem(z + o, 4)
        y_peers(lambda t: dv_part(t, y, t, h).start())

    def send_weights(o):
        h = lax.rem(z + o, 4)
        g = sum(nn(dvg[h, 2 * b:2 * b + 2].reshape(512, 128).T, xc[:, b].reshape(512, 512)) for b in range(4))
        for n in range(4):
            gwp[h, :, n] = g[:, n * 128:(n + 1) * 128].T.astype(BF).reshape(8, 16, 128)
        dp_peers(lambda d: gw_part(d, dp, d, h).start())

    def dv_ring(j):
        return Ring(lambda i, part: dvg.at[i, j] if part is None else dvg.at[i, j, pl.ds(128 * part, 128)],
                    gs.at[0], lambda n: gr.at[j, n] if n < 2 else gf.at[n - 2], z, along_z)

    def main(n, c):
        j = NB - 1 - n
        dv, dk1, dk2 = keys_block(j, vn, qz1, qz2, kt, p1, p2, aa, dot, do, delta, dqt)
        dvg[z, j] = dv.astype(BF)
        dv_ring(j).start()
        gkb[rows(j), :] = ((dk1 + dk2) * ks).astype(BF)

        @pl.when(n == 2)
        def _():
            wrow.near()

        @pl.when(n == 4)
        def _():
            cring.near()
            dv_ring(7).near()

        @pl.when(n == 5)
        def _():
            dv_ring(6).near()

        @pl.when(n == 6)
        def _():
            dv_ring(5).near()

        @pl.when(n == 7)
        def _():
            dv_ring(4).near()
            wrow.full()
            for o in (-1, 1):
                other(w, wrow, o, wds, wdr).start()
        return c
    with scope("main"):
        lax.fori_loop(0, NB, main, 0)
    send_dv(0)
    save_k = pltpu.make_async_copy(gkb, gk_h, save.at[0])
    save_k.start()

    def fin(i, c):
        gqb[rows(i), :] = (dqt[i].T * ks).astype(BF)
        return c
    with scope("fin"):
        lax.fori_loop(0, NB, fin, 0)
    save_q = pltpu.make_async_copy(gqb, gq_h, save.at[1])
    save_q.start()
    with scope("near3"):
        dv_ring(3).near()
    with scope("cfar"):
        cring.full()
        cring.far()
    with scope("near21"):
        dv_ring(2).near()
    with scope("weights0"):
        send_weights(0)
    with scope("near1"):
        dv_ring(1).near()

    def gather(o):
        h = lax.rem(z + o, 4)
        dvin[h, y] = dvg[h, 2 * z + lax.div(y, 2), rows(lax.rem(y, 2), 128), :]
        pltpu.make_async_copy(dvin.at[h, pl.ds(0, 3)], dvin.at[h, pl.ds(0, 3)], dr.at[h]).wait()
        for a in range(4):
            dvrow[h, :, a * 128:(a + 1) * 128] = dvin[h, a]

    def times_rows(n, o):
        h = lax.rem(z + o, 4)
        return nt(dvrow[h], w[pl.ds(2 * n, 2), :, :, lanes(h, 512)].reshape(B, 512))

    with scope("near0"):
        dv_ring(0).near()
    with scope("full"):
        pltpu.make_async_copy(dvg.at[0], dvg.at[0], gf.at[0]).wait()
    for o in (1, 3):
        send_dv(o)
    with scope("wrowfar"):
        wrow.far()
        other(w, wrow, 2, wds, wdr).start()
    with scope("weights13"):
        for o in (1, 3):
            send_weights(o)
    with scope("far"):
        pltpu.make_async_copy(dvg.at[0], dvg.at[0], gf.at[1]).wait()
    send_dv(2)
    with scope("distant"):
        send_weights(2)
    dp_peers(lambda d: gl_part(d, dp, d).start())
    glin[dp] = glb[...]
    for h in range(4):
        gwin[h, dp] = gwp[h, dp]
    with scope("gather"):
        for o in (0, 1, 3):
            gather(o)
    with scope("wrowall"):
        all_of(w.at[:, pl.ds(0, 4)], wdr)

    def most(n, c):
        gta[:, rows(n)] = times_rows(n, 0) + times_rows(n, 1) + times_rows(n, 3)
        return c
    with scope("tgrada"):
        lax.fori_loop(0, NB, most, 0)
    with scope("gwwait"):
        all_of(gwin.at[:, pl.ds(0, 7)], er)
    for h in range(4):
        acc = gwin[h, 0].astype(F32)
        for d in range(1, 8):
            acc = acc + gwin[h, d].astype(F32)
        gws[:, h] = acc.astype(BF)

    def fin_part(yy, src, to):
        return remote(gws.at[to], gwf.at[src], fs.at[0], fr.at[0], z * 4 + yy, dp)
    y_peers(lambda t: fin_part(t, y, t).start())
    gwf[y] = gws[y]
    all_of(glin.at[pl.ds(0, 7)], lr)
    tot = glin[0]
    for d in range(1, 8):
        tot = tot + glin[d]
    delta[0] = jnp.concatenate([tot, tot], axis=1)
    save_l = pltpu.make_async_copy(delta.at[0, :, pl.ds(0, 128)], gl_h, save.at[3])
    save_l.start()
    with scope("dvwait"):
        gather(2)

    def tokens_grad(n, c):
        gtb[:, rows(n)] = (gta[:, rows(n)] + times_rows(n, 2)).astype(BF)
        return c
    with scope("tgradb"):
        lax.fori_loop(0, NB, tokens_grad, 0)
    save_t = pltpu.make_async_copy(gtb, gt_h, save.at[2])
    save_t.start()
    with scope("finwait"):
        all_of(gwf.at[pl.ds(0, 3)], fr)
    for a in range(4):
        for b in range(4):
            gwo[:, (4 * b + a) * 128:(4 * b + a + 1) * 128] = gwf[a, b].astype(F32)
    save_w = pltpu.make_async_copy(gwo, gw_h, save.at[4])
    save_w.start()
    all_of(xr.at[pl.ds(0, 3)], xs)
    all_of(xc.at[pl.ds(0, 3)], ys)
    all_of(w.at[pl.ds(0, 3), 0], ws)
    pltpu.make_async_copy(w.at[pl.ds(0, 12), 0], w.at[pl.ds(0, 12), 0], ws.at[1]).wait()
    all_of(w.at[:, pl.ds(0, 3)], rs_)
    all_of(wq.at[:, pl.ds(0, 3)], qs)
    all_of(w.at[:, pl.ds(0, 4)], wds)
    all_of(wq.at[:, pl.ds(0, 4)], qds)
    all_of(dvg.at[pl.ds(0, 3)], gs)
    all_of(wq.at[pl.ds(0, 15), 0], h1s)
    all_of(cota.at[pl.ds(0, 1920)], cs)
    all_of(dvin.at[pl.ds(0, 3)], ds_)
    all_of(gwin.at[:, pl.ds(0, 7)], es)
    all_of(xc.at[0, pl.ds(0, 3)], zs)
    all_of(v4.at[pl.ds(0, 3)], vs)
    all_of(glin.at[pl.ds(0, 7)], ls)
    all_of(gwf.at[pl.ds(0, 3)], fs)
    with scope("savewait"):
        for a in (save_k, save_q, save_t, save_l, save_w):
            a.wait()


def hand_out(*refs):
    came, outs, held, (got, put) = refs[:5], refs[5:10], refs[10:15], refs[15:]
    loads = [pltpu.make_async_copy(came[n], held[n], got.at[n]) for n in range(5)]
    saves = [pltpu.make_async_copy(held[n], outs[n], put.at[n]) for n in range(4)]
    for a in loads:
        a.start()
    for n in range(4):
        loads[n].wait()
        saves[n].start()
    loads[4].wait()
    outs[4][0] = held[4][0, 0]
    for a in saves:
        a.wait()


def body(tokens, cotangent, value_weight, query_heads, key_heads, lambdas):
    L = query_heads.shape[1]
    smem = pl.BlockSpec(memory_space=pltpu.SMEM)
    anywhere = pl.BlockSpec(memory_space=pl.ANY)
    hbm = pl.BlockSpec(memory_space=pltpu.HBM)
    tiles = (NB * (NB + 1) // 2, B, B)
    dma = lambda *n: pltpu.SemaphoreType.DMA(n)
    gq, gk, gt, gw, gl = pl.pallas_call(
        kernel,
        out_shape=(S((L, 128), BF), S((L, 128), BF), S((128, 2048), BF), S((16, 2048), F32), S((8, 128), F32)),
        in_specs=[anywhere] * 6, out_specs=[anywhere] * 5,
        scratch_shapes=[
            V((4, 128, 2048), BF), V((4, 4, 128, 512), BF), V((16, 8, 16, 2048), BF), V((4, 16, 512), BF), V((16, 8, 16, 512), BF),
            V((L, 128), BF), V((L, 128), BF), V((L, 128), BF),
            V((NB, B, 128), BF), V((NB, B, 128), BF), V((NB, 128, B), BF), V((NB, 128, B), BF), V((NB, B, 128), BF), V((4, 4, 128, 128), BF),
            V((NB, B, B), F32), V((NB, B, B), F32), V(tiles, BF), V(tiles, BF), V(tiles, BF),
            V((NB, 128, B), BF), V((NB, B, 128), BF), V((NB, 8, B), F32), V((NB, 128, B), F32), V((NB, 128, B), F32), V((NB, 128, B), F32),
            V((4, NB, B, 128), BF), V((4, 4, 128, 128), BF), V((4, 128, 512), BF), V((128, 2048), F32), V((4, 8, 4, 16, 128), BF), V((4, 8, 4, 16, 128), BF),
            V((4, 4, 16, 128), BF), V((4, 4, 16, 128), BF), V((L, 128), BF), V((L, 128), BF), V((128, 2048), BF), V((16, 2048), F32),
            V((8, 128), F32), V((8, 8, 128), F32), pltpu.SMEM((1,), F32),
            dma(6), dma(1), dma(5), dma(1), dma(4), dma(1), dma(4), dma(1), dma(1), dma(2), dma(2, 4), dma(1), dma(4), dma(1), dma(4), dma(1), dma(1), dma(1), dma(1), dma(1), dma(4), dma(1), dma(8, 2), dma(1), dma(4), dma(1), dma(1), dma(1), dma(1), dma(1), dma(1), dma(1), dma(1), dma(1), dma(1), dma(2)],
        compiler_params=pltpu.CompilerParams(vmem_limit_bytes=60 * 1024 * 1024, collective_id=0, has_side_effects=True),
        name="whole")(lambdas, tokens[0], cotangent[0], value_weight, query_heads.reshape(L, 128), key_heads.reshape(L, 128))
    gq, gk, gt, gw, gl = pl.pallas_call(
        hand_out,
        out_shape=(S((L, 128), BF), S((L, 128), BF), S((128, 2048), BF), S((16, 2048), F32), S((1,), F32)),
        in_specs=[hbm] * 5, out_specs=[hbm] * 4 + [smem],
        scratch_shapes=[V((L, 128), BF), V((L, 128), BF), V((128, 2048), BF), V((16, 2048), F32), pltpu.SMEM((8, 128), F32), dma(5), dma(4)],
        compiler_params=pltpu.CompilerParams(vmem_limit_bytes=60 * 1024 * 1024),
        name="hand_out")(gq, gk, gt, gw, gl)
    return gq.reshape(query_heads.shape), gk.reshape(key_heads.shape), gt[None], gw, gl


def solution(mesh):
    placed = (P("dp", "sp", None), P("dp", "sp", None), P(("sp", "dp"), None),
              P("dp", None, "sp", None), P("dp", None, "sp", None), P("sp"))
    outs = (P("dp", None, "sp", None), P("dp", None, "sp", None), P("dp", "sp", None), P(("sp", "dp"), None), P("sp"))
    return jax.shard_map(body, mesh=mesh, in_specs=placed, out_specs=outs, check_vma=False)
```

```python
import functools, math
import jax, jax.numpy as jnp
from jax import lax
from jax.experimental import pallas as pl
from jax.experimental.pallas import tpu as pltpu
from jax.sharding import PartitionSpec as P

EPS = 1e-6
B = 256
NB = 8
SCALE = 0.125
LOG2E = 1.4426950408889634
F32 = jnp.float32
BF = jnp.bfloat16

def nt(a, b):
    return lax.dot_general(a, b, (((1,), (1,)), ((), ())), preferred_element_type=F32)

def nn(a, b):
    return lax.dot_general(a, b, (((1,), (0,)), ((), ())), preferred_element_type=F32)

def tri(i, j):
    return (i * (i + 1)) // 2 + j

def paired(lo, n, body):
    def two(p, c):
        body(lo + 2 * p, 2)
        return c
    lax.fori_loop(0, n // 2, two, 0)
    def one(p, c):
        body(lo + n - 1, 1)
        return c
    lax.fori_loop(0, n % 2, one, 0)

def prepare(i, q_ref, k_ref, qz1, qz2, kt):
    rows = pl.ds(pl.multiple_of(i * B, B), B)
    q = q_ref[rows, :]
    first = lax.broadcasted_iota(jnp.int32, (B, 128), 1) < 64
    zero = jnp.zeros_like(q)
    qz1[i] = jnp.where(first, q, zero)
    qz2[i] = jnp.where(first, zero, q)
    kt[i] = k_ref[rows, :].T

def softmaxes(i, lam, k_ref, qz1, qz2, s1, s2, p1, p2, aa):
    q1, q2 = qz1[i], qz2[i]

    def score(j, m):
        k = k_ref[pl.ds(pl.multiple_of(j * B, B), B), :]
        a, b = nt(k, q1), nt(k, q2)
        return a, b

    def keep(j, a, b, m):
        s1[j] = a
        s2[j] = b
        return (jnp.maximum(m[0], jnp.max(a.reshape(B // 8, 8, B), axis=0)),
                jnp.maximum(m[1], jnp.max(b.reshape(B // 8, 8, B), axis=0)))

    a, b = score(i, None)
    seen = lax.broadcasted_iota(jnp.int32, (B, B), 0) <= lax.broadcasted_iota(jnp.int32, (B, B), 1)
    a = jnp.where(seen, a, -1e30)
    b = jnp.where(seen, b, -1e30)
    low = jnp.full((8, B), -1e30, F32)
    m = keep(i, a, b, (low, low))

    def off(j, m):
        a, b = score(j, m)
        return keep(j, a, b, m)
    def two(p, m):
        a, b = score(2 * p, m)
        c, d = score(2 * p + 1, m)
        m = keep(2 * p, a, b, m)
        return keep(2 * p + 1, c, d, m)
    m = lax.fori_loop(0, i // 2, two, m)
    m = lax.fori_loop(i - i % 2, i, off, m)
    m1 = jnp.max(m[0], axis=0, keepdims=True)
    m2 = jnp.max(m[1], axis=0, keepdims=True)
    c = SCALE * LOG2E

    def power(j, l):
        e1 = jnp.exp2((s1[j] - m1) * c)
        e2 = jnp.exp2((s2[j] - m2) * c)
        s1[j] = e1
        s2[j] = e2
        return (l[0] + jnp.sum(e1.reshape(B // 8, 8, B), axis=0),
                l[1] + jnp.sum(e2.reshape(B // 8, 8, B), axis=0))
    l = lax.fori_loop(0, i + 1, power, (jnp.zeros((8, B), F32), jnp.zeros((8, B), F32)))
    r1 = 1.0 / jnp.sum(l[0], axis=0, keepdims=True)
    r2 = 1.0 / jnp.sum(l[1], axis=0, keepdims=True)

    def norm(j, _):
        x1 = s1[j] * r1
        x2 = s2[j] * r2
        t = tri(i, j)
        p1[t] = x1.astype(BF)
        p2[t] = x2.astype(BF)
        aa[t] = (x1 - lam * x2).astype(BF)
        return _
    lax.fori_loop(0, i + 1, norm, 0)

def keys_block(j, vn, qz1, qz2, kt, p1, p2, aa, dot, do, delta, dqt):
    v = vn[j]
    k1t, k2t = kt[j, 0:64, :], kt[j, 64:128, :]

    def parts(i):
        t = tri(i, j)
        da = nn(v, dot[i])
        x1 = (p1[t].astype(F32) * (da - delta[i, 0:1, :])).astype(BF)
        x2 = (p2[t].astype(F32) * (da - delta[i, 1:2, :])).astype(BF)
        dv = nn(aa[t], do[i])
        dk1 = nn(x1, qz1[i])
        dk2 = nn(x2, qz2[i])
        dqt[i, 0:64, :] += nn(k1t, x1)
        dqt[i, 64:128, :] += nn(k2t, x2)
        return dv, dk1 , dk2

    def two(p, c):
        a = parts(j + 2 * p)
        b = parts(j + 2 * p + 1)
        return tuple(x + (y + z) for x, y, z in zip(c, a, b))
    def one(p, c):
        a = parts(p)
        return tuple(x + y for x, y in zip(c, a))
    n = NB - j
    zero = jnp.zeros((B, 128), F32)
    c = lax.fori_loop(0, n // 2, two, (zero, zero, zero))
    c = lax.fori_loop(NB - n % 2, NB, one, c)
    return c[0], c[1], c[2]


MESH = pl.DeviceIdType.MESH
V = pltpu.VMEM
S = jax.ShapeDtypeStruct


class Ring:
    def __init__(self, at, ss, rs, me, to):
        self.at, self.ss, self.rs, self.me, self.to = at, ss, rs, me, to

    def index(self, o):
        return lax.rem(self.me + (o + 4), 4)

    def copy(self, o, part, delta, sem):
        s, d = self.to(self.index(delta))
        ref = self.at(self.index(o), part)
        return pltpu.make_async_remote_copy(
            src_ref=ref, dst_ref=ref, send_sem=self.ss, recv_sem=self.rs(sem),
            device_id={"sp": s, "dp": d}, device_id_type=MESH)

    def start(self):
        self.copy(0, 0, 1, 0).start()
        self.copy(0, 1, -1, 1).start()
        self.copy(0, 1, 1, 2).start()
        self.copy(0, 0, -1, 2).start()

    def near(self):
        self.copy(-1, 0, 1, 0).wait_recv()
        self.copy(-1, 0, 1, 3).start()
        self.copy(1, 1, -1, 1).wait_recv()
        self.copy(1, 1, -1, 3).start()

    def both(self, o, sem):
        ref = self.at(self.index(o), None)
        pltpu.make_async_copy(ref, ref, self.rs(sem)).wait()

    def full(self):
        self.both(1, 2)

    def far(self):
        self.both(2, 3)


def kernel(lam_h, tok_h, cot_h, w_h, q_h, k_h, gq_h, gk_h, gt_h, gw_h, gl_h,
           xr, xc, w, wo, wq, cota, q_ref, k_ref, qz1, qz2, kt, vt, vn, v4, s1, s2, p1, p2, aa, dot, do, delta, dqt, ot, o2t,
           dvg, dvin, dvrow, gta, gwp, gwin, gws, gwf, gqb, gkb, gtb, gwo, glb, glin,
           lam_ref, load, wload, save, xs, xr_, ys, yr, zs, zr, ws, wr, rs_, rr, qs, qr, h1s, h1r, cs, cr, vs, vr, gs, gr, ds_, dr,
           es, er, ls, lr, fs, fr, wds, wdr, qds, qdr, gf):
    sp, dp = lax.axis_index("sp"), lax.axis_index("dp")
    y, z = lax.rem(sp, 4), lax.div(sp, 4)
    scope = jax.named_scope

    def sp_peers(body):
        lax.fori_loop(1, 16, lambda d, c: (body(lax.rem(sp + d, 16)), c)[1], 0)

    def dp_peers(body):
        lax.fori_loop(1, 8, lambda d, c: (body(lax.rem(dp + d, 8)), c)[1], 0)

    def remote(src, dst, ss, rs, s, d):
        return pltpu.make_async_remote_copy(src_ref=src, dst_ref=dst, send_sem=ss, recv_sem=rs,
                                            device_id={"sp": s, "dp": d}, device_id_type=MESH)

    def all_of(ref, sem):
        pltpu.make_async_copy(ref, ref, sem.at[0]).wait()

    def lanes(h, n=128):
        return pl.ds(pl.multiple_of(h * n, n), n)

    def rows(i, n=B):
        return pl.ds(pl.multiple_of(i * n, n), n)

    barrier = pltpu.get_barrier_semaphore()
    sp_peers(lambda s: pl.semaphore_signal(barrier, inc=1, device_id={"sp": s, "dp": dp}, device_id_type=MESH))
    dp_peers(lambda d: pl.semaphore_signal(barrier, inc=1, device_id={"sp": sp, "dp": d}, device_id_type=MESH))
    loads = [pltpu.make_async_copy(a, b, load.at[n]) for n, (a, b) in enumerate((
        (w_h, w.at[sp, dp]), (tok_h, xr.at[y]), (q_h, q_ref), (k_h, k_ref), (cot_h.at[:, lanes(sp)], cota.at[rows(sp, 128)]), (lam_h, lam_ref)))]
    for a in loads:
        a.start()
    parts = [pltpu.make_async_copy(w_h.at[:, pl.ds((4 * b + a) * 128, 128)], wo.at[a, :, pl.ds(b * 128, 128)], wload.at[0])
             for a in range(4) for b in range(4)]
    for a in parts:
        a.start()

    x_, core = lax.div(dp, 2), lax.rem(dp, 2)
    along_y = lambda i: (z * 4 + i, dp)
    along_z = lambda i: (i * 4 + y, dp)
    along_x = lambda i: (sp, 2 * i + core)

    def split(ref, view, n):
        return lambda i, part: view(i, pl.ds(0, n) if part is None else pl.ds(n // 2 * part, n // 2))

    wy = Ring(lambda i, part: w.at[z * 4 + i, dp] if part is None else w.at[z * 4 + i, dp, :, pl.ds(1024 * part, 1024)],
              ws.at[0], lambda n: wr.at[0, n], y, along_y)
    wz = Ring(lambda i, part: w.at[pl.ds(4 * i, 4), dp] if part is None else w.at[pl.ds(4 * i + 2 * part, 2), dp],
              ws.at[1], lambda n: wr.at[1, n], z, along_z)
    xring = Ring(split(xr, lambda i, d: xr.at[i, d], 128), xs.at[0], lambda n: xr_.at[n], y, along_y)
    cring = Ring(split(xc, lambda i, d: xc.at[i, d], 4), ys.at[0], lambda n: yr.at[n], y, along_y)
    wrow = Ring(split(w, lambda i, d: w.at[d, 2 * i + core], 16), rs_.at[0], lambda n: rr.at[n], x_, along_x)
    qrow = Ring(split(wq, lambda i, d: wq.at[d, 2 * i + core], 16), qs.at[0], lambda n: qr.at[n], x_, along_x)

    def other(ref, ring, o, ss, rs):
        d = 2 * ring.index(o) + core
        return remote(ref.at[:, d], ref.at[:, d], ss.at[0], rs.at[0], sp, dp + 1 - 2 * core)

    for a in loads[:2]:
        a.wait()
    all_of(wo, wload)
    wq[sp, dp] = wo[y]
    xc[y, z] = xr[y, :, lanes(z, 512)]
    with scope("barrier"):
        pl.semaphore_wait(barrier, 22)

    def head_rows(s, src, to):
        return remote(wo.at[lax.rem(to, 4)], wq.at[src, dp], h1s.at[0], h1r.at[0], s, dp)

    def columns(zz, src, to):
        return remote(xr.at[y, :, lanes(to, 512)], xc.at[y, src], zs.at[0], zr.at[0], zz * 4 + y, dp)

    def z_peers(body):
        for d in (1, 3, 2):
            body(lax.rem(z + d, 4))

    wy.start()
    sp_peers(lambda s: head_rows(s, sp, s).start())
    z_peers(lambda t: columns(t, z, t).start())
    def cot_part(s, src, to):
        return remote(cot_h.at[:, lanes(to)], cota.at[rows(src, 128)], cs.at[0], cr.at[0], s, dp)

    for n in (2, 3, 5):
        loads[n].wait()
    lam = lam_ref[0]

    def prep(i, c):
        prepare(i, q_ref, k_ref, qz1, qz2, kt)
        zero = jnp.zeros((128, B), F32)
        dqt[i] = zero
        ot[i] = zero
        o2t[i] = zero
        return c
    lax.fori_loop(0, NB, prep, 0)

    def soft(lo, hi):
        lax.fori_loop(lo, hi, lambda i, c: (softmaxes(i, lam, k_ref, qz1, qz2, s1, s2, p1, p2, aa), c)[1], 0)

    with scope("soft03"):
        soft(0, 3)
    with scope("wynear"):
        wy.near()
    xring.start()
    with scope("heads"):
        all_of(wq.at[pl.ds(0, 15), 0], h1r)
    qrow.start()
    other(wq, qrow, 0, qds, qdr).start()
    with scope("soft34"):
        soft(3, 4)
    with scope("wyfar"):
        wy.full()
        wy.far()
    wz.start()
    with scope("soft46"):
        soft(4, 6)
    with scope("xnear0"):
        xring.near()
    with scope("soft67"):
        soft(6, 7)
    with scope("qnear"):
        qrow.near()
        qrow.full()
        for o in (1, -1):
            other(wq, qrow, o, qds, qdr).start()
    with scope("wznear"):
        wz.near()
    sp_peers(lambda s: cot_part(s, sp, s).start())
    with scope("xfull"):
        xring.full()
    with scope("soft78"):
        soft(7, 8)
    with scope("wzfar"):
        wz.full()
        wz.far()
    wrow.start()
    with scope("qfar"):
        qrow.far()
        other(wq, qrow, 2, qds, qdr).start()
    with scope("qall"):
        all_of(wq.at[:, pl.ds(0, 4)], qdr)
    def v_part(zz, src, to, b):
        return remote(v4.at[to, b], vn.at[2 * src + lax.div(b, 2), rows(lax.rem(b, 2), 128)], vs.at[0], vr.at[src], zz * 4 + y, dp)

    def values(b):
        v = nn(xr[b], wq[...].reshape(2048, 512)).astype(BF)
        for t in range(4):
            v4[t, b] = v[:, t * 128:(t + 1) * 128]

            @pl.when(t != z)
            def _():
                v_part(t, z, t, b).start()
        vn[2 * z + lax.div(b, 2), rows(lax.rem(b, 2), 128), :] = v4[z, b]

    with scope("values3"):
        lax.fori_loop(0, 3, lambda n, c: (values(lax.rem(y + n + lax.div(n, 2), 4)), c)[1], 0)
    with scope("xfar"):
        xring.far()
    with scope("values1"):
        values(lax.rem(y + 2, 4))
    with scope("columns"):
        all_of(xc.at[0, pl.ds(0, 3)], zr)
    cring.start()

    def mixed(r):
        def one(e, c):
            j = 2 * r + e
            v = vn[j].T
            vt[j] = v

            def add(i, count):
                for m in range(count):
                    t = tri(i + m, j)
                    ot[i + m] += nn(v, aa[t])
                    o2t[i + m] += nn(v, p2[t])
            paired(j, NB - j, add)
            return c
        lax.fori_loop(0, 2, one, 0)

    def all_v(t):
        ref = vn.at[pl.ds(2 * t, 2)]
        pltpu.make_async_copy(ref, ref, vr.at[t]).wait()

    with scope("mix0"):
        mixed(z)
    for d in (1, 3):
        t = lax.rem(z + d, 4)
        with scope("v%d" % d):
            all_v(t)
        with scope("mix%d" % d):
            mixed(t)
    t = lax.rem(z + 2, 4)
    with scope("v2"):
        all_v(t)
    with scope("mix2"):
        mixed(t)
    other(w, wrow, 0, wds, wdr).start()
    with scope("cot"):
        loads[4].wait()
        all_of(cota.at[pl.ds(0, 1920)], cr)

    def mix(i, total):
        o, o2 = ot[i], o2t[i]
        g = cota[rows(i), :].astype(F32).T
        r = lax.rsqrt(jnp.mean(o * o, axis=0, keepdims=True) + EPS)
        yy = r * o
        d = (r * (g - yy * jnp.mean(g * yy, axis=0, keepdims=True))).astype(BF)
        dw = d.astype(F32)
        d2 = jnp.sum(dw * o2, axis=0, keepdims=True)
        d1 = jnp.sum(dw * o, axis=0, keepdims=True) + lam * d2
        dot[i] = d
        do[i] = dw.T.astype(BF)
        delta[i, 0:1, :] = d1
        delta[i, 1:2, :] = d2
        return total + d2
    with scope("mix"):
        total = lax.fori_loop(0, NB, mix, jnp.zeros((1, B), F32))
    glb[...] = jnp.broadcast_to(-jnp.sum(total, axis=1, keepdims=True), (8, 128))

    half = lax.broadcasted_iota(jnp.int32, (1, 128), 1) < 64
    ks = jnp.where(half, SCALE, -lam * SCALE)

    def gl_part(d, src, to):
        return remote(glb, glin.at[src], ls.at[0], lr.at[0], sp, d)

    def dv_part(yy, src, to, h):
        part = rows(lax.rem(to, 2), 128)
        return remote(dvg.at[h, 2 * z + lax.div(to, 2), part], dvin.at[h, src], ds_.at[0], dr.at[h], z * 4 + yy, dp)

    def y_peers(body):
        for d in (1, 3, 2):
            body(lax.rem(y + d, 4))

    def gw_part(d, src, to, h):
        return remote(gwp.at[h, to], gwin.at[h, src], es.at[0], er.at[0], sp, d)

    def send_dv(o):
        h = lax.rem(z + o, 4)
        y_peers(lambda t: dv_part(t, y, t, h).start())

    def send_weights(o):
        h = lax.rem(z + o, 4)
        g = sum(nn(dvg[h, 2 * b:2 * b + 2].reshape(512, 128).T, xc[:, b].reshape(512, 512)) for b in range(4))
        for n in range(4):
            gwp[h, :, n] = g[:, n * 128:(n + 1) * 128].T.astype(BF).reshape(8, 16, 128)
        dp_peers(lambda d: gw_part(d, dp, d, h).start())

    def dv_ring(j):
        return Ring(lambda i, part: dvg.at[i, j] if part is None else dvg.at[i, j, pl.ds(128 * part, 128)],
                    gs.at[0], lambda n: gr.at[j, n] if n < 2 else gf.at[n - 2], z, along_z)

    def main(n, c):
        j = NB - 1 - n
        dv, dk1, dk2 = keys_block(j, vn, qz1, qz2, kt, p1, p2, aa, dot, do, delta, dqt)
        dvg[z, j] = dv.astype(BF)
        dv_ring(j).start()
        gkb[rows(j), :] = ((dk1 + dk2) * ks).astype(BF)

        @pl.when(n == 2)
        def _():
            wrow.near()

        @pl.when(n == 4)
        def _():
            cring.near()
            dv_ring(7).near()

        @pl.when(n == 5)
        def _():
            dv_ring(6).near()

        @pl.when(n == 6)
        def _():
            dv_ring(5).near()

        @pl.when(n == 7)
        def _():
            dv_ring(4).near()
            wrow.full()
            for o in (-1, 1):
                other(w, wrow, o, wds, wdr).start()
        return c
    with scope("main"):
        lax.fori_loop(0, NB, main, 0)
    send_dv(0)
    save_k = pltpu.make_async_copy(gkb, gk_h, save.at[0])
    save_k.start()

    def fin(i, c):
        gqb[rows(i), :] = (dqt[i].T * ks).astype(BF)
        return c
    with scope("fin"):
        lax.fori_loop(0, NB, fin, 0)
    save_q = pltpu.make_async_copy(gqb, gq_h, save.at[1])
    save_q.start()
    with scope("near3"):
        dv_ring(3).near()
    with scope("cfar"):
        cring.full()
        cring.far()
    with scope("near21"):
        dv_ring(2).near()
    with scope("weights0"):
        send_weights(0)
    with scope("near1"):
        dv_ring(1).near()

    def gather(o):
        h = lax.rem(z + o, 4)
        dvin[h, y] = dvg[h, 2 * z + lax.div(y, 2), rows(lax.rem(y, 2), 128), :]
        pltpu.make_async_copy(dvin.at[h, pl.ds(0, 3)], dvin.at[h, pl.ds(0, 3)], dr.at[h]).wait()
        for a in range(4):
            dvrow[h, :, a * 128:(a + 1) * 128] = dvin[h, a]

    def times_rows(n, o):
        h = lax.rem(z + o, 4)
        return nt(dvrow[h], w[pl.ds(2 * n, 2), :, :, lanes(h, 512)].reshape(B, 512))

    with scope("near0"):
        dv_ring(0).near()
    with scope("full"):
        pltpu.make_async_copy(dvg.at[0], dvg.at[0], gf.at[0]).wait()
    for o in (1, 3):
        send_dv(o)
    with scope("wrowfar"):
        wrow.far()
        other(w, wrow, 2, wds, wdr).start()
    with scope("weights13"):
        for o in (1, 3):
            send_weights(o)
    with scope("far"):
        pltpu.make_async_copy(dvg.at[0], dvg.at[0], gf.at[1]).wait()
    send_dv(2)
    with scope("distant"):
        send_weights(2)
    dp_peers(lambda d: gl_part(d, dp, d).start())
    glin[dp] = glb[...]
    for h in range(4):
        gwin[h, dp] = gwp[h, dp]
    with scope("gather"):
        for o in (0, 1, 3):
            gather(o)
    with scope("wrowall"):
        all_of(w.at[:, pl.ds(0, 4)], wdr)

    def most(n, c):
        gta[:, rows(n)] = times_rows(n, 0) + times_rows(n, 1) + times_rows(n, 3)
        return c
    with scope("tgrada"):
        lax.fori_loop(0, 6, most, 0)
    with scope("gwwait"):
        all_of(gwin.at[:, pl.ds(0, 7)], er)
    for h in range(4):
        acc = gwin[h, 0].astype(F32)
        for d in range(1, 8):
            acc = acc + gwin[h, d].astype(F32)
        gws[:, h] = acc.astype(BF)

    def fin_part(yy, src, to):
        return remote(gws.at[to], gwf.at[src], fs.at[0], fr.at[0], z * 4 + yy, dp)
    y_peers(lambda t: fin_part(t, y, t).start())
    gwf[y] = gws[y]
    all_of(glin.at[pl.ds(0, 7)], lr)
    tot = glin[0]
    for d in range(1, 8):
        tot = tot + glin[d]
    delta[0] = jnp.concatenate([tot, tot], axis=1)
    save_l = pltpu.make_async_copy(delta.at[0, :, pl.ds(0, 128)], gl_h, save.at[3])
    save_l.start()
    with scope("tgradc"):
        lax.fori_loop(6, NB, most, 0)
    with scope("dvwait"):
        gather(2)

    def tokens_grad(n, c):
        gtb[:, rows(n)] = (gta[:, rows(n)] + times_rows(n, 2)).astype(BF)
        return c
    with scope("tgradb"):
        lax.fori_loop(0, NB, tokens_grad, 0)
    save_t = pltpu.make_async_copy(gtb, gt_h, save.at[2])
    save_t.start()
    with scope("finwait"):
        all_of(gwf.at[pl.ds(0, 3)], fr)
    for a in range(4):
        for b in range(4):
            gwo[:, (4 * b + a) * 128:(4 * b + a + 1) * 128] = gwf[a, b].astype(F32)
    save_w = pltpu.make_async_copy(gwo, gw_h, save.at[4])
    save_w.start()
    all_of(xr.at[pl.ds(0, 3)], xs)
    all_of(xc.at[pl.ds(0, 3)], ys)
    all_of(w.at[pl.ds(0, 3), 0], ws)
    pltpu.make_async_copy(w.at[pl.ds(0, 12), 0], w.at[pl.ds(0, 12), 0], ws.at[1]).wait()
    all_of(w.at[:, pl.ds(0, 3)], rs_)
    all_of(wq.at[:, pl.ds(0, 3)], qs)
    all_of(w.at[:, pl.ds(0, 4)], wds)
    all_of(wq.at[:, pl.ds(0, 4)], qds)
    all_of(dvg.at[pl.ds(0, 3)], gs)
    all_of(wq.at[pl.ds(0, 15), 0], h1s)
    all_of(cota.at[pl.ds(0, 1920)], cs)
    all_of(dvin.at[pl.ds(0, 3)], ds_)
    all_of(gwin.at[:, pl.ds(0, 7)], es)
    all_of(xc.at[0, pl.ds(0, 3)], zs)
    all_of(v4.at[pl.ds(0, 3)], vs)
    all_of(glin.at[pl.ds(0, 7)], ls)
    all_of(gwf.at[pl.ds(0, 3)], fs)
    with scope("savewait"):
        for a in (save_k, save_q, save_t, save_l, save_w):
            a.wait()


def hand_out(*refs):
    came, outs, (held, got, put) = refs[:5], refs[5:10], refs[10:]
    saves = [pltpu.make_async_copy(came[n], outs[n], put.at[n]) for n in range(4)]
    scalar = pltpu.make_async_copy(came[4], held, got.at[0])
    scalar.start()
    for a in saves:
        a.start()
    scalar.wait()
    outs[4][0] = held[0, 0]
    for a in saves:
        a.wait()


def body(tokens, cotangent, value_weight, query_heads, key_heads, lambdas):
    L = query_heads.shape[1]
    smem = pl.BlockSpec(memory_space=pltpu.SMEM)
    anywhere = pl.BlockSpec(memory_space=pl.ANY)
    hbm = pl.BlockSpec(memory_space=pltpu.HBM)
    tiles = (NB * (NB + 1) // 2, B, B)
    dma = lambda *n: pltpu.SemaphoreType.DMA(n)
    gq, gk, gt, gw, gl = pl.pallas_call(
        kernel,
        out_shape=(S((L, 128), BF), S((L, 128), BF), S((128, 2048), BF), S((16, 2048), F32), S((8, 128), F32)),
        in_specs=[anywhere] * 6, out_specs=[anywhere] * 5,
        scratch_shapes=[
            V((4, 128, 2048), BF), V((4, 4, 128, 512), BF), V((16, 8, 16, 2048), BF), V((4, 16, 512), BF), V((16, 8, 16, 512), BF),
            V((L, 128), BF), V((L, 128), BF), V((L, 128), BF),
            V((NB, B, 128), BF), V((NB, B, 128), BF), V((NB, 128, B), BF), V((NB, 128, B), BF), V((NB, B, 128), BF), V((4, 4, 128, 128), BF),
            V((NB, B, B), F32), V((NB, B, B), F32), V(tiles, BF), V(tiles, BF), V(tiles, BF),
            V((NB, 128, B), BF), V((NB, B, 128), BF), V((NB, 8, B), F32), V((NB, 128, B), F32), V((NB, 128, B), F32), V((NB, 128, B), F32),
            V((4, NB, B, 128), BF), V((4, 4, 128, 128), BF), V((4, 128, 512), BF), V((128, 2048), F32), V((4, 8, 4, 16, 128), BF), V((4, 8, 4, 16, 128), BF),
            V((4, 4, 16, 128), BF), V((4, 4, 16, 128), BF), V((L, 128), BF), V((L, 128), BF), V((128, 2048), BF), V((16, 2048), F32),
            V((8, 128), F32), V((8, 8, 128), F32), pltpu.SMEM((1,), F32),
            dma(6), dma(1), dma(5), dma(1), dma(4), dma(1), dma(4), dma(1), dma(1), dma(2), dma(2, 4), dma(1), dma(4), dma(1), dma(4), dma(1), dma(1), dma(1), dma(1), dma(1), dma(4), dma(1), dma(8, 2), dma(1), dma(4), dma(1), dma(1), dma(1), dma(1), dma(1), dma(1), dma(1), dma(1), dma(1), dma(1), dma(2)],
        compiler_params=pltpu.CompilerParams(vmem_limit_bytes=53000 * 1024, collective_id=0, has_side_effects=True),
        name="whole")(lambdas, tokens[0], cotangent[0], value_weight, query_heads.reshape(L, 128), key_heads.reshape(L, 128))
    gq, gk, gt, gw, gl = pl.pallas_call(
        hand_out,
        out_shape=(S((L, 128), BF), S((L, 128), BF), S((128, 2048), BF), S((16, 2048), F32), S((1,), F32)),
        in_specs=[anywhere] * 5, out_specs=[hbm] * 4 + [smem],
        scratch_shapes=[pltpu.SMEM((8, 128), F32), dma(1), dma(4)],
        compiler_params=pltpu.CompilerParams(vmem_limit_bytes=8 * 1024 * 1024),
        name="hand_out")(gq, gk, gt, gw, gl)
    return gq.reshape(query_heads.shape), gk.reshape(key_heads.shape), gt[None], gw, gl


def solution(mesh):
    placed = (P("dp", "sp", None), P("dp", "sp", None), P(("sp", "dp"), None),
              P("dp", None, "sp", None), P("dp", None, "sp", None), P("sp"))
    outs = (P("dp", None, "sp", None), P("dp", None, "sp", None), P("dp", "sp", None), P(("sp", "dp"), None), P("sp"))
    return jax.shard_map(body, mesh=mesh, in_specs=placed, out_specs=outs, check_vma=False)
```

```python
import functools, math
import jax, jax.numpy as jnp
from jax import lax
from jax.experimental import pallas as pl
from jax.experimental.pallas import tpu as pltpu
from jax.sharding import PartitionSpec as P

EPS = 1e-6
B = 256
NB = 8
SCALE = 0.125
LOG2E = 1.4426950408889634
F32 = jnp.float32
BF = jnp.bfloat16

def nt(a, b):
    return lax.dot_general(a, b, (((1,), (1,)), ((), ())), preferred_element_type=F32)

def nn(a, b):
    return lax.dot_general(a, b, (((1,), (0,)), ((), ())), preferred_element_type=F32)

def tri(i, j):
    return (i * (i + 1)) // 2 + j

def paired(lo, n, body):
    def two(p, c):
        body(lo + 2 * p, 2)
        return c
    lax.fori_loop(0, n // 2, two, 0)
    def one(p, c):
        body(lo + n - 1, 1)
        return c
    lax.fori_loop(0, n % 2, one, 0)

def prepare(i, q_ref, k_ref, qz1, qz2, kt):
    rows = pl.ds(pl.multiple_of(i * B, B), B)
    q = q_ref[rows, :]
    first = lax.broadcasted_iota(jnp.int32, (B, 128), 1) < 64
    zero = jnp.zeros_like(q)
    qz1[i] = jnp.where(first, q, zero)
    qz2[i] = jnp.where(first, zero, q)
    kt[i] = k_ref[rows, :].T

def softmaxes(i, lam, k_ref, qz1, qz2, s1, s2, p1, p2, aa):
    q1, q2 = qz1[i], qz2[i]

    def score(j, m):
        k = k_ref[pl.ds(pl.multiple_of(j * B, B), B), :]
        a, b = nt(k, q1), nt(k, q2)
        return a, b

    def keep(j, a, b, m):
        s1[j] = a
        s2[j] = b
        return (jnp.maximum(m[0], jnp.max(a.reshape(B // 8, 8, B), axis=0)),
                jnp.maximum(m[1], jnp.max(b.reshape(B // 8, 8, B), axis=0)))

    a, b = score(i, None)
    seen = lax.broadcasted_iota(jnp.int32, (B, B), 0) <= lax.broadcasted_iota(jnp.int32, (B, B), 1)
    a = jnp.where(seen, a, -1e30)
    b = jnp.where(seen, b, -1e30)
    low = jnp.full((8, B), -1e30, F32)
    m = keep(i, a, b, (low, low))

    def off(j, m):
        a, b = score(j, m)
        return keep(j, a, b, m)
    def two(p, m):
        a, b = score(2 * p, m)
        c, d = score(2 * p + 1, m)
        m = keep(2 * p, a, b, m)
        return keep(2 * p + 1, c, d, m)
    m = lax.fori_loop(0, i // 2, two, m)
    m = lax.fori_loop(i - i % 2, i, off, m)
    m1 = jnp.max(m[0], axis=0, keepdims=True)
    m2 = jnp.max(m[1], axis=0, keepdims=True)
    c = SCALE * LOG2E

    def power(j, l):
        e1 = jnp.exp2((s1[j] - m1) * c)
        e2 = jnp.exp2((s2[j] - m2) * c)
        s1[j] = e1
        s2[j] = e2
        return (l[0] + jnp.sum(e1.reshape(B // 8, 8, B), axis=0),
                l[1] + jnp.sum(e2.reshape(B // 8, 8, B), axis=0))
    l = lax.fori_loop(0, i + 1, power, (jnp.zeros((8, B), F32), jnp.zeros((8, B), F32)))
    r1 = 1.0 / jnp.sum(l[0], axis=0, keepdims=True)
    r2 = 1.0 / jnp.sum(l[1], axis=0, keepdims=True)

    def norm(j, _):
        x1 = s1[j] * r1
        x2 = s2[j] * r2
        t = tri(i, j)
        p1[t] = x1.astype(BF)
        p2[t] = x2.astype(BF)
        aa[t] = (x1 - lam * x2).astype(BF)
        return _
    lax.fori_loop(0, i + 1, norm, 0)

def keys_block(j, vn, qz1, qz2, kt, p1, p2, aa, dot, do, delta, dqt):
    v = vn[j]
    k1t, k2t = kt[j, 0:64, :], kt[j, 64:128, :]

    def parts(i):
        t = tri(i, j)
        da = nn(v, dot[i])
        x1 = (p1[t].astype(F32) * (da - delta[i, 0:1, :])).astype(BF)
        x2 = (p2[t].astype(F32) * (da - delta[i, 1:2, :])).astype(BF)
        dv = nn(aa[t], do[i])
        dk1 = nn(x1, qz1[i])
        dk2 = nn(x2, qz2[i])
        dqt[i, 0:64, :] += nn(k1t, x1)
        dqt[i, 64:128, :] += nn(k2t, x2)
        return dv, dk1 , dk2

    def two(p, c):
        a = parts(j + 2 * p)
        b = parts(j + 2 * p + 1)
        return tuple(x + (y + z) for x, y, z in zip(c, a, b))
    def one(p, c):
        a = parts(p)
        return tuple(x + y for x, y in zip(c, a))
    n = NB - j
    zero = jnp.zeros((B, 128), F32)
    c = lax.fori_loop(0, n // 2, two, (zero, zero, zero))
    c = lax.fori_loop(NB - n % 2, NB, one, c)
    return c[0], c[1], c[2]


MESH = pl.DeviceIdType.MESH
V = pltpu.VMEM
S = jax.ShapeDtypeStruct


class Ring:
    def __init__(self, at, ss, rs, me, to):
        self.at, self.ss, self.rs, self.me, self.to = at, ss, rs, me, to

    def index(self, o):
        return lax.rem(self.me + (o + 4), 4)

    def copy(self, o, part, delta, sem):
        s, d = self.to(self.index(delta))
        ref = self.at(self.index(o), part)
        return pltpu.make_async_remote_copy(
            src_ref=ref, dst_ref=ref, send_sem=self.ss, recv_sem=self.rs(sem),
            device_id={"sp": s, "dp": d}, device_id_type=MESH)

    def start(self):
        self.copy(0, 0, 1, 0).start()
        self.copy(0, 1, -1, 0).start()
        self.copy(0, 1, 1, 1).start()
        self.copy(0, 0, -1, 1).start()

    def near(self):
        self.both(1, 0)
        self.copy(-1, 0, 1, 2).start()
        self.copy(1, 1, -1, 2).start()

    def both(self, o, sem):
        ref = self.at(self.index(o), None)
        pltpu.make_async_copy(ref, ref, self.rs(sem)).wait()

    def full(self):
        self.both(1, 1)

    def far(self):
        self.both(2, 2)


def kernel(lam_h, tok_h, cot_h, w_h, q_h, k_h, gq_h, gk_h, gt_h, gw_h, gl_h,
           xr, xc, w, wo, wq, cota, q_ref, k_ref, qz1, qz2, kt, vt, vn, v4, s1, s2, p1, p2, aa, dot, do, delta, dqt, ot, o2t,
           dvg, dvin, dvrow, gta, gwp, gwin, gws, gwf, gqb, gkb, gtb, gwo, glb, glin,
           lam_ref, load, wload, save, xs, xr_, ys, yr, zs, zr, ws, wr, rs_, rr, qs, qr, h1s, h1r, cs, cr, vs, vr, gs, gr, ds_, dr,
           es, er, ls, lr, fs, fr, wds, wdr, qds, qdr, gf):
    sp, dp = lax.axis_index("sp"), lax.axis_index("dp")
    y, z = lax.rem(sp, 4), lax.div(sp, 4)
    scope = jax.named_scope

    def sp_peers(body):
        lax.fori_loop(1, 16, lambda d, c: (body(lax.rem(sp + d, 16)), c)[1], 0)

    def dp_peers(body):
        lax.fori_loop(1, 8, lambda d, c: (body(lax.rem(dp + d, 8)), c)[1], 0)

    def remote(src, dst, ss, rs, s, d):
        return pltpu.make_async_remote_copy(src_ref=src, dst_ref=dst, send_sem=ss, recv_sem=rs,
                                            device_id={"sp": s, "dp": d}, device_id_type=MESH)

    def all_of(ref, sem):
        pltpu.make_async_copy(ref, ref, sem.at[0]).wait()

    def lanes(h, n=128):
        return pl.ds(pl.multiple_of(h * n, n), n)

    def rows(i, n=B):
        return pl.ds(pl.multiple_of(i * n, n), n)

    barrier = pltpu.get_barrier_semaphore()
    sp_peers(lambda s: pl.semaphore_signal(barrier, inc=1, device_id={"sp": s, "dp": dp}, device_id_type=MESH))
    dp_peers(lambda d: pl.semaphore_signal(barrier, inc=1, device_id={"sp": sp, "dp": d}, device_id_type=MESH))
    loads = [pltpu.make_async_copy(a, b, load.at[n]) for n, (a, b) in enumerate((
        (w_h, w.at[sp, dp]), (tok_h, xr.at[y]), (q_h, q_ref), (k_h, k_ref), (cot_h.at[:, lanes(sp)], cota.at[rows(sp, 128)]), (lam_h, lam_ref)))]
    for a in loads:
        a.start()
    parts = [pltpu.make_async_copy(w_h.at[:, pl.ds((4 * b + a) * 128, 128)], wo.at[a, :, pl.ds(b * 128, 128)], wload.at[0])
             for a in range(4) for b in range(4)]
    for a in parts:
        a.start()

    x_, core = lax.div(dp, 2), lax.rem(dp, 2)
    along_y = lambda i: (z * 4 + i, dp)
    along_z = lambda i: (i * 4 + y, dp)
    along_x = lambda i: (sp, 2 * i + core)

    def split(ref, view, n):
        return lambda i, part: view(i, pl.ds(0, n) if part is None else pl.ds(n // 2 * part, n // 2))

    wy = Ring(lambda i, part: w.at[z * 4 + i, dp] if part is None else w.at[z * 4 + i, dp, :, pl.ds(1024 * part, 1024)],
              ws.at[0], lambda n: wr.at[0, n], y, along_y)
    wz = Ring(lambda i, part: w.at[pl.ds(4 * i, 4), dp] if part is None else w.at[pl.ds(4 * i + 2 * part, 2), dp],
              ws.at[1], lambda n: wr.at[1, n], z, along_z)
    xring = Ring(split(xr, lambda i, d: xr.at[i, d], 128), xs.at[0], lambda n: xr_.at[n], y, along_y)
    cring = Ring(split(xc, lambda i, d: xc.at[i, d], 4), ys.at[0], lambda n: yr.at[n], y, along_y)
    wrow = Ring(split(w, lambda i, d: w.at[d, 2 * i + core], 16), rs_.at[0], lambda n: rr.at[n], x_, along_x)
    qrow = Ring(split(wq, lambda i, d: wq.at[d, 2 * i + core], 16), qs.at[0], lambda n: qr.at[n], x_, along_x)

    def other(ref, ring, o, ss, rs):
        d = 2 * ring.index(o) + core
        return remote(ref.at[:, d], ref.at[:, d], ss.at[0], rs.at[0], sp, dp + 1 - 2 * core)

    for a in loads[:2]:
        a.wait()
    all_of(wo, wload)
    wq[sp, dp] = wo[y]
    xc[y, z] = xr[y, :, lanes(z, 512)]
    with scope("barrier"):
        pl.semaphore_wait(barrier, 22)

    def head_rows(s, src, to):
        return remote(wo.at[lax.rem(to, 4)], wq.at[src, dp], h1s.at[0], h1r.at[0], s, dp)

    def columns(zz, src, to):
        return remote(xr.at[y, :, lanes(to, 512)], xc.at[y, src], zs.at[0], zr.at[0], zz * 4 + y, dp)

    def z_peers(body):
        for d in (1, 3, 2):
            body(lax.rem(z + d, 4))

    wy.start()
    sp_peers(lambda s: head_rows(s, sp, s).start())
    z_peers(lambda t: columns(t, z, t).start())
    def cot_part(s, src, to):
        return remote(cot_h.at[:, lanes(to)], cota.at[rows(src, 128)], cs.at[0], cr.at[0], s, dp)

    for n in (2, 3, 5):
        loads[n].wait()
    lam = lam_ref[0]

    def prep(i, c):
        prepare(i, q_ref, k_ref, qz1, qz2, kt)
        zero = jnp.zeros((128, B), F32)
        dqt[i] = zero
        ot[i] = zero
        o2t[i] = zero
        return c
    lax.fori_loop(0, NB, prep, 0)

    def soft(lo, hi):
        lax.fori_loop(lo, hi, lambda i, c: (softmaxes(i, lam, k_ref, qz1, qz2, s1, s2, p1, p2, aa), c)[1], 0)

    with scope("soft03"):
        soft(0, 3)
    with scope("wynear"):
        wy.near()
    xring.start()
    with scope("heads"):
        all_of(wq.at[pl.ds(0, 15), 0], h1r)
    qrow.start()
    other(wq, qrow, 0, qds, qdr).start()
    with scope("soft34"):
        soft(3, 4)
    with scope("wyfar"):
        wy.full()
        wy.far()
    wz.start()
    with scope("soft46"):
        soft(4, 6)
    with scope("xnear0"):
        xring.near()
    with scope("soft67"):
        soft(6, 7)
    with scope("qnear"):
        qrow.near()
        qrow.full()
        for o in (1, -1):
            other(wq, qrow, o, qds, qdr).start()
    with scope("wznear"):
        wz.near()
    sp_peers(lambda s: cot_part(s, sp, s).start())
    with scope("xfull"):
        xring.full()
    with scope("soft78"):
        soft(7, 8)
    with scope("wzfar"):
        wz.full()
        wz.far()
    wrow.start()
    with scope("qfar"):
        qrow.far()
        other(wq, qrow, 2, qds, qdr).start()
    with scope("qall"):
        all_of(wq.at[:, pl.ds(0, 4)], qdr)
    def v_part(zz, src, to, b):
        return remote(v4.at[to, b], vn.at[2 * src + lax.div(b, 2), rows(lax.rem(b, 2), 128)], vs.at[0], vr.at[src], zz * 4 + y, dp)

    def values(b):
        v = nn(xr[b], wq[...].reshape(2048, 512)).astype(BF)
        for t in range(4):
            v4[t, b] = v[:, t * 128:(t + 1) * 128]

            @pl.when(t != z)
            def _():
                v_part(t, z, t, b).start()
        vn[2 * z + lax.div(b, 2), rows(lax.rem(b, 2), 128), :] = v4[z, b]

    with scope("values3"):
        lax.fori_loop(0, 3, lambda n, c: (values(lax.rem(y + n + lax.div(n, 2), 4)), c)[1], 0)
    with scope("xfar"):
        xring.far()
    with scope("values1"):
        values(lax.rem(y + 2, 4))
    with scope("columns"):
        all_of(xc.at[0, pl.ds(0, 3)], zr)
    cring.start()

    def mixed(r):
        def one(e, c):
            j = 2 * r + e
            v = vn[j].T
            vt[j] = v

            def add(i, count):
                for m in range(count):
                    t = tri(i + m, j)
                    ot[i + m] += nn(v, aa[t])
                    o2t[i + m] += nn(v, p2[t])
            paired(j, NB - j, add)
            return c
        lax.fori_loop(0, 2, one, 0)

    def all_v(t):
        ref = vn.at[pl.ds(2 * t, 2)]
        pltpu.make_async_copy(ref, ref, vr.at[t]).wait()

    with scope("mix0"):
        mixed(z)
    for d in (1, 3):
        t = lax.rem(z + d, 4)
        with scope("v%d" % d):
            all_v(t)
        with scope("mix%d" % d):
            mixed(t)
    t = lax.rem(z + 2, 4)
    with scope("v2"):
        all_v(t)
    with scope("mix2"):
        mixed(t)
    other(w, wrow, 0, wds, wdr).start()
    with scope("cot"):
        loads[4].wait()
        all_of(cota.at[pl.ds(0, 1920)], cr)

    def mix(i, total):
        o, o2 = ot[i], o2t[i]
        g = cota[rows(i), :].astype(F32).T
        r = lax.rsqrt(jnp.mean(o * o, axis=0, keepdims=True) + EPS)
        yy = r * o
        d = (r * (g - yy * jnp.mean(g * yy, axis=0, keepdims=True))).astype(BF)
        dw = d.astype(F32)
        d2 = jnp.sum(dw * o2, axis=0, keepdims=True)
        d1 = jnp.sum(dw * o, axis=0, keepdims=True) + lam * d2
        dot[i] = d
        do[i] = dw.T.astype(BF)
        delta[i, 0:1, :] = d1
        delta[i, 1:2, :] = d2
        return total + d2
    with scope("mix"):
        total = lax.fori_loop(0, NB, mix, jnp.zeros((1, B), F32))
    glb[...] = jnp.broadcast_to(-jnp.sum(total, axis=1, keepdims=True), (8, 128))

    half = lax.broadcasted_iota(jnp.int32, (1, 128), 1) < 64
    ks = jnp.where(half, SCALE, -lam * SCALE)

    def gl_part(d, src, to):
        return remote(glb, glin.at[src], ls.at[0], lr.at[0], sp, d)

    def dv_part(yy, src, to, h):
        part = rows(lax.rem(to, 2), 128)
        return remote(dvg.at[h, 2 * z + lax.div(to, 2), part], dvin.at[h, src], ds_.at[0], dr.at[h], z * 4 + yy, dp)

    def y_peers(body):
        for d in (1, 3, 2):
            body(lax.rem(y + d, 4))

    def gw_part(d, src, to, h):
        return remote(gwp.at[h, to], gwin.at[h, src], es.at[0], er.at[0], sp, d)

    def send_dv(o):
        h = lax.rem(z + o, 4)
        y_peers(lambda t: dv_part(t, y, t, h).start())

    def send_weights(o):
        h = lax.rem(z + o, 4)
        g = sum(nn(dvg[h, 2 * b:2 * b + 2].reshape(512, 128).T, xc[:, b].reshape(512, 512)) for b in range(4))
        for n in range(4):
            gwp[h, :, n] = g[:, n * 128:(n + 1) * 128].T.astype(BF).reshape(8, 16, 128)
        dp_peers(lambda d: gw_part(d, dp, d, h).start())

    def dv_ring(j):
        return Ring(lambda i, part: dvg.at[i, j] if part is None else dvg.at[i, j, pl.ds(128 * part, 128)],
                    gs.at[0], lambda n: gr.at[j] if n < 1 else gf.at[n - 1], z, along_z)

    def main(n, c):
        j = NB - 1 - n
        dv, dk1, dk2 = keys_block(j, vn, qz1, qz2, kt, p1, p2, aa, dot, do, delta, dqt)
        dvg[z, j] = dv.astype(BF)
        dv_ring(j).start()
        gkb[rows(j), :] = ((dk1 + dk2) * ks).astype(BF)

        @pl.when(n == 2)
        def _():
            wrow.near()

        @pl.when(n == 4)
        def _():
            cring.near()
            dv_ring(7).near()

        @pl.when(n == 5)
        def _():
            dv_ring(6).near()

        @pl.when(n == 6)
        def _():
            dv_ring(5).near()

        @pl.when(n == 7)
        def _():
            dv_ring(4).near()
            wrow.full()
            for o in (-1, 1):
                other(w, wrow, o, wds, wdr).start()
        return c
    with scope("main"):
        lax.fori_loop(0, NB, main, 0)
    send_dv(0)
    save_k = pltpu.make_async_copy(gkb, gk_h, save.at[0])
    save_k.start()

    def fin(i, c):
        gqb[rows(i), :] = (dqt[i].T * ks).astype(BF)
        return c
    with scope("fin"):
        lax.fori_loop(0, NB, fin, 0)
    save_q = pltpu.make_async_copy(gqb, gq_h, save.at[1])
    save_q.start()
    with scope("near3"):
        dv_ring(3).near()
    with scope("cfar"):
        cring.full()
        cring.far()
    with scope("near21"):
        dv_ring(2).near()
    with scope("weights0"):
        send_weights(0)
    with scope("near1"):
        dv_ring(1).near()

    def gather(o):
        h = lax.rem(z + o, 4)
        dvin[h, y] = dvg[h, 2 * z + lax.div(y, 2), rows(lax.rem(y, 2), 128), :]
        pltpu.make_async_copy(dvin.at[h, pl.ds(0, 3)], dvin.at[h, pl.ds(0, 3)], dr.at[h]).wait()
        for a in range(4):
            dvrow[h, :, a * 128:(a + 1) * 128] = dvin[h, a]

    def times_rows(n, o):
        h = lax.rem(z + o, 4)
        return nt(dvrow[h], w[pl.ds(2 * n, 2), :, :, lanes(h, 512)].reshape(B, 512))

    with scope("near0"):
        dv_ring(0).near()
    with scope("full"):
        pltpu.make_async_copy(dvg.at[0], dvg.at[0], gf.at[0]).wait()
    for o in (1, 3):
        send_dv(o)
    with scope("wrowfar"):
        wrow.far()
        other(w, wrow, 2, wds, wdr).start()
    with scope("weights13"):
        for o in (1, 3):
            send_weights(o)
    with scope("far"):
        pltpu.make_async_copy(dvg.at[0], dvg.at[0], gf.at[1]).wait()
    send_dv(2)
    with scope("distant"):
        send_weights(2)
    dp_peers(lambda d: gl_part(d, dp, d).start())
    glin[dp] = glb[...]
    for h in range(4):
        gwin[h, dp] = gwp[h, dp]
    with scope("gather"):
        for o in (0, 1, 3):
            gather(o)
    with scope("wrowall"):
        all_of(w.at[:, pl.ds(0, 4)], wdr)

    def most(n, c):
        gta[:, rows(n)] = times_rows(n, 0) + times_rows(n, 1) + times_rows(n, 3)
        return c
    with scope("tgrada"):
        lax.fori_loop(0, 6, most, 0)
    with scope("gwwait"):
        all_of(gwin.at[:, pl.ds(0, 7)], er)
    for h in range(4):
        acc = gwin[h, 0].astype(F32)
        for d in range(1, 8):
            acc = acc + gwin[h, d].astype(F32)
        gws[:, h] = acc.astype(BF)

    def fin_part(yy, src, to):
        return remote(gws.at[to], gwf.at[src], fs.at[0], fr.at[0], z * 4 + yy, dp)
    y_peers(lambda t: fin_part(t, y, t).start())
    gwf[y] = gws[y]
    all_of(glin.at[pl.ds(0, 7)], lr)
    tot = glin[0]
    for d in range(1, 8):
        tot = tot + glin[d]
    delta[0] = jnp.concatenate([tot, tot], axis=1)
    save_l = pltpu.make_async_copy(delta.at[0, :, pl.ds(0, 128)], gl_h, save.at[3])
    save_l.start()
    with scope("tgradc"):
        lax.fori_loop(6, NB, most, 0)
    with scope("dvwait"):
        gather(2)

    def tokens_grad(n, c):
        gtb[:, rows(n)] = (gta[:, rows(n)] + times_rows(n, 2)).astype(BF)
        return c
    with scope("tgradb"):
        lax.fori_loop(0, NB, tokens_grad, 0)
    save_t = pltpu.make_async_copy(gtb, gt_h, save.at[2])
    save_t.start()
    with scope("finwait"):
        all_of(gwf.at[pl.ds(0, 3)], fr)
    for a in range(4):
        for b in range(4):
            gwo[:, (4 * b + a) * 128:(4 * b + a + 1) * 128] = gwf[a, b].astype(F32)
    save_w = pltpu.make_async_copy(gwo, gw_h, save.at[4])
    save_w.start()
    all_of(xr.at[pl.ds(0, 3)], xs)
    all_of(xc.at[pl.ds(0, 3)], ys)
    all_of(w.at[pl.ds(0, 3), 0], ws)
    pltpu.make_async_copy(w.at[pl.ds(0, 12), 0], w.at[pl.ds(0, 12), 0], ws.at[1]).wait()
    all_of(w.at[:, pl.ds(0, 3)], rs_)
    all_of(wq.at[:, pl.ds(0, 3)], qs)
    all_of(w.at[:, pl.ds(0, 4)], wds)
    all_of(wq.at[:, pl.ds(0, 4)], qds)
    all_of(dvg.at[pl.ds(0, 3)], gs)
    all_of(wq.at[pl.ds(0, 15), 0], h1s)
    all_of(cota.at[pl.ds(0, 1920)], cs)
    all_of(dvin.at[pl.ds(0, 3)], ds_)
    all_of(gwin.at[:, pl.ds(0, 7)], es)
    all_of(xc.at[0, pl.ds(0, 3)], zs)
    all_of(v4.at[pl.ds(0, 3)], vs)
    all_of(glin.at[pl.ds(0, 7)], ls)
    all_of(gwf.at[pl.ds(0, 3)], fs)
    with scope("savewait"):
        for a in (save_k, save_q, save_t, save_l, save_w):
            a.wait()


def hand_out(*refs):
    came, outs, (held, got, put) = refs[:5], refs[5:10], refs[10:]
    saves = [pltpu.make_async_copy(came[n], outs[n], put.at[n]) for n in range(4)]
    scalar = pltpu.make_async_copy(came[4], held, got.at[0])
    scalar.start()
    for a in saves:
        a.start()
    scalar.wait()
    outs[4][0] = held[0, 0]
    for a in saves:
        a.wait()


def body(tokens, cotangent, value_weight, query_heads, key_heads, lambdas):
    L = query_heads.shape[1]
    smem = pl.BlockSpec(memory_space=pltpu.SMEM)
    anywhere = pl.BlockSpec(memory_space=pl.ANY)
    hbm = pl.BlockSpec(memory_space=pltpu.HBM)
    tiles = (NB * (NB + 1) // 2, B, B)
    dma = lambda *n: pltpu.SemaphoreType.DMA(n)
    gq, gk, gt, gw, gl = pl.pallas_call(
        kernel,
        out_shape=(S((L, 128), BF), S((L, 128), BF), S((128, 2048), BF), S((16, 2048), F32), S((8, 128), F32)),
        in_specs=[anywhere] * 6, out_specs=[anywhere] * 5,
        scratch_shapes=[
            V((4, 128, 2048), BF), V((4, 4, 128, 512), BF), V((16, 8, 16, 2048), BF), V((4, 16, 512), BF), V((16, 8, 16, 512), BF),
            V((L, 128), BF), V((L, 128), BF), V((L, 128), BF),
            V((NB, B, 128), BF), V((NB, B, 128), BF), V((NB, 128, B), BF), V((NB, 128, B), BF), V((NB, B, 128), BF), V((4, 4, 128, 128), BF),
            V((NB, B, B), F32), V((NB, B, B), F32), V(tiles, BF), V(tiles, BF), V(tiles, BF),
            V((NB, 128, B), BF), V((NB, B, 128), BF), V((NB, 8, B), F32), V((NB, 128, B), F32), V((NB, 128, B), F32), V((NB, 128, B), F32),
            V((4, NB, B, 128), BF), V((4, 4, 128, 128), BF), V((4, 128, 512), BF), V((128, 2048), F32), V((4, 8, 4, 16, 128), BF), V((4, 8, 4, 16, 128), BF),
            V((4, 4, 16, 128), BF), V((4, 4, 16, 128), BF), V((L, 128), BF), V((L, 128), BF), V((128, 2048), BF), V((16, 2048), F32),
            V((8, 128), F32), V((8, 8, 128), F32), pltpu.SMEM((1,), F32),
            dma(6), dma(1), dma(5), dma(1), dma(3), dma(1), dma(3), dma(1), dma(1), dma(2), dma(2, 3), dma(1), dma(3), dma(1), dma(3), dma(1), dma(1), dma(1), dma(1), dma(1), dma(4), dma(1), dma(8), dma(1), dma(4), dma(1), dma(1), dma(1), dma(1), dma(1), dma(1), dma(1), dma(1), dma(1), dma(1), dma(2)],
        compiler_params=pltpu.CompilerParams(vmem_limit_bytes=53000 * 1024, collective_id=0, has_side_effects=True),
        name="whole")(lambdas, tokens[0], cotangent[0], value_weight, query_heads.reshape(L, 128), key_heads.reshape(L, 128))
    gq, gk, gt, gw, gl = pl.pallas_call(
        hand_out,
        out_shape=(S((L, 128), BF), S((L, 128), BF), S((128, 2048), BF), S((16, 2048), F32), S((1,), F32)),
        in_specs=[anywhere] * 5, out_specs=[hbm] * 4 + [smem],
        scratch_shapes=[pltpu.SMEM((8, 128), F32), dma(1), dma(4)],
        compiler_params=pltpu.CompilerParams(vmem_limit_bytes=8 * 1024 * 1024),
        name="hand_out")(gq, gk, gt, gw, gl)
    return gq.reshape(query_heads.shape), gk.reshape(key_heads.shape), gt[None], gw, gl


def solution(mesh):
    placed = (P("dp", "sp", None), P("dp", "sp", None), P(("sp", "dp"), None),
              P("dp", None, "sp", None), P("dp", None, "sp", None), P("sp"))
    outs = (P("dp", None, "sp", None), P("dp", None, "sp", None), P("dp", "sp", None), P(("sp", "dp"), None), P("sp"))
    return jax.shard_map(body, mesh=mesh, in_specs=placed, out_specs=outs, check_vma=False)
```
